256 devices in a mesh: grp: 2 (over y), sp: 16 (over z), fs: 4 (over x), tp: 2 (over core).
Axes of the slice: x: 4, y: 2, z: 16, core: 2. Of those that a mesh axis runs over, the one named last changes fastest.
The devices are a block of a 4x16x16 slice.
Arguments:
- inputs: bfloat16 [16, 2048, 2048], P(('grp', 'fs'), 'sp', 'tp'), parts along dimension 0, may hold values from -20 to 20
- input_norm_gain: bfloat16 [2048], replicated, may hold values from 0.099609375 to 1.8984375
- softmax_query_matrix: bfloat16 [2048, 1024], P('fs', 'tp'), may hold values from -0.088388348 to 0.088388348
- softmax_key_matrix: bfloat16 [2048, 1024], P('fs', 'tp'), may hold values from -3.557631 to 3.557631
- softmax_value_matrix: bfloat16 [2048, 1024], P('fs', 'tp'), may hold values from -0.125 to 0.125
- running_forget_gate: float32 [16, 2048, 16], P(('grp', 'fs'), None, 'tp'), parts along dimension 0, may hold values from -105 to 0, as said below
- receptance_weight: bfloat16 [2048, 1024], P('fs', 'tp'), may hold values from -0.125 to 0.125
- linear_key_weight: bfloat16 [2048, 1024], P('fs', 'tp'), may hold values from -0.125 to 0.125
- linear_value_weight: bfloat16 [2048, 1024], P('fs', 'tp'), may hold values from -0.125 to 0.125
- decay_lower_map: bfloat16 [2048, 128], replicated, may hold values from -0.125 to 0.125
- decay_upper_map: bfloat16 [128, 1024], replicated, may hold values from -1 to 1
- decay_offset_base: float32 [1024], replicated, may hold values from -12 to -2
- decay_extra_log: float32 [16, 2048, 16], P(('grp', 'fs'), 'sp', 'tp'), parts along dimension 0, may hold values from -1 to 0
- rate_lower_map: bfloat16 [2048, 128], replicated, may hold values from -0.125 to 0.125
- rate_upper_map: bfloat16 [128, 1024], replicated, may hold values from -1 to 1
- rate_offset_base: float32 [1024], replicated, may hold values from -2 to 2
- linear_head_gain: bfloat16 [1024], replicated, may hold values from 0.099609375 to 1.8984375
- starting_state: float32 [16, 16, 64, 64], P(('grp', 'fs'), 'tp'), parts along dimension 0, may hold values from -144.81547 to 144.81547
- softmax_output_weight: bfloat16 [2048, 1024], P(None, 'tp'), may hold values from -1.5 to 1.5
- linear_output_weight: bfloat16 [2048, 1024], P(None, 'tp'), may hold values from -0.125 to 0.125
Outputs:
- mixed: bfloat16 [16, 2048, 2048], P(('grp', 'fs', 'tp'), 'sp'), parts along dimension 0
The draws below stay inside these ranges and needn't reach their ends.
There are 2 independent parts, one for each index of `grp`. The reference program is written for one: setup_inputs(seed, part) draws one part's arguments, and reference() takes and returns one part's arrays. A program takes and returns all parts, laid end to end along the dimension named above; an argument that names none is the same for every part. Nothing has to cross between parts.
Inputs may be any that keep to these rules, and one draw needn't show every extreme that they name: `running_forget_gate`: never rising along positions.
All inputs are finite; a program needn't handle non-finite values.
Results may differ from the reference program's by a relative error of at most 0.0095.
The reference program's roundings to bfloat16 on the way count: a program that leaves them out, or rounds other values in their place, can miss the bound.
Values may be sent and summed in bfloat16 or wider, within the bound.
No kernel may reach another device: no remote copies, remote signals or barrier semaphores. Data moves between devices by JAX's collectives and lax.ppermute only.
A program may use at most 128 MiB of HBM per device.

```python
import math
import jax
import jax.numpy as jnp
from jax import lax

D = 2048
HF = 16
LINEAR_HEADS = 16
HEAD_CHANNELS = 64
LR = 128
TOK_DEV = 128
FW = 1024
RW = 1024
SEQUENCE_LENGTH = 2048
BATCH_SERIES_NUM = 8
N_TP = 2


def draw_inputs(key, part):
    base_key = jax.random.fold_in(key, 0)
    values = jnp.clip(jax.random.normal(base_key, (BATCH_SERIES_NUM, SEQUENCE_LENGTH, D), jnp.float32), -6.0, 6.0)
    return values.astype(jnp.bfloat16)


def attention_pair(key):
    query_key, other_key = jax.random.split(jax.random.fold_in(key, 71), 2)
    query_part = jnp.clip(jax.random.normal(query_key, (D, FW), jnp.float32), -4.0, 4.0) / math.sqrt(D)
    other_part = jnp.clip(jax.random.normal(other_key, (D, FW), jnp.float32), -4.0, 4.0) / math.sqrt(D)
    return (query_part, other_part)


def draw_softmax_query_matrix(key, part):
    return attention_pair(key)[0].astype(jnp.bfloat16)


def draw_softmax_key_matrix(key, part):
    return attention_pair(key)[1].astype(jnp.bfloat16)


def spike_rows_list(location_seed, extent_seed, item_number):
    places = jax.random.randint(location_seed, (item_number, 2), 1, SEQUENCE_LENGTH)
    sizes = jnp.log(jax.random.uniform(extent_seed, (item_number, 2), jnp.float32, 0.5, 0.8))
    positions = jnp.arange(SEQUENCE_LENGTH)
    hits = jnp.where(positions[None, None, :] == places[:, :, None], sizes[:, :, None], 0.0)
    return jnp.sum(hits, axis=1)


def draw_running_forget_gate(key, part):
    fast_key, speed_key, block_key, jitter_key, location_seed, extent_seed = jax.random.split(key, 6)
    fast_share = 0.5
    is_fast = jax.random.uniform(fast_key, (BATCH_SERIES_NUM, 1, HF), jnp.float32) < fast_share
    fast_rate = jnp.exp(jax.random.uniform(speed_key, (BATCH_SERIES_NUM, 1, HF), jnp.float32, math.log(1.0 / 100.0), math.log(1.0 / 30.0)))
    blocks = SEQUENCE_LENGTH // TOK_DEV
    tile_pace = jnp.exp(jax.random.uniform(block_key, (BATCH_SERIES_NUM, blocks, 1, HF), jnp.float32, math.log(0.5), math.log(2.0))) / SEQUENCE_LENGTH
    tile_pace = jnp.broadcast_to(tile_pace, (BATCH_SERIES_NUM, blocks, TOK_DEV, HF)).reshape(BATCH_SERIES_NUM, SEQUENCE_LENGTH, HF)
    tiny_jitter = jax.random.uniform(jitter_key, (BATCH_SERIES_NUM, SEQUENCE_LENGTH, HF), jnp.float32, 0.5, 1.5)
    iterations_done = -jnp.where(is_fast, fast_rate, tile_pace) * tiny_jitter
    iterations_done = iterations_done + spike_rows_list(location_seed, extent_seed, BATCH_SERIES_NUM)[:, :, None]
    return jnp.cumsum(iterations_done, axis=1)


def draw_decay_offset_base(key, part):
    fast_key, jitter_key = jax.random.split(key, 2)
    fast_share = 0.5
    is_fast = jax.random.uniform(fast_key, (LINEAR_HEADS, 1), jnp.float32) < fast_share
    tiny_jitter = jax.random.uniform(jitter_key, (LINEAR_HEADS, HEAD_CHANNELS), jnp.float32, -0.5, 0.5)
    slow_level = -(math.log(SEQUENCE_LENGTH) + 2.0)
    return (jnp.where(is_fast, -3.4, slow_level) + tiny_jitter).reshape(RW)


def draw_decay_extra_log(key, part):
    block_key, jitter_key, location_seed, extent_seed = jax.random.split(key, 4)
    blocks = SEQUENCE_LENGTH // TOK_DEV
    tile_pace = jnp.exp(jax.random.uniform(block_key, (BATCH_SERIES_NUM, blocks, 1, LINEAR_HEADS), jnp.float32, math.log(0.15), math.log(0.6))) / SEQUENCE_LENGTH
    tile_pace = jnp.broadcast_to(tile_pace, (BATCH_SERIES_NUM, blocks, TOK_DEV, LINEAR_HEADS)).reshape(BATCH_SERIES_NUM, SEQUENCE_LENGTH, LINEAR_HEADS)
    tiny_jitter = jax.random.uniform(jitter_key, (BATCH_SERIES_NUM, SEQUENCE_LENGTH, LINEAR_HEADS), jnp.float32, 0.5, 1.5)
    return -tile_pace * tiny_jitter + spike_rows_list(location_seed, extent_seed, BATCH_SERIES_NUM)[:, :, None]


def draw_starting_state(key, part):
    level = 0.8 * math.sqrt(SEQUENCE_LENGTH)
    values = jnp.clip(jax.random.normal(key, (BATCH_SERIES_NUM, LINEAR_HEADS, HEAD_CHANNELS, HEAD_CHANNELS), jnp.float32), -4.0, 4.0) * level
    return values


def block_scale(key, dims, cuts, smallest, top_value):
    def one(dim, parts):
        heights = jax.random.uniform(jax.random.fold_in(jax.random.fold_in(key, 6), dim), (parts,), jnp.float32, smallest / len(cuts), top_value / len(cuts))
        return jnp.repeat(jnp.exp(heights), dims[dim] // parts).reshape((-1,) + (1,) * (len(dims) - dim - 1))

    factor_of = one(*cuts[0])
    for cut in cuts[1:]:
        factor_of = factor_of * one(*cut)
    return factor_of


def noise(stream_key, dims, scale, bound, shards=(), kind=jnp.bfloat16):
    values = scale * jax.random.normal(stream_key, dims, jnp.float32)
    if shards:
        values = values * block_scale(stream_key, dims, shards, -0.22, 0.18)
    return jnp.clip(values, -bound, bound).astype(kind)


def setup_inputs(seed: int = 0, part: int = 0) -> dict:
    key_list = jax.random.split(jax.random.key(seed), 21)
    part_keys = jax.random.split(jax.random.fold_in(key_list[20], part), 21)
    inputs = draw_inputs(jax.random.fold_in(jax.random.fold_in(key_list[20], part), 71), part)
    input_norm_gain = jnp.clip(1.0 + 0.18 * jax.random.normal(key_list[1], (D,), jnp.float32), 0.099609375, 1.8984375).astype(jnp.bfloat16)
    softmax_query_matrix = draw_softmax_query_matrix(jax.random.fold_in(key_list[20], 71), part)
    softmax_key_matrix = draw_softmax_key_matrix(jax.random.fold_in(key_list[20], 71), part)
    softmax_value_matrix = noise(key_list[4], (D, FW), D ** -0.5, 0.125, ((0, 4), (1, 2)))
    running_forget_gate = draw_running_forget_gate(jax.random.fold_in(jax.random.fold_in(key_list[20], part), 71), part)
    receptance_weight = noise(key_list[6], (D, RW), D ** -0.5, 0.125, ((0, 4), (1, 2)))
    linear_key_weight = noise(key_list[7], (D, RW), D ** -0.5, 0.125, ((0, 4), (1, 2)))
    linear_value_weight = noise(key_list[8], (D, RW), D ** -0.5, 0.125, ((0, 4), (1, 2)))
    decay_lower_map = noise(key_list[9], (D, LR), D ** -0.5, 0.125)
    decay_upper_map = noise(key_list[10], (LR, RW), (LR // 4) ** -0.5, 1.0)
    decay_offset_base = draw_decay_offset_base(jax.random.fold_in(key_list[20], 71), part)
    decay_extra_log = draw_decay_extra_log(jax.random.fold_in(jax.random.fold_in(key_list[20], part), 71), part)
    rate_lower_map = noise(key_list[13], (D, LR), D ** -0.5, 0.125)
    rate_upper_map = noise(key_list[14], (LR, RW), (LR // 4) ** -0.5, 1.0)
    rate_offset_base = jnp.clip(jax.random.uniform(key_list[15], (RW,), jnp.float32, -2.0, 2.0), -2.0, 2.0)
    linear_head_gain = jnp.clip(1.0 + 0.18 * jax.random.normal(key_list[16], (RW,), jnp.float32), 0.099609375, 1.8984375).astype(jnp.bfloat16)
    starting_state = draw_starting_state(jax.random.fold_in(jax.random.fold_in(key_list[20], part), 71), part)
    softmax_output_weight = noise(key_list[18], (D, FW), (FW // 64) ** -0.5, 1.5, ((1, 2),))
    linear_output_weight = noise(key_list[19], (D, RW), (2 * RW) ** -0.5, 0.125, ((1, 2),))
    return dict(inputs=inputs, input_norm_gain=input_norm_gain, softmax_query_matrix=softmax_query_matrix, softmax_key_matrix=softmax_key_matrix, softmax_value_matrix=softmax_value_matrix, running_forget_gate=running_forget_gate, receptance_weight=receptance_weight, linear_key_weight=linear_key_weight, linear_value_weight=linear_value_weight, decay_lower_map=decay_lower_map, decay_upper_map=decay_upper_map, decay_offset_base=decay_offset_base, decay_extra_log=decay_extra_log, rate_lower_map=rate_lower_map, rate_upper_map=rate_upper_map, rate_offset_base=rate_offset_base, linear_head_gain=linear_head_gain, starting_state=starting_state, softmax_output_weight=softmax_output_weight, linear_output_weight=linear_output_weight)


HIGH = lax.Precision.HIGHEST

def to_stored(values):
    return lax.optimization_barrier(values.astype(jnp.bfloat16)).astype(jnp.float32)

def normed_rows(inputs, input_norm_gain):
    values = inputs.astype(jnp.float32)
    scaling = lax.rsqrt(lax.optimization_barrier(jnp.mean(values * values, axis=-1, keepdims=True)) + 1e-06)
    return (values * scaling * input_norm_gain.astype(jnp.float32)).astype(jnp.bfloat16)

def product(left, right):
    return jnp.dot(left, right, preferred_element_type=jnp.float32)

def fox_sequence(items):
    queries, key_rows, value_rows, gates = items
    query_float = queries.astype(jnp.float32)
    key_float = key_rows.astype(jnp.float32)
    value_float = value_rows.astype(jnp.float32)
    key_place = jnp.arange(SEQUENCE_LENGTH).astype(jnp.int32)
    gates_by_head = gates.T

    def one_block(block_index):
        begin = (block_index * TOK_DEV).astype(jnp.int32)
        query_block = lax.dynamic_slice_in_dim(query_float, begin, TOK_DEV, 0)
        gate_block = lax.dynamic_slice_in_dim(gates, begin, TOK_DEV, 0)
        score = jnp.einsum('qhd,khd->hqk', query_block, key_float, precision=HIGH) * HEAD_CHANNELS ** (-0.5)
        score = score + gate_block.T[:, :, None] - gates_by_head[:, None, :]
        query_place = begin + jnp.arange(TOK_DEV).astype(jnp.int32)
        live = query_place[:, None] >= key_place[None, :]
        peak = lax.optimization_barrier(jnp.max(jnp.where(live, score, -jnp.inf), axis=-1, keepdims=True))
        weights = jnp.where(live, jnp.exp(score - peak), 0.0)
        totals = lax.optimization_barrier(jnp.sum(weights, axis=-1))
        rounded = to_stored(weights)
        mixed_values = jnp.einsum('hqk,khd->hqd', rounded, value_float, precision=HIGH)
        return (mixed_values / totals[:, :, None]).astype(jnp.bfloat16)
    blocks = lax.map(one_block, jnp.arange(SEQUENCE_LENGTH // TOK_DEV).astype(jnp.int32))
    return blocks.transpose(0, 2, 1, 3).reshape(SEQUENCE_LENGTH, HF * HEAD_CHANNELS)

def linear_all(receptance, lin_keys, lin_values, decay_logged, rate, starting_state):
    norms = lax.rsqrt(lax.optimization_barrier(jnp.sum(lin_keys * lin_keys, axis=-1, keepdims=True)) + 1e-06)
    unit = lin_keys * norms
    zeta = -unit
    beta = unit * rate
    fading = jnp.exp(decay_logged)

    def advance(state, items):
        rec_now, fade_now, key_now, value_now, zeta_now, beta_now = items
        pulled = jnp.einsum('shvk,shk->shv', state, zeta_now, precision=HIGH)
        state = state * fade_now[:, :, None, :] + pulled[..., None] * beta_now[:, :, None, :] + value_now[..., None] * key_now[:, :, None, :]
        return (state, jnp.einsum('shvk,shk->shv', state, rec_now, precision=HIGH))
    items = tuple((array.transpose(1, 0, 2, 3) for array in (receptance, fading, lin_keys, lin_values, zeta, beta)))
    final_state, outputs = lax.scan(advance, starting_state, items)
    return outputs.transpose(1, 0, 2, 3)

def reference(inputs, input_norm_gain, softmax_query_matrix, softmax_key_matrix, softmax_value_matrix, running_forget_gate, receptance_weight, linear_key_weight, linear_value_weight, decay_lower_map, decay_upper_map, decay_offset_base, decay_extra_log, rate_lower_map, rate_upper_map, rate_offset_base, linear_head_gain, starting_state, softmax_output_weight, linear_output_weight):
    normed = normed_rows(inputs, input_norm_gain)
    flat_rows = normed.reshape(BATCH_SERIES_NUM * SEQUENCE_LENGTH, D)

    def head_split(weight, item_number):
        return product(flat_rows, weight).astype(jnp.bfloat16).reshape(BATCH_SERIES_NUM, SEQUENCE_LENGTH, item_number, HEAD_CHANNELS)
    queries = head_split(softmax_query_matrix, HF)
    key_rows = head_split(softmax_key_matrix, HF)
    value_rows = head_split(softmax_value_matrix, HF)
    fox_out = lax.map(fox_sequence, (queries, key_rows, value_rows, running_forget_gate))
    receptance = to_stored(product(flat_rows, receptance_weight)).reshape(BATCH_SERIES_NUM, SEQUENCE_LENGTH, LINEAR_HEADS, HEAD_CHANNELS)
    lin_keys = to_stored(product(flat_rows, linear_key_weight)).reshape(BATCH_SERIES_NUM, SEQUENCE_LENGTH, LINEAR_HEADS, HEAD_CHANNELS)
    lin_values = to_stored(product(flat_rows, linear_value_weight)).reshape(BATCH_SERIES_NUM, SEQUENCE_LENGTH, LINEAR_HEADS, HEAD_CHANNELS)
    decay_low = jnp.tanh(product(flat_rows, decay_lower_map)).astype(jnp.bfloat16)
    decay_preact = decay_offset_base + product(decay_low, decay_upper_map)
    decay_logged = (-jnp.exp(-jax.nn.softplus(-decay_preact) - 0.5)).reshape(BATCH_SERIES_NUM, SEQUENCE_LENGTH, LINEAR_HEADS, HEAD_CHANNELS) + decay_extra_log[..., None]
    rate_low = product(flat_rows, rate_lower_map).astype(jnp.bfloat16)
    rate = jax.nn.sigmoid(rate_offset_base + product(rate_low, rate_upper_map)).reshape(BATCH_SERIES_NUM, SEQUENCE_LENGTH, LINEAR_HEADS, HEAD_CHANNELS)
    lin_raw = linear_all(receptance, lin_keys, lin_values, decay_logged, rate, starting_state)
    center = lax.optimization_barrier(jnp.mean(lin_raw, axis=-1, keepdims=True))
    spread = lax.optimization_barrier(jnp.mean(jnp.square(lin_raw - center), axis=-1, keepdims=True))
    lin_out = ((lin_raw - center) * lax.rsqrt(spread + 0.00064) * linear_head_gain.astype(jnp.float32).reshape(LINEAR_HEADS, HEAD_CHANNELS)).astype(jnp.bfloat16)
    fox_rows = fox_out.reshape(BATCH_SERIES_NUM * SEQUENCE_LENGTH, FW)
    lin_rows = lin_out.reshape(BATCH_SERIES_NUM * SEQUENCE_LENGTH, RW)
    fox_group = FW // N_TP
    lin_group = RW // N_TP
    summed = jnp.zeros((BATCH_SERIES_NUM * SEQUENCE_LENGTH, D), jnp.float32)
    for group in range(N_TP):
        partial_value = product(fox_rows[:, group * fox_group:(group + 1) * fox_group], softmax_output_weight[:, group * fox_group:(group + 1) * fox_group].T)
        partial_value = partial_value + product(lin_rows[:, group * lin_group:(group + 1) * lin_group], linear_output_weight[:, group * lin_group:(group + 1) * lin_group].T)
        summed = summed + to_stored(partial_value)
    return summed.astype(jnp.bfloat16).reshape(BATCH_SERIES_NUM, SEQUENCE_LENGTH, D)
```

```python
import functools

import jax
import jax.numpy as jnp
from jax import lax
from jax.experimental import pallas as pl
from jax.experimental.pallas import tpu as pltpu
from jax.sharding import PartitionSpec as P

HEAD_CHANNELS = 64
CHUNK = 64
F32 = jnp.float32
BF16 = jnp.bfloat16
VMEM_BYTES = 56 * 1024 * 1024

MM = (((1,), (0,)), ((), ()))
NT = (((1,), (1,)), ((), ()))
TN = (((0,), (0,)), ((), ()))


def mul(left, right, dims=MM):
    return lax.dot_general(
        left.astype(BF16), right.astype(BF16), dims, preferred_element_type=F32
    )


def places(shape, dim):
    return lax.broadcasted_iota(jnp.int32, shape, dim)


def attention_kernel(blocks_ref, gate_ref, out_ref, key_scr, value_scr):
    count, _, width = blocks_ref.shape
    channels = HEAD_CHANNELS
    for i in range(count):
        gate = gate_ref[:, i * width : (i + 1) * width]
        high = gate.astype(BF16).astype(F32)
        rest = gate - high
        middle = rest.astype(BF16).astype(F32)
        low = rest - middle
        row = places((channels, width), 0)
        extra = jnp.where(row == 0, high, jnp.where(row == 1, middle, jnp.where(row == 2, low, 0.0)))
        key_rows = blocks_ref[i, channels : 2 * channels, :].astype(F32)
        key_scr[i * width : (i + 1) * width, :] = jnp.concatenate((key_rows, extra), 0).T.astype(BF16)
        value_scr[:, i * width : (i + 1) * width] = blocks_ref[i, 2 * channels :, :]
    step = 2 * width
    row = places((channels, step), 0)
    tail = jnp.where(row < 3, -1.0, 0.0).astype(BF16)
    live = places((step, step), 0) <= places((step, step), 1)
    for i in range(count // 2):
        query = jnp.concatenate(
            (blocks_ref[2 * i, :channels, :], blocks_ref[2 * i + 1, :channels, :]), 1
        )
        query = (query.astype(F32) * channels ** (-0.5)).astype(BF16)
        query = jnp.concatenate((query, tail), 0)
        before = i * step
        own = lax.dot_general(
            key_scr[before : before + step, :], query, MM, preferred_element_type=F32
        )
        own = jnp.where(live, own, -1e30)
        top = jnp.max(own, axis=0, keepdims=True)
        if before:
            past = lax.dot_general(key_scr[:before, :], query, MM, preferred_element_type=F32)
            top = jnp.maximum(top, jnp.max(past, axis=0, keepdims=True))
        weight = jnp.exp(own - top)
        total = jnp.sum(weight, axis=0, keepdims=True)
        mixed = lax.dot_general(
            value_scr[:, before : before + step],
            weight.astype(BF16),
            MM,
            preferred_element_type=F32,
        )
        if before:
            weight = jnp.exp(past - top)
            total = total + jnp.sum(weight, axis=0, keepdims=True)
            mixed = mixed + lax.dot_general(
                value_scr[:, :before], weight.astype(BF16), MM, preferred_element_type=F32
            )
        mixed = (mixed / total).astype(BF16)
        out_ref[2 * i] = mixed[:, :width]
        out_ref[2 * i + 1] = mixed[:, width:]


def attention(blocks, gate):
    count, rows, width = blocks.shape
    whole = pl.BlockSpec(memory_space=pltpu.VMEM)
    return pl.pallas_call(
        attention_kernel,
        out_shape=jax.ShapeDtypeStruct((count, HEAD_CHANNELS, width), BF16),
        in_specs=[whole, whole],
        out_specs=whole,
        scratch_shapes=[
            pltpu.VMEM((count * width, 2 * HEAD_CHANNELS), BF16),
            pltpu.VMEM((HEAD_CHANNELS, count * width), BF16),
        ],
        compiler_params=pltpu.CompilerParams(vmem_limit_bytes=VMEM_BYTES),
        cost_estimate=pl.CostEstimate(
            flops=4 * HEAD_CHANNELS * (count * width) ** 2,
            bytes_accessed=4 * count * rows * width,
            transcendentals=(count * width) ** 2 // 2,
        ),
        name="attention",
    )(blocks, gate)


def chunk_masks(size):
    row, col = places((2 * size, 2 * size), 0), places((2 * size, 2 * size), 1)
    same = row // CHUNK == col // CHUNK
    return row, col, same


def maps_kernel(proj_ref, log_ref, rate_ref, q_ref, o_ref, maps_ref):
    size = proj_ref.shape[0]
    cols = log_ref.shape[1]
    lanes = 2 * HEAD_CHANNELS
    pairs = cols // lanes
    row, col, same = chunk_masks(size)
    strict = same & (row > col)
    upto = same & (row >= col)
    merges = []
    block = 2
    while block < CHUNK:
        merges.append((row // (2 * block) == col // (2 * block)) & (row // block > col // block))
        block *= 2
    pairs_of_two = (row // 2 == col // 2) & (row > col)
    identity = (row == col).astype(F32)
    lane = places((size, lanes), 1)
    first_head = lane < HEAD_CHANNELS
    head_block = (places((lanes, lanes), 0) < HEAD_CHANNELS) == (
        places((lanes, lanes), 1) < HEAD_CHANNELS
    )
    diagonal = places((lanes, lanes), 0) == places((lanes, lanes), 1)
    small_row, small_col = places((size, size), 0), places((size, size), 1)
    running = ((small_row // CHUNK == small_col // CHUNK) & (small_row >= small_col)).astype(F32)
    head_sum = head_block.astype(F32)
    tops, bottoms = slice(0, CHUNK), slice(CHUNK, 2 * CHUNK)

    def stacked(values):
        return jnp.concatenate(
            (jnp.where(first_head, values, 0.0), jnp.where(first_head, 0.0, values)), 0
        )

    def each_chunk(values, at):
        return jnp.concatenate(
            [jnp.broadcast_to(values[c + at : c + at + 1], (CHUNK, lanes)) for c in (0, CHUNK)], 0
        )

    held = []
    for p in range(pairs):
        at = slice(p * lanes, (p + 1) * lanes)
        rec = proj_ref[:, p * lanes : (p + 1) * lanes].astype(F32)
        key = proj_ref[:, cols + p * lanes : cols + (p + 1) * lanes].astype(F32)
        value = proj_ref[:, 2 * cols + p * lanes : 2 * cols + (p + 1) * lanes].astype(F32)
        logged = log_ref[:, at]
        squares = lax.dot_general(
            key * key, head_sum, MM, precision=lax.Precision.HIGHEST, preferred_element_type=F32
        )
        unit = key * lax.rsqrt(squares + 1e-06)
        beta = unit * rate_ref[:, at]
        total = lax.dot_general(
            running, logged, MM, precision=lax.Precision.HIGHEST, preferred_element_type=F32
        )
        middle = each_chunk(total, CHUNK // 2 - 1)
        ending = each_chunk(total, CHUNK - 1)
        previous = total - logged
        fall = jnp.exp(middle - total)
        to_end = jnp.exp(ending - total)
        zeta = -unit
        left = jnp.concatenate(
            (stacked(zeta * jnp.exp(previous - middle)), stacked(rec * jnp.exp(total - middle))), 0
        )
        right = jnp.concatenate((beta * fall, key * fall), 0)
        held.append(
            dict(
                grams=mul(left, right, NT),
                zeta_true=zeta * jnp.exp(previous),
                rec_true=rec * jnp.exp(total),
                beta_end=beta * to_end,
                key_end=key * to_end,
                value=value,
                ending=jnp.exp(total),
            )
        )
    for h in held:
        grams = h.pop("grams")
        blank = jnp.zeros((size, size), F32)

        def spread(first, second, mask):
            both = jnp.concatenate(
                (
                    jnp.concatenate((first, blank), 1),
                    jnp.concatenate((blank, second), 1),
                ),
                0,
            )
            return jnp.where(mask, both, 0.0).astype(BF16)

        h["zb"] = spread(grams[:size, :size], grams[size : 2 * size, :size], strict)
        h["zk"] = spread(grams[:size, size:], grams[size : 2 * size, size:], strict)
        h["rb"] = spread(grams[2 * size : 3 * size, :size], grams[3 * size :, :size], upto)
        h["rk"] = spread(grams[2 * size : 3 * size, size:], grams[3 * size :, size:], upto)
        h["inverse"] = identity + jnp.where(pairs_of_two, h["zb"].astype(F32), 0.0)
        h["from_values"] = mul(
            jnp.concatenate((h["zk"], h["rk"]), 0), stacked(h["value"])
        )
    for merge in merges:
        for h in held:
            inner = mul(jnp.where(merge, h["zb"].astype(F32), 0.0), h["inverse"])
            h["inner"] = inner
        for h in held:
            h["inverse"] = h["inverse"] + mul(h["inverse"], h["inner"])
    for h in held:
        right = jnp.concatenate((stacked(h["zeta_true"]), h["from_values"][: 2 * size]), 1)
        h["pulled"] = mul(h["inverse"], right)
    for p, h in enumerate(held):
        start = jnp.concatenate((stacked(h["rec_true"]), h["from_values"][2 * size :]), 1)
        seen = start + mul(h["rb"], h["pulled"])
        seen = seen[:size] + seen[size:]
        pulled = h["pulled"][:size] + h["pulled"][size:]
        query, ready = seen[:, :lanes], seen[:, lanes:]
        maps = []
        for part, last in ((tops, CHUNK - 1), (bottoms, 2 * CHUNK - 1)):
            moved = mul(pulled[part], h["beta_end"][part], TN)
            added = mul(h["value"][part], h["key_end"][part], TN)
            kept = jnp.where(diagonal, h["ending"][last : last + 1], 0.0)
            maps.append(
                (
                    kept + jnp.where(head_block, moved[:lanes], 0.0),
                    jnp.where(head_block, moved[lanes:] + added, 0.0),
                )
            )
        both = mul(jnp.concatenate(maps[0], 0), maps[1][0])
        carry = both[:lanes]
        offset = both[lanes:] + maps[1][1]
        later = mul(query[bottoms], jnp.concatenate(maps[0], 0), NT)
        query = jnp.concatenate((query[tops], later[:, :lanes]), 0)
        ready = jnp.concatenate((ready[tops], ready[bottoms] + later[:, lanes:]), 0)
        at = slice(p * lanes, (p + 1) * lanes)
        q_ref[:, at] = query.astype(BF16)
        o_ref[:, at] = ready
        half = places((HEAD_CHANNELS, lanes), 1) < HEAD_CHANNELS
        turned_offset = pltpu.roll(offset, HEAD_CHANNELS, 1)
        turned_carry = pltpu.roll(carry, HEAD_CHANNELS, 1)
        maps_ref[2 * p] = jnp.where(
            half, carry[:HEAD_CHANNELS], turned_offset[:HEAD_CHANNELS]
        ).astype(BF16)
        maps_ref[2 * p + 1] = jnp.where(
            half, turned_carry[HEAD_CHANNELS:], offset[HEAD_CHANNELS:]
        ).astype(BF16)


def position_maps(proj, logged, rate, tok_count):
    rows, cols = logged.shape
    seqs = rows // tok_count
    heads = cols // HEAD_CHANNELS
    lanes = 2 * HEAD_CHANNELS
    return pl.pallas_call(
        maps_kernel,
        grid=(seqs,),
        out_shape=(
            jax.ShapeDtypeStruct((rows, cols), BF16),
            jax.ShapeDtypeStruct((rows, cols), F32),
            jax.ShapeDtypeStruct((seqs * heads, HEAD_CHANNELS, lanes), BF16),
        ),
        in_specs=[
            pl.BlockSpec((tok_count, 3 * cols), lambda s: (s, 0)),
            pl.BlockSpec((tok_count, cols), lambda s: (s, 0)),
            pl.BlockSpec((tok_count, cols), lambda s: (s, 0)),
        ],
        out_specs=(
            pl.BlockSpec((tok_count, cols), lambda s: (s, 0)),
            pl.BlockSpec((tok_count, cols), lambda s: (s, 0)),
            pl.BlockSpec((heads, HEAD_CHANNELS, lanes), lambda s: (s, 0, 0)),
        ),
        compiler_params=pltpu.CompilerParams(vmem_limit_bytes=VMEM_BYTES),
        cost_estimate=pl.CostEstimate(
            flops=rows * cols * 2 * 256 * 20,
            bytes_accessed=rows * cols * 20,
            transcendentals=6 * rows * cols,
        ),
        name="position_maps",
    )(proj, logged, rate)


def states_kernel(maps_ref, start_ref, out_ref):
    count = maps_ref.shape[0]
    n = HEAD_CHANNELS
    state = start_ref[...]
    for i in range(count):
        out_ref[i] = jnp.concatenate((state[: n // 2], state[n // 2 :]), 1).astype(BF16)
        if i + 1 < count:
            pair = maps_ref[i]
            high = state.astype(BF16)
            low = (state - high.astype(F32)).astype(BF16)
            moved = mul(jnp.concatenate((high, low), 0), pair[:, :n])
            state = moved[:n] + moved[n:] + pair[:, n:].astype(F32)


def states_ahead(maps, start):
    count = maps.shape[0]
    whole = pl.BlockSpec(memory_space=pltpu.VMEM)
    return pl.pallas_call(
        states_kernel,
        out_shape=jax.ShapeDtypeStruct((count, HEAD_CHANNELS // 2, 2 * HEAD_CHANNELS), BF16),
        in_specs=[whole, whole],
        out_specs=whole,
        cost_estimate=pl.CostEstimate(
            flops=count * 4 * HEAD_CHANNELS**3, bytes_accessed=1 << 19, transcendentals=0
        ),
        name="states_ahead",
    )(maps, start)


def closing_kernel(back_ref, q_ref, o_ref, gain_ref, fox_w_ref, lin_w_ref, out_ref, act_scr):
    n = HEAD_CHANNELS
    lanes = 2 * n
    rows, cols = q_ref.shape
    count, _, tok_count = back_ref.shape
    heads = cols // n
    seqs = rows // tok_count

    @pl.when(pl.program_id(0) == 0)
    def _():
        head_block = (places((lanes, lanes), 0) < n) == (places((lanes, lanes), 1) < n)
        average = jnp.where(head_block, 1.0 / n, 0.0).astype(BF16)
        first = places((n // 2, lanes), 1) < n

        def mean(values):
            high = values.astype(BF16)
            low = (values - high.astype(F32)).astype(BF16)
            return mul(high, average) + mul(low, average)

        for s in range(seqs):
            here = slice(s * tok_count, (s + 1) * tok_count)
            for p in range(heads // 2):
                at = slice(p * lanes, (p + 1) * lanes)
                j = s * heads + 2 * p
                fox = jnp.concatenate((back_ref[j, :n, :], back_ref[j + 1, :n, :]), 0)
                act_scr[here, at] = fox.astype(F32).T.astype(BF16)
                parts = []
                for k in range(2):
                    packed = back_ref[j + k, n:, :].astype(F32)
                    turned = pltpu.roll(packed, n, 1)
                    upper, lower = (packed, turned) if k == 0 else (turned, packed)
                    if k == 0:
                        parts += [jnp.where(first, packed, 0.0), jnp.where(first, turned, 0.0)]
                    else:
                        parts += [jnp.where(first, 0.0, turned), jnp.where(first, 0.0, packed)]
                state = jnp.concatenate(parts, 0)
                raw = mul(q_ref[here, at], state, NT) + o_ref[here, at]
                centred = raw - mean(raw)
                spread = mean(centred * centred)
                lin = centred * lax.rsqrt(spread + 0.00064) * gain_ref[:, at].astype(F32)
                act_scr[here, slice(cols + p * lanes, cols + (p + 1) * lanes)] = lin.astype(BF16)

    out_ref[...] = (
        lax.dot_general(act_scr[:, :cols], fox_w_ref[...], NT, preferred_element_type=F32)
        + lax.dot_general(act_scr[:, cols:], lin_w_ref[...], NT, preferred_element_type=F32)
    ).astype(BF16)


def closing(back, query, ready, gain, fox_w, lin_w):
    rows, cols = query.shape
    width = fox_w.shape[0]
    tile = 512
    whole = pl.BlockSpec(memory_space=pltpu.VMEM)
    return pl.pallas_call(
        closing_kernel,
        grid=(width // tile,),
        out_shape=jax.ShapeDtypeStruct((rows, width), BF16),
        in_specs=[
            whole,
            whole,
            whole,
            whole,
            pl.BlockSpec((tile, cols), lambda i: (i, 0)),
            pl.BlockSpec((tile, cols), lambda i: (i, 0)),
        ],
        out_specs=pl.BlockSpec((rows, tile), lambda i: (0, i)),
        scratch_shapes=[pltpu.VMEM((rows, 2 * cols), BF16)],
        compiler_params=pltpu.CompilerParams(vmem_limit_bytes=VMEM_BYTES),
        cost_estimate=pl.CostEstimate(
            flops=4 * rows * cols * width,
            bytes_accessed=4 * cols * width + 2 * rows * width,
            transcendentals=0,
        ),
        name="closing",
    )(back, query, ready, gain, fox_w, lin_w)


def gathered(arrays, axis):
    return lax.all_gather(jnp.concatenate(arrays, axis=1), axis, axis=0, tiled=True)


def per_device(
    inputs,
    input_norm_gain,
    softmax_query_matrix,
    softmax_key_matrix,
    softmax_value_matrix,
    running_forget_gate,
    receptance_weight,
    linear_key_weight,
    linear_value_weight,
    decay_lower_map,
    decay_upper_map,
    decay_offset_base,
    decay_extra_log,
    rate_lower_map,
    rate_upper_map,
    rate_offset_base,
    linear_head_gain,
    starting_state,
    softmax_output_weight,
    linear_output_weight,
):
    n = HEAD_CHANNELS
    seq_count, tok_count, half_width = inputs.shape
    rows = seq_count * tok_count
    cols = softmax_query_matrix.shape[1]
    heads = cols // n
    place = lax.axis_index("sp")
    col_start = lax.axis_index("tp") * cols

    fox_w = gathered((softmax_query_matrix, softmax_key_matrix, softmax_value_matrix), "fs")
    lin_w = gathered((receptance_weight, linear_key_weight, linear_value_weight), "fs")

    flat = inputs.reshape(rows, half_width)
    tp = lax.axis_size("tp")
    both = lax.all_to_all(
        jnp.broadcast_to(flat, (tp, rows, half_width)), "tp", 0, 0, tiled=True
    )
    whole = jnp.moveaxis(both, 0, 1).reshape(rows, tp * half_width).astype(F32)
    scaling = lax.rsqrt(jnp.mean(whole * whole, axis=-1, keepdims=True) + 1e-06)
    normed = (whole * scaling * input_norm_gain.astype(F32)).astype(BF16)

    def project(weight):
        return jnp.dot(normed, weight, preferred_element_type=F32)

    def own_columns(table, axis):
        return lax.dynamic_slice_in_dim(table, col_start, cols, axis)

    decay_low = jnp.tanh(project(decay_lower_map)).astype(BF16)
    decay_preact = own_columns(decay_offset_base, 0) + jnp.dot(
        decay_low, own_columns(decay_upper_map, 1), preferred_element_type=F32
    )
    extra = jnp.repeat(decay_extra_log.reshape(rows, heads), n, axis=1)
    decay_logged = -jnp.exp(-jax.nn.softplus(-decay_preact) - 0.5) + extra
    rate_low = project(rate_lower_map).astype(BF16)
    rate = jax.nn.sigmoid(
        own_columns(rate_offset_base, 0)
        + jnp.dot(rate_low, own_columns(rate_upper_map, 1), preferred_element_type=F32)
    )
    gate_rows = running_forget_gate.transpose(0, 2, 1).reshape(seq_count * heads, 1, -1)
    gate = lax.dynamic_index_in_dim(gate_rows, place, 0, False)
    start = lax.dynamic_index_in_dim(
        starting_state.reshape(seq_count * heads, n, n), place, 0, False
    )

    fox = lax.dot_general(
        fox_w, normed, (((0,), (1,)), ((), ())), preferred_element_type=F32
    ).astype(BF16)
    fox = fox.reshape(3, heads, n, seq_count, tok_count).transpose(3, 1, 0, 2, 4)
    fox = fox.reshape(seq_count * heads, 3 * n, tok_count)
    fox = lax.all_to_all(fox, "sp", 0, 0, tiled=True)
    fox_out = attention(fox, gate)

    lin = project(lin_w).astype(BF16)
    query, ready, maps = position_maps(lin, decay_logged, rate, tok_count)
    maps = lax.all_to_all(maps, "sp", 0, 0, tiled=True)
    states = states_ahead(maps, start)
    back = lax.all_to_all(jnp.concatenate((fox_out, states), 1), "sp", 0, 0, tiled=True)
    gain = own_columns(linear_head_gain, 0).reshape(1, cols)
    partial = closing(back, query, ready, gain, softmax_output_weight, linear_output_weight)
    pieces = lax.all_to_all(
        partial.reshape(seq_count, tok_count, -1), "tp", 0, 0, tiled=True
    )
    mixed = jnp.sum(
        pieces.reshape(tp, seq_count // tp, tok_count, -1).astype(F32), axis=0
    )
    return mixed.astype(BF16)


def solution(mesh):
    placed = (
        P(("grp", "fs"), "sp", "tp"),
        P(),
        P("fs", "tp"),
        P("fs", "tp"),
        P("fs", "tp"),
        P(("grp", "fs"), None, "tp"),
        P("fs", "tp"),
        P("fs", "tp"),
        P("fs", "tp"),
        P(),
        P(),
        P(),
        P(("grp", "fs"), "sp", "tp"),
        P(),
        P(),
        P(),
        P(),
        P(("grp", "fs"), "tp", None, None),
        P(None, "tp"),
        P(None, "tp"),
    )
    return jax.shard_map(
        per_device,
        mesh=mesh,
        in_specs=placed,
        out_specs=P(("grp", "fs", "tp"), "sp", None),
        check_vma=False,
    )
```

```python
import functools

import jax
import jax.numpy as jnp
from jax import lax
from jax.experimental import pallas as pl
from jax.experimental.pallas import tpu as pltpu
from jax.sharding import PartitionSpec as P

HEAD_CHANNELS = 64
CHUNK = 64
F32 = jnp.float32
BF16 = jnp.bfloat16
VMEM_BYTES = 56 * 1024 * 1024

MM = (((1,), (0,)), ((), ()))
NT = (((1,), (1,)), ((), ()))
TN = (((0,), (0,)), ((), ()))


def mul(left, right, dims=MM):
    return lax.dot_general(
        left.astype(BF16), right.astype(BF16), dims, preferred_element_type=F32
    )


def places(shape, dim):
    return lax.broadcasted_iota(jnp.int32, shape, dim)


def attention_kernel(blocks_ref, gate_ref, out_ref, key_scr, value_scr):
    count, _, width = blocks_ref.shape
    channels = HEAD_CHANNELS
    for i in range(count):
        gate = gate_ref[i : i + 1, :]
        high = gate.astype(BF16).astype(F32)
        rest = gate - high
        middle = rest.astype(BF16).astype(F32)
        low = rest - middle
        row = places((channels, width), 0)
        extra = jnp.where(row == 0, high, jnp.where(row == 1, middle, jnp.where(row == 2, low, 0.0)))
        key_rows = blocks_ref[i, channels : 2 * channels, :].astype(F32)
        key_scr[i * width : (i + 1) * width, :] = jnp.concatenate((key_rows, extra), 0).T.astype(BF16)
        value_scr[:, i * width : (i + 1) * width] = blocks_ref[i, 2 * channels :, :]
    step = 2 * width
    row = places((channels, step), 0)
    tail = jnp.where(row < 3, -1.0, 0.0).astype(BF16)
    live = places((step, step), 0) <= places((step, step), 1)
    for i in range(count // 2):
        query = jnp.concatenate(
            (blocks_ref[2 * i, :channels, :], blocks_ref[2 * i + 1, :channels, :]), 1
        )
        query = (query.astype(F32) * channels ** (-0.5)).astype(BF16)
        query = jnp.concatenate((query, tail), 0)
        before = i * step
        own = lax.dot_general(
            key_scr[before : before + step, :], query, MM, preferred_element_type=F32
        )
        own = jnp.where(live, own, -1e30)
        top = jnp.max(own, axis=0, keepdims=True)
        if before:
            past = lax.dot_general(key_scr[:before, :], query, MM, preferred_element_type=F32)
            top = jnp.maximum(top, jnp.max(past, axis=0, keepdims=True))
        weight = jnp.exp(own - top)
        total = jnp.sum(weight, axis=0, keepdims=True)
        mixed = lax.dot_general(
            value_scr[:, before : before + step],
            weight.astype(BF16),
            MM,
            preferred_element_type=F32,
        )
        if before:
            weight = jnp.exp(past - top)
            total = total + jnp.sum(weight, axis=0, keepdims=True)
            mixed = mixed + lax.dot_general(
                value_scr[:, :before], weight.astype(BF16), MM, preferred_element_type=F32
            )
        mixed = (mixed / total).astype(BF16)
        out_ref[2 * i] = mixed[:, :width]
        out_ref[2 * i + 1] = mixed[:, width:]


def attention(blocks, gate):
    count, rows, width = blocks.shape
    whole = pl.BlockSpec(memory_space=pltpu.VMEM)
    return pl.pallas_call(
        attention_kernel,
        out_shape=jax.ShapeDtypeStruct((count, HEAD_CHANNELS, width), BF16),
        in_specs=[whole, whole],
        out_specs=whole,
        scratch_shapes=[
            pltpu.VMEM((count * width, 2 * HEAD_CHANNELS), BF16),
            pltpu.VMEM((HEAD_CHANNELS, count * width), BF16),
        ],
        compiler_params=pltpu.CompilerParams(vmem_limit_bytes=VMEM_BYTES),
        cost_estimate=pl.CostEstimate(
            flops=4 * HEAD_CHANNELS * (count * width) ** 2,
            bytes_accessed=4 * count * rows * width,
            transcendentals=(count * width) ** 2 // 2,
        ),
        name="attention",
    )(blocks, gate)


def chunk_masks(size):
    row, col = places((2 * size, 2 * size), 0), places((2 * size, 2 * size), 1)
    same = row // CHUNK == col // CHUNK
    return row, col, same


def maps_kernel(proj_ref, log_ref, rate_ref, extra_ref, q_ref, o_ref, maps_ref):
    seqs, _, size = extra_ref.shape
    lanes = 2 * HEAD_CHANNELS
    row, col, same = chunk_masks(size)
    strict = same & (row > col)
    upto = same & (row >= col)
    merges = []
    block = 2
    while block < CHUNK:
        merges.append((row // (2 * block) == col // (2 * block)) & (row // block > col // block))
        block *= 2
    pairs_of_two = (row // 2 == col // 2) & (row > col)
    identity = (row == col).astype(F32)
    lane = places((size, lanes), 1)
    first_head = lane < HEAD_CHANNELS
    head_block = (places((lanes, lanes), 0) < HEAD_CHANNELS) == (
        places((lanes, lanes), 1) < HEAD_CHANNELS
    )
    diagonal = places((lanes, lanes), 0) == places((lanes, lanes), 1)
    small_row, small_col = places((size, size), 0), places((size, size), 1)
    running = ((small_row // CHUNK == small_col // CHUNK) & (small_row >= small_col)).astype(F32)
    head_sum = head_block.astype(F32)
    tops, bottoms = slice(0, CHUNK), slice(CHUNK, 2 * CHUNK)

    def stacked(values):
        return jnp.concatenate(
            (jnp.where(first_head, values, 0.0), jnp.where(first_head, 0.0, values)), 0
        )

    def each_chunk(values, at):
        return jnp.concatenate(
            [jnp.broadcast_to(values[c + at : c + at + 1], (CHUNK, lanes)) for c in (0, CHUNK)], 0
        )

    held = []
    for p in range(seqs):
        at = slice(p * size, (p + 1) * size)
        rec = proj_ref[at, :lanes].astype(F32)
        key = proj_ref[at, lanes : 2 * lanes].astype(F32)
        value = proj_ref[at, 2 * lanes :].astype(F32)
        by_head = [
            jnp.broadcast_to(extra_ref[p, k : k + 1, :], (HEAD_CHANNELS, size)) for k in range(2)
        ]
        logged = log_ref[at, :] + jnp.concatenate(by_head, 0).T
        squares = lax.dot_general(
            key * key, head_sum, MM, precision=lax.Precision.HIGHEST, preferred_element_type=F32
        )
        unit = key * lax.rsqrt(squares + 1e-06)
        beta = unit * rate_ref[at, :]
        total = lax.dot_general(
            running, logged, MM, precision=lax.Precision.HIGHEST, preferred_element_type=F32
        )
        middle = each_chunk(total, CHUNK // 2 - 1)
        ending = each_chunk(total, CHUNK - 1)
        previous = total - logged
        fall = jnp.exp(middle - total)
        to_end = jnp.exp(ending - total)
        zeta = -unit
        left = jnp.concatenate(
            (stacked(zeta * jnp.exp(previous - middle)), stacked(rec * jnp.exp(total - middle))), 0
        )
        right = jnp.concatenate((beta * fall, key * fall), 0)
        held.append(
            dict(
                grams=mul(left, right, NT),
                zeta_true=zeta * jnp.exp(previous),
                rec_true=rec * jnp.exp(total),
                beta_end=beta * to_end,
                key_end=key * to_end,
                value=value,
                ending=jnp.exp(total),
            )
        )
    for h in held:
        grams = h.pop("grams")
        blank = jnp.zeros((size, size), F32)

        def spread(first, second, mask):
            both = jnp.concatenate(
                (
                    jnp.concatenate((first, blank), 1),
                    jnp.concatenate((blank, second), 1),
                ),
                0,
            )
            return jnp.where(mask, both, 0.0).astype(BF16)

        h["zb"] = spread(grams[:size, :size], grams[size : 2 * size, :size], strict)
        h["zk"] = spread(grams[:size, size:], grams[size : 2 * size, size:], strict)
        h["rb"] = spread(grams[2 * size : 3 * size, :size], grams[3 * size :, :size], upto)
        h["rk"] = spread(grams[2 * size : 3 * size, size:], grams[3 * size :, size:], upto)
        h["inverse"] = identity + jnp.where(pairs_of_two, h["zb"].astype(F32), 0.0)
        h["from_values"] = mul(
            jnp.concatenate((h["zk"], h["rk"]), 0), stacked(h["value"])
        )
    for merge in merges:
        for h in held:
            inner = mul(jnp.where(merge, h["zb"].astype(F32), 0.0), h["inverse"])
            h["inner"] = inner
        for h in held:
            h["inverse"] = h["inverse"] + mul(h["inverse"], h["inner"])
    for h in held:
        right = jnp.concatenate((stacked(h["zeta_true"]), h["from_values"][: 2 * size]), 1)
        h["pulled"] = mul(h["inverse"], right)
    for p, h in enumerate(held):
        start = jnp.concatenate((stacked(h["rec_true"]), h["from_values"][2 * size :]), 1)
        seen = start + mul(h["rb"], h["pulled"])
        seen = seen[:size] + seen[size:]
        pulled = h["pulled"][:size] + h["pulled"][size:]
        query, ready = seen[:, :lanes], seen[:, lanes:]
        maps = []
        for part, last in ((tops, CHUNK - 1), (bottoms, 2 * CHUNK - 1)):
            moved = mul(pulled[part], h["beta_end"][part], TN)
            added = mul(h["value"][part], h["key_end"][part], TN)
            kept = jnp.where(diagonal, h["ending"][last : last + 1], 0.0)
            maps.append(
                (
                    kept + jnp.where(head_block, moved[:lanes], 0.0),
                    jnp.where(head_block, moved[lanes:] + added, 0.0),
                )
            )
        both = mul(jnp.concatenate(maps[0], 0), maps[1][0])
        carry = both[:lanes]
        offset = both[lanes:] + maps[1][1]
        later = mul(query[bottoms], jnp.concatenate(maps[0], 0), NT)
        query = jnp.concatenate((query[tops], later[:, :lanes]), 0)
        ready = jnp.concatenate((ready[tops], ready[bottoms] + later[:, lanes:]), 0)
        at = slice(p * size, (p + 1) * size)
        q_ref[at, :] = query.astype(BF16)
        o_ref[at, :] = ready
        half = places((HEAD_CHANNELS, lanes), 1) < HEAD_CHANNELS
        turned_offset = pltpu.roll(offset, HEAD_CHANNELS, 1)
        turned_carry = pltpu.roll(carry, HEAD_CHANNELS, 1)
        maps_ref[2 * p] = jnp.where(
            half, carry[:HEAD_CHANNELS], turned_offset[:HEAD_CHANNELS]
        ).astype(BF16)
        maps_ref[2 * p + 1] = jnp.where(
            half, turned_carry[HEAD_CHANNELS:], offset[HEAD_CHANNELS:]
        ).astype(BF16)


def position_maps(proj, logged, rate, extra):
    seqs, heads, tok_count = extra.shape
    rows, lanes = logged.shape
    group = seqs // 2
    return pl.pallas_call(
        maps_kernel,
        grid=(seqs // group,),
        out_shape=(
            jax.ShapeDtypeStruct((rows, lanes), BF16),
            jax.ShapeDtypeStruct((rows, lanes), F32),
            jax.ShapeDtypeStruct((seqs * heads, HEAD_CHANNELS, lanes), BF16),
        ),
        in_specs=[
            pl.BlockSpec((group * tok_count, 3 * lanes), lambda s: (s, 0)),
            pl.BlockSpec((group * tok_count, lanes), lambda s: (s, 0)),
            pl.BlockSpec((group * tok_count, lanes), lambda s: (s, 0)),
            pl.BlockSpec((group, heads, tok_count), lambda s: (s, 0, 0)),
        ],
        out_specs=(
            pl.BlockSpec((group * tok_count, lanes), lambda s: (s, 0)),
            pl.BlockSpec((group * tok_count, lanes), lambda s: (s, 0)),
            pl.BlockSpec((group * heads, HEAD_CHANNELS, lanes), lambda s: (s, 0, 0)),
        ),
        compiler_params=pltpu.CompilerParams(vmem_limit_bytes=VMEM_BYTES),
        cost_estimate=pl.CostEstimate(
            flops=rows * lanes * 2 * 256 * 20,
            bytes_accessed=rows * lanes * 20,
            transcendentals=6 * rows * lanes,
        ),
        name="position_maps",
    )(proj, logged, rate, extra)


def states_kernel(maps_ref, start_ref, out_ref):
    count = maps_ref.shape[0]
    n = HEAD_CHANNELS
    state = jnp.concatenate((start_ref[:, :n], start_ref[:, n:]), 0)
    for i in range(count):
        out_ref[i] = jnp.concatenate((state[: n // 2], state[n // 2 :]), 1).astype(BF16)
        if i + 1 < count:
            pair = maps_ref[i]
            high = state.astype(BF16)
            low = (state - high.astype(F32)).astype(BF16)
            moved = mul(jnp.concatenate((high, low), 0), pair[:, :n])
            state = moved[:n] + moved[n:] + pair[:, n:].astype(F32)


def states_ahead(maps, start):
    count = maps.shape[0]
    whole = pl.BlockSpec(memory_space=pltpu.VMEM)
    return pl.pallas_call(
        states_kernel,
        out_shape=jax.ShapeDtypeStruct((count, HEAD_CHANNELS // 2, 2 * HEAD_CHANNELS), BF16),
        in_specs=[whole, whole],
        out_specs=whole,
        cost_estimate=pl.CostEstimate(
            flops=count * 4 * HEAD_CHANNELS**3, bytes_accessed=1 << 19, transcendentals=0
        ),
        name="states_ahead",
    )(maps, start)


def project_kernel(
    both_ref,
    gain_ref,
    fox_w_ref,
    lin_w_ref,
    decay_low_ref,
    rate_low_ref,
    decay_up_ref,
    rate_up_ref,
    decay_base_ref,
    rate_base_ref,
    fox_ref,
    lin_ref,
    log_ref,
    rate_ref,
):
    n = HEAD_CHANNELS
    parts, rows, width = both_ref.shape
    pairs, _, tok_count = fox_ref.shape
    heads = pairs * tok_count // rows
    lanes = heads * n
    pieces = [both_ref[i].astype(F32) for i in range(parts)]
    square = sum(jnp.sum(x * x, axis=1, keepdims=True) for x in pieces)
    scaling = lax.rsqrt(square / (parts * width) + 1e-06)
    normed = jnp.concatenate(
        [
            (x * scaling * gain_ref[:, i * width : (i + 1) * width].astype(F32)).astype(BF16)
            for i, x in enumerate(pieces)
        ],
        1,
    )

    def project(weight_ref):
        return lax.dot_general(normed, weight_ref[...], MM, preferred_element_type=F32)

    fox = project(fox_w_ref)
    for s in range(rows // tok_count):
        here = slice(s * tok_count, (s + 1) * tok_count)
        for k in range(3):
            turned = fox[here, k * lanes : (k + 1) * lanes].T.astype(BF16)
            for h in range(heads):
                fox_ref[s * heads + h, k * n : (k + 1) * n, :] = turned[h * n : (h + 1) * n]
    lin_ref[...] = project(lin_w_ref).astype(BF16)
    decay_low = jnp.tanh(project(decay_low_ref))
    decay = mul(decay_low, decay_up_ref[...]) + decay_base_ref[...]
    log_ref[...] = jax.nn.sigmoid(decay) * -(2.718281828459045**-0.5)
    rate = mul(project(rate_low_ref), rate_up_ref[...]) + rate_base_ref[...]
    rate_ref[...] = jax.nn.sigmoid(rate)


def projections(both, gain, fox_w, lin_w, lows, ups, bases, tok_count):
    parts, rows, width = both.shape
    lanes = fox_w.shape[1] // 3
    heads = lanes // HEAD_CHANNELS
    seqs = rows // tok_count
    group = 2
    whole = pl.BlockSpec(memory_space=pltpu.VMEM)
    tall = group * tok_count
    return pl.pallas_call(
        project_kernel,
        grid=(seqs // group,),
        out_shape=(
            jax.ShapeDtypeStruct((seqs * heads, 3 * HEAD_CHANNELS, tok_count), BF16),
            jax.ShapeDtypeStruct((rows, 3 * lanes), BF16),
            jax.ShapeDtypeStruct((rows, lanes), F32),
            jax.ShapeDtypeStruct((rows, lanes), F32),
        ),
        in_specs=[pl.BlockSpec((parts, tall, width), lambda s: (0, s, 0))] + [whole] * 9,
        out_specs=(
            pl.BlockSpec((group * heads, 3 * HEAD_CHANNELS, tok_count), lambda s: (s, 0, 0)),
            pl.BlockSpec((tall, 3 * lanes), lambda s: (s, 0)),
            pl.BlockSpec((tall, lanes), lambda s: (s, 0)),
            pl.BlockSpec((tall, lanes), lambda s: (s, 0)),
        ),
        compiler_params=pltpu.CompilerParams(vmem_limit_bytes=VMEM_BYTES),
        cost_estimate=pl.CostEstimate(
            flops=16 * rows * parts * width * lanes,
            bytes_accessed=2 * (rows + 8 * lanes) * parts * width,
            transcendentals=3 * rows * lanes,
        ),
        name="projections",
    )(both, gain, fox_w, lin_w, *lows, *ups, *bases)


def heads_kernel(back_ref, q_ref, o_ref, gain_ref, out_ref):
    n = HEAD_CHANNELS
    lanes = 2 * n
    pairs, _, tok_count = back_ref.shape
    groups, rows, _ = out_ref.shape
    head_block = (places((lanes, lanes), 0) < n) == (places((lanes, lanes), 1) < n)
    average = jnp.where(head_block, 1.0 / n, 0.0).astype(BF16)
    first = places((n // 2, lanes), 1) < n
    gain = gain_ref[...].astype(F32)

    def mean(values):
        high = values.astype(BF16)
        low = (values - high.astype(F32)).astype(BF16)
        return mul(high, average) + mul(low, average)

    raws = []
    for s in range(pairs // 2):
        here = slice(s * tok_count, (s + 1) * tok_count)
        group, at = s * tok_count // rows, s * tok_count % rows
        fox = jnp.concatenate((back_ref[2 * s, :n, :], back_ref[2 * s + 1, :n, :]), 0)
        out_ref[group, at : at + tok_count, :lanes] = fox.astype(F32).T.astype(BF16)
        packed = [back_ref[2 * s + k, n:, :].astype(F32) for k in range(2)]
        turned = [pltpu.roll(x, n, 1) for x in packed]
        state = jnp.concatenate(
            (
                jnp.where(first, packed[0], 0.0),
                jnp.where(first, turned[0], 0.0),
                jnp.where(first, 0.0, turned[1]),
                jnp.where(first, 0.0, packed[1]),
            ),
            0,
        )
        raws.append(mul(q_ref[here, :], state, NT) + o_ref[here, :])
    centred = [raw - mean(raw) for raw in raws]
    spreads = [mean(x * x) for x in centred]
    for s, (x, spread) in enumerate(zip(centred, spreads)):
        group, at = s * tok_count // rows, s * tok_count % rows
        lin = x * lax.rsqrt(spread + 0.00064) * gain
        out_ref[group, at : at + tok_count, lanes:] = lin.astype(BF16)


def heads_out(back, query, ready, gain, groups):
    rows, lanes = query.shape
    whole = pl.BlockSpec(memory_space=pltpu.VMEM)
    return pl.pallas_call(
        heads_kernel,
        out_shape=jax.ShapeDtypeStruct((groups, rows // groups, 2 * lanes), BF16),
        in_specs=[whole] * 4,
        out_specs=whole,
        compiler_params=pltpu.CompilerParams(vmem_limit_bytes=VMEM_BYTES),
        cost_estimate=pl.CostEstimate(
            flops=10 * rows * lanes * lanes, bytes_accessed=12 * rows * lanes, transcendentals=0
        ),
        name="heads_out",
    )(back, query, ready, gain)


def closing_kernel(acts_ref, fox_w_ref, lin_w_ref, out_ref, act_scr):
    groups, rows, both = acts_ref.shape
    lanes = both // 2
    cols = groups * lanes

    @pl.when(pl.program_id(0) == 0)
    def _():
        for g in range(groups):
            act_scr[:, g * lanes : (g + 1) * lanes] = acts_ref[g, :, :lanes]
            act_scr[:, cols + g * lanes : cols + (g + 1) * lanes] = acts_ref[g, :, lanes:]

    out_ref[...] = (
        lax.dot_general(act_scr[:, :cols], fox_w_ref[...], NT, preferred_element_type=F32)
        + lax.dot_general(act_scr[:, cols:], lin_w_ref[...], NT, preferred_element_type=F32)
    ).astype(BF16)


def closing(acts, fox_w, lin_w):
    groups, rows, both = acts.shape
    width, cols = fox_w.shape
    tile = 512
    return pl.pallas_call(
        closing_kernel,
        grid=(width // tile,),
        out_shape=jax.ShapeDtypeStruct((rows, width), BF16),
        in_specs=[
            pl.BlockSpec(memory_space=pltpu.VMEM),
            pl.BlockSpec((tile, cols), lambda i: (i, 0)),
            pl.BlockSpec((tile, cols), lambda i: (i, 0)),
        ],
        out_specs=pl.BlockSpec((rows, tile), lambda i: (0, i)),
        scratch_shapes=[pltpu.VMEM((rows, 2 * cols), BF16)],
        compiler_params=pltpu.CompilerParams(vmem_limit_bytes=VMEM_BYTES),
        cost_estimate=pl.CostEstimate(
            flops=4 * rows * cols * width,
            bytes_accessed=4 * cols * width + 2 * rows * width,
            transcendentals=0,
        ),
        name="closing",
    )(acts, fox_w, lin_w)


def exchange(x, axis):
    return lax.all_to_all(x, axis, 0, 0, tiled=True)


def from_everyone(x, axis):
    return exchange(jnp.broadcast_to(x, (lax.axis_size(axis), *x.shape)), axis)


def own_weights(arrays, axis):
    groups = lax.axis_size(axis)
    rows, cols = arrays[0].shape
    lanes = cols // groups
    sent = jnp.stack(
        [
            jnp.concatenate([a[:, g * lanes : (g + 1) * lanes] for a in arrays], 1)
            for g in range(groups)
        ]
    )
    return exchange(sent, axis).reshape(groups * rows, len(arrays) * lanes)


def per_device(
    inputs,
    input_norm_gain,
    softmax_query_matrix,
    softmax_key_matrix,
    softmax_value_matrix,
    running_forget_gate,
    receptance_weight,
    linear_key_weight,
    linear_value_weight,
    decay_lower_map,
    decay_upper_map,
    decay_offset_base,
    decay_extra_log,
    rate_lower_map,
    rate_upper_map,
    rate_offset_base,
    linear_head_gain,
    starting_state,
    softmax_output_weight,
    linear_output_weight,
):
    n = HEAD_CHANNELS
    seq_count, tok_count, half_width = inputs.shape
    rows = seq_count * tok_count
    cols = softmax_query_matrix.shape[1]
    groups, tp = lax.axis_size("fs"), lax.axis_size("tp")
    lanes = cols // groups
    heads = lanes // n
    seqs = groups * seq_count
    length = running_forget_gate.shape[1]
    place = lax.axis_index("sp")
    col_start = lax.axis_index("tp") * cols + lax.axis_index("fs") * lanes

    mine = from_everyone(inputs.reshape(rows, half_width), "fs")
    fox_w = own_weights((softmax_query_matrix, softmax_key_matrix, softmax_value_matrix), "fs")
    lin_w = own_weights((receptance_weight, linear_key_weight, linear_value_weight), "fs")

    pair_seq, pair_head = place // heads, lax.rem(place, heads)
    pair_group, pair_slot = pair_seq // seq_count, lax.rem(pair_seq, seq_count)

    def of_pair(table, head_dim):
        table = lax.dynamic_index_in_dim(table, pair_slot, 0, False)
        shape = table.shape
        table = table.reshape(*shape[:head_dim], groups, heads, *shape[head_dim + 1 :])
        return lax.dynamic_index_in_dim(table, pair_head, head_dim + 1, False)

    state = of_pair(starting_state, 0)
    state = jnp.concatenate((state[:, : n // 2], state[:, n // 2 :]), 2)
    gates = of_pair(running_forget_gate, 1).T.reshape(groups, length // tok_count, tok_count)
    extra = decay_extra_log.reshape(seq_count, tok_count, groups, heads).transpose(2, 0, 3, 1)
    extra = extra.reshape(groups, seq_count * heads, tok_count)
    small = exchange(jnp.concatenate((state, gates, extra), 1), "fs")
    half, after = n // 2, n // 2 + length // tok_count
    extra = small[:, after:].reshape(seqs, heads, tok_count)
    pair = lax.dynamic_index_in_dim(small, pair_group, 0, False)
    start, gate = pair[:half], pair[half:after]

    def own_columns(table, axis):
        return lax.dynamic_slice_in_dim(table, col_start, lanes, axis)

    both = from_everyone(mine.reshape(seqs * tok_count, half_width), "tp")
    fox, lin, logged, rate = projections(
        both,
        input_norm_gain.reshape(1, -1),
        fox_w,
        lin_w,
        (decay_lower_map, rate_lower_map),
        (own_columns(decay_upper_map, 1), own_columns(rate_upper_map, 1)),
        (
            own_columns(decay_offset_base, 0).reshape(1, lanes),
            own_columns(rate_offset_base, 0).reshape(1, lanes),
        ),
        tok_count,
    )
    fox = exchange(fox, "sp")
    query, ready, maps = position_maps(lin, logged, rate, extra)
    maps = exchange(maps, "sp")
    fox_out = attention(fox, gate)
    states = states_ahead(maps, start)
    back = exchange(jnp.concatenate((fox_out, states), 1), "sp")
    gain = own_columns(linear_head_gain, 0).reshape(1, lanes)
    acts = exchange(heads_out(back, query, ready, gain, groups), "fs")
    partial = closing(acts, softmax_output_weight, linear_output_weight)
    pieces = exchange(partial.reshape(seq_count, tok_count, -1), "tp")
    mixed = jnp.sum(
        pieces.reshape(tp, seq_count // tp, tok_count, -1).astype(F32), axis=0
    )
    return mixed.astype(BF16)


def solution(mesh):
    placed = (
        P(("grp", "fs"), "sp", "tp"),
        P(),
        P("fs", "tp"),
        P("fs", "tp"),
        P("fs", "tp"),
        P(("grp", "fs"), None, "tp"),
        P("fs", "tp"),
        P("fs", "tp"),
        P("fs", "tp"),
        P(),
        P(),
        P(),
        P(("grp", "fs"), "sp", "tp"),
        P(),
        P(),
        P(),
        P(),
        P(("grp", "fs"), "tp", None, None),
        P(None, "tp"),
        P(None, "tp"),
    )
    return jax.shard_map(
        per_device,
        mesh=mesh,
        in_specs=placed,
        out_specs=P(("grp", "fs", "tp"), "sp", None),
        check_vma=False,
    )
```

```python
import functools

import jax
import jax.numpy as jnp
from jax import lax
from jax.experimental import pallas as pl
from jax.experimental.pallas import tpu as pltpu
from jax.sharding import PartitionSpec as P

HEAD_CHANNELS = 64
CHUNK = 64
F32 = jnp.float32
BF16 = jnp.bfloat16
VMEM_BYTES = 56 * 1024 * 1024

MM = (((1,), (0,)), ((), ()))
NT = (((1,), (1,)), ((), ()))
TN = (((0,), (0,)), ((), ()))


def mul(left, right, dims=MM):
    return lax.dot_general(
        left.astype(BF16), right.astype(BF16), dims, preferred_element_type=F32
    )


def places(shape, dim):
    return lax.broadcasted_iota(jnp.int32, shape, dim)


def attention_kernel(blocks_ref, gate_ref, out_ref, key_scr, value_scr):
    count, _, width = blocks_ref.shape
    channels = HEAD_CHANNELS
    for i in range(count):
        gate = gate_ref[i : i + 1, :]
        high = gate.astype(BF16).astype(F32)
        rest = gate - high
        middle = rest.astype(BF16).astype(F32)
        low = rest - middle
        row = places((channels, width), 0)
        extra = jnp.where(row == 0, high, jnp.where(row == 1, middle, jnp.where(row == 2, low, 0.0)))
        key_rows = blocks_ref[i, channels : 2 * channels, :].astype(F32)
        key_scr[i * width : (i + 1) * width, :] = jnp.concatenate((key_rows, extra), 0).T.astype(BF16)
        value_scr[:, i * width : (i + 1) * width] = blocks_ref[i, 2 * channels :, :]
    step = 2 * width
    row = places((channels, step), 0)
    tail = jnp.where(row < 3, -1.0, 0.0).astype(BF16)
    live = places((step, step), 0) <= places((step, step), 1)
    for i in range(count // 2):
        query = jnp.concatenate(
            (blocks_ref[2 * i, :channels, :], blocks_ref[2 * i + 1, :channels, :]), 1
        )
        query = (query.astype(F32) * channels ** (-0.5)).astype(BF16)
        query = jnp.concatenate((query, tail), 0)
        before = i * step
        own = lax.dot_general(
            key_scr[before : before + step, :], query, MM, preferred_element_type=F32
        )
        own = jnp.where(live, own, -1e30)
        top = jnp.max(own, axis=0, keepdims=True)
        if before:
            past = lax.dot_general(key_scr[:before, :], query, MM, preferred_element_type=F32)
            top = jnp.maximum(top, jnp.max(past, axis=0, keepdims=True))
        weight = jnp.exp(own - top)
        total = jnp.sum(weight, axis=0, keepdims=True)
        mixed = lax.dot_general(
            value_scr[:, before : before + step],
            weight.astype(BF16),
            MM,
            preferred_element_type=F32,
        )
        if before:
            weight = jnp.exp(past - top)
            total = total + jnp.sum(weight, axis=0, keepdims=True)
            mixed = mixed + lax.dot_general(
                value_scr[:, :before], weight.astype(BF16), MM, preferred_element_type=F32
            )
        mixed = (mixed / total).astype(BF16)
        out_ref[2 * i] = mixed[:, :width]
        out_ref[2 * i + 1] = mixed[:, width:]


def attention(blocks, gate):
    count, rows, width = blocks.shape
    whole = pl.BlockSpec(memory_space=pltpu.VMEM)
    return pl.pallas_call(
        attention_kernel,
        out_shape=jax.ShapeDtypeStruct((count, HEAD_CHANNELS, width), BF16),
        in_specs=[whole, whole],
        out_specs=whole,
        scratch_shapes=[
            pltpu.VMEM((count * width, 2 * HEAD_CHANNELS), BF16),
            pltpu.VMEM((HEAD_CHANNELS, count * width), BF16),
        ],
        compiler_params=pltpu.CompilerParams(vmem_limit_bytes=VMEM_BYTES),
        cost_estimate=pl.CostEstimate(
            flops=4 * HEAD_CHANNELS * (count * width) ** 2,
            bytes_accessed=4 * count * rows * width,
            transcendentals=(count * width) ** 2 // 2,
        ),
        name="attention",
    )(blocks, gate)


def chunk_masks(size):
    row, col = places((2 * size, 2 * size), 0), places((2 * size, 2 * size), 1)
    same = row // CHUNK == col // CHUNK
    return row, col, same


def maps_kernel(proj_ref, log_ref, rate_ref, extra_ref, q_ref, o_ref, maps_ref):
    seqs, _, size = extra_ref.shape
    lanes = 2 * HEAD_CHANNELS
    row, col, same = chunk_masks(size)
    strict = same & (row > col)
    upto = same & (row >= col)
    merges = []
    block = 2
    while block < CHUNK:
        merges.append((row // (2 * block) == col // (2 * block)) & (row // block > col // block))
        block *= 2
    pairs_of_two = (row // 2 == col // 2) & (row > col)
    identity = (row == col).astype(F32)
    lane = places((size, lanes), 1)
    first_head = lane < HEAD_CHANNELS
    head_block = (places((lanes, lanes), 0) < HEAD_CHANNELS) == (
        places((lanes, lanes), 1) < HEAD_CHANNELS
    )
    diagonal = places((lanes, lanes), 0) == places((lanes, lanes), 1)
    small_row, small_col = places((size, size), 0), places((size, size), 1)
    running = ((small_row // CHUNK == small_col // CHUNK) & (small_row >= small_col)).astype(F32)
    head_sum = head_block.astype(F32)
    tops, bottoms = slice(0, CHUNK), slice(CHUNK, 2 * CHUNK)

    def stacked(values):
        return jnp.concatenate(
            (jnp.where(first_head, values, 0.0), jnp.where(first_head, 0.0, values)), 0
        )

    def each_chunk(values, at):
        return jnp.concatenate(
            [jnp.broadcast_to(values[c + at : c + at + 1], (CHUNK, lanes)) for c in (0, CHUNK)], 0
        )

    held = []
    for p in range(seqs):
        at = slice(p * size, (p + 1) * size)
        rec = proj_ref[at, :lanes].astype(F32)
        key = proj_ref[at, lanes : 2 * lanes].astype(F32)
        value = proj_ref[at, 2 * lanes :].astype(F32)
        by_head = [
            jnp.broadcast_to(extra_ref[p, k : k + 1, :], (HEAD_CHANNELS, size)) for k in range(2)
        ]
        logged = log_ref[at, :] + jnp.concatenate(by_head, 0).T
        squares = lax.dot_general(
            key * key, head_sum, MM, precision=lax.Precision.HIGHEST, preferred_element_type=F32
        )
        unit = key * lax.rsqrt(squares + 1e-06)
        beta = unit * rate_ref[at, :]
        total = lax.dot_general(
            running, logged, MM, precision=lax.Precision.HIGHEST, preferred_element_type=F32
        )
        middle = each_chunk(total, CHUNK // 2 - 1)
        ending = each_chunk(total, CHUNK - 1)
        previous = total - logged
        fall = jnp.exp(middle - total)
        to_end = jnp.exp(ending - total)
        zeta = -unit
        left = jnp.concatenate(
            (stacked(zeta * jnp.exp(previous - middle)), stacked(rec * jnp.exp(total - middle))), 0
        )
        right = jnp.concatenate((beta * fall, key * fall), 0)
        held.append(
            dict(
                grams=mul(left, right, NT),
                zeta_true=zeta * jnp.exp(previous),
                rec_true=rec * jnp.exp(total),
                beta_end=beta * to_end,
                key_end=key * to_end,
                value=value,
                ending=jnp.exp(total),
            )
        )
    for h in held:
        grams = h.pop("grams")
        blank = jnp.zeros((size, size), F32)

        def spread(first, second, mask):
            both = jnp.concatenate(
                (
                    jnp.concatenate((first, blank), 1),
                    jnp.concatenate((blank, second), 1),
                ),
                0,
            )
            return jnp.where(mask, both, 0.0).astype(BF16)

        h["zb"] = spread(grams[:size, :size], grams[size : 2 * size, :size], strict)
        h["zk"] = spread(grams[:size, size:], grams[size : 2 * size, size:], strict)
        h["rb"] = spread(grams[2 * size : 3 * size, :size], grams[3 * size :, :size], upto)
        h["rk"] = spread(grams[2 * size : 3 * size, size:], grams[3 * size :, size:], upto)
        h["inverse"] = identity + jnp.where(pairs_of_two, h["zb"].astype(F32), 0.0)
        h["from_values"] = mul(
            jnp.concatenate((h["zk"], h["rk"]), 0), stacked(h["value"])
        )
    for merge in merges:
        for h in held:
            inner = mul(jnp.where(merge, h["zb"].astype(F32), 0.0), h["inverse"])
            h["inner"] = inner
        for h in held:
            h["inverse"] = h["inverse"] + mul(h["inverse"], h["inner"])
    for h in held:
        right = jnp.concatenate((stacked(h["zeta_true"]), h["from_values"][: 2 * size]), 1)
        h["pulled"] = mul(h["inverse"], right)
    for p, h in enumerate(held):
        start = jnp.concatenate((stacked(h["rec_true"]), h["from_values"][2 * size :]), 1)
        seen = start + mul(h["rb"], h["pulled"])
        seen = seen[:size] + seen[size:]
        pulled = h["pulled"][:size] + h["pulled"][size:]
        query, ready = seen[:, :lanes], seen[:, lanes:]
        maps = []
        for part, last in ((tops, CHUNK - 1), (bottoms, 2 * CHUNK - 1)):
            moved = mul(pulled[part], h["beta_end"][part], TN)
            added = mul(h["value"][part], h["key_end"][part], TN)
            kept = jnp.where(diagonal, h["ending"][last : last + 1], 0.0)
            maps.append(
                (
                    kept + jnp.where(head_block, moved[:lanes], 0.0),
                    jnp.where(head_block, moved[lanes:] + added, 0.0),
                )
            )
        both = mul(jnp.concatenate(maps[0], 0), maps[1][0])
        carry = both[:lanes]
        offset = both[lanes:] + maps[1][1]
        later = mul(query[bottoms], jnp.concatenate(maps[0], 0), NT)
        query = jnp.concatenate((query[tops], later[:, :lanes]), 0)
        ready = jnp.concatenate((ready[tops], ready[bottoms] + later[:, lanes:]), 0)
        at = slice(p * size, (p + 1) * size)
        q_ref[at, :] = query.astype(BF16)
        o_ref[at, :] = ready
        half = places((HEAD_CHANNELS, lanes), 1) < HEAD_CHANNELS
        turned_offset = pltpu.roll(offset, HEAD_CHANNELS, 1)
        turned_carry = pltpu.roll(carry, HEAD_CHANNELS, 1)
        maps_ref[2 * p] = jnp.where(
            half, carry[:HEAD_CHANNELS], turned_offset[:HEAD_CHANNELS]
        ).astype(BF16)
        maps_ref[2 * p + 1] = jnp.where(
            half, turned_carry[HEAD_CHANNELS:], offset[HEAD_CHANNELS:]
        ).astype(BF16)


def position_maps(proj, logged, rate, extra):
    seqs, heads, tok_count = extra.shape
    rows, lanes = logged.shape
    group = seqs // 2
    return pl.pallas_call(
        maps_kernel,
        grid=(seqs // group,),
        out_shape=(
            jax.ShapeDtypeStruct((rows, lanes), BF16),
            jax.ShapeDtypeStruct((rows, lanes), F32),
            jax.ShapeDtypeStruct((seqs * heads, HEAD_CHANNELS, lanes), BF16),
        ),
        in_specs=[
            pl.BlockSpec((group * tok_count, 3 * lanes), lambda s: (s, 0)),
            pl.BlockSpec((group * tok_count, lanes), lambda s: (s, 0)),
            pl.BlockSpec((group * tok_count, lanes), lambda s: (s, 0)),
            pl.BlockSpec((group, heads, tok_count), lambda s: (s, 0, 0)),
        ],
        out_specs=(
            pl.BlockSpec((group * tok_count, lanes), lambda s: (s, 0)),
            pl.BlockSpec((group * tok_count, lanes), lambda s: (s, 0)),
            pl.BlockSpec((group * heads, HEAD_CHANNELS, lanes), lambda s: (s, 0, 0)),
        ),
        compiler_params=pltpu.CompilerParams(vmem_limit_bytes=VMEM_BYTES),
        cost_estimate=pl.CostEstimate(
            flops=rows * lanes * 2 * 256 * 20,
            bytes_accessed=rows * lanes * 20,
            transcendentals=6 * rows * lanes,
        ),
        name="position_maps",
    )(proj, logged, rate, extra)


def states_kernel(maps_ref, start_ref, out_ref):
    count = maps_ref.shape[0]
    n = HEAD_CHANNELS
    state = jnp.concatenate((start_ref[:, :n], start_ref[:, n:]), 0)
    for i in range(count):
        out_ref[i] = jnp.concatenate((state[: n // 2], state[n // 2 :]), 1).astype(BF16)
        if i + 1 < count:
            pair = maps_ref[i]
            high = state.astype(BF16)
            low = (state - high.astype(F32)).astype(BF16)
            moved = mul(jnp.concatenate((high, low), 0), pair[:, :n])
            state = moved[:n] + moved[n:] + pair[:, n:].astype(F32)


def states_ahead(maps, start):
    count = maps.shape[0]
    whole = pl.BlockSpec(memory_space=pltpu.VMEM)
    return pl.pallas_call(
        states_kernel,
        out_shape=jax.ShapeDtypeStruct((count, HEAD_CHANNELS // 2, 2 * HEAD_CHANNELS), BF16),
        in_specs=[whole, whole],
        out_specs=whole,
        cost_estimate=pl.CostEstimate(
            flops=count * 4 * HEAD_CHANNELS**3, bytes_accessed=1 << 19, transcendentals=0
        ),
        name="states_ahead",
    )(maps, start)


def halves(weights):
    rows = weights[0].shape[0] // 2
    return [w[k * rows : (k + 1) * rows, :] for k in range(2) for w in weights]


def pack_kernel(*refs):
    out_ref = refs[-1]
    at = 0
    for piece in [r[...] for r in refs[:-4]] + halves([r[...] for r in refs[-4:-1]]):
        out_ref[0, :, at : at + piece.shape[1]] = piece
        at += piece.shape[1]


def packed(leading, weights, groups):
    rows, cols = weights[0].shape
    lanes = cols // groups
    width = sum(x.shape[1] for x in leading) + 6 * lanes
    whole = pl.BlockSpec(memory_space=pltpu.VMEM)
    return pl.pallas_call(
        pack_kernel,
        grid=(groups,),
        out_shape=jax.ShapeDtypeStruct((groups, rows // 2, width), BF16),
        in_specs=[whole] * len(leading) + [pl.BlockSpec((rows, lanes), lambda g: (0, g))] * 3,
        out_specs=pl.BlockSpec((1, rows // 2, width), lambda g: (g, 0, 0)),
        compiler_params=pltpu.CompilerParams(vmem_limit_bytes=VMEM_BYTES),
        cost_estimate=pl.CostEstimate(
            flops=1 << 20, bytes_accessed=4 * groups * rows * width, transcendentals=0
        ),
        name="packed",
    )(*leading, *weights)


def fox_kernel(at_ref, mine_ref, other_ref, gain_ref, fox_ref, normed_ref, weight_scr):
    n = HEAD_CHANNELS
    groups, rows, width = other_ref.shape
    pairs, _, tok_count = fox_ref.shape
    heads = pairs * tok_count // rows
    lanes = heads * n
    step = pl.program_id(0)

    @pl.when(step == 0)
    def _():
        for i in range(groups):
            source = lax.rem(i + at_ref[0] * (groups // 2), groups)
            for k in range(2):
                at = width + 3 * k * lanes
                weight_scr[(2 * i + k) * rows : (2 * i + k + 1) * rows, :] = mine_ref[
                    source, :, at : at + 3 * lanes
                ]

    pieces = [mine_ref[step, :, :width].astype(F32), other_ref[step].astype(F32)]
    square = sum(jnp.sum(x * x, axis=1, keepdims=True) for x in pieces)
    scaling = lax.rsqrt(square / (2 * width) + 1e-06)
    normed = jnp.concatenate(
        [
            (x * scaling * gain_ref[:, i * width : (i + 1) * width].astype(F32)).astype(BF16)
            for i, x in enumerate(pieces)
        ],
        1,
    )
    normed_ref[...] = normed
    fox = lax.dot_general(normed, weight_scr[...], MM, preferred_element_type=F32)
    for s in range(rows // tok_count):
        here = slice(s * tok_count, (s + 1) * tok_count)
        for k in range(3):
            turned = fox[here, k * lanes : (k + 1) * lanes].T.astype(BF16)
            for h in range(heads):
                fox_ref[s * heads + h, k * n : (k + 1) * n, :] = turned[h * n : (h + 1) * n]


def fox_projections(at, mine, other, gain, tok_count):
    groups, rows, width = other.shape
    lanes = (mine.shape[2] - width) // 6
    heads = lanes // HEAD_CHANNELS
    pairs = rows // tok_count * heads
    whole = pl.BlockSpec(memory_space=pltpu.VMEM)
    return pl.pallas_call(
        fox_kernel,
        grid=(groups,),
        out_shape=(
            jax.ShapeDtypeStruct((groups * pairs, 3 * HEAD_CHANNELS, tok_count), BF16),
            jax.ShapeDtypeStruct((groups * rows, 2 * width), BF16),
        ),
        in_specs=[pl.BlockSpec(memory_space=pltpu.SMEM), whole, whole, whole],
        out_specs=(
            pl.BlockSpec((pairs, 3 * HEAD_CHANNELS, tok_count), lambda g: (g, 0, 0)),
            pl.BlockSpec((rows, 2 * width), lambda g: (g, 0)),
        ),
        scratch_shapes=[pltpu.VMEM((2 * width, 3 * lanes), BF16)],
        compiler_params=pltpu.CompilerParams(vmem_limit_bytes=VMEM_BYTES),
        cost_estimate=pl.CostEstimate(
            flops=12 * groups * rows * width * lanes,
            bytes_accessed=8 * groups * rows * width,
            transcendentals=0,
        ),
        name="fox_projections",
    )(at, mine, other, gain)


def lin_kernel(at_ref, normed_ref, low_ref, decay_up_ref, rate_up_ref, base_ref, *rest):
    sent_refs, (lin_ref, log_ref, rate_ref, weight_scr) = rest[:-4], rest[-4:]
    groups = len(sent_refs)
    rows, both = sent_refs[0].shape
    lanes = both // 6

    @pl.when(pl.program_id(0) == 0)
    def _():
        for d, ref in enumerate(sent_refs):
            source = lax.rem(at_ref[1] + (groups - d), groups)
            place = lax.rem(source + at_ref[0] * (groups // 2), groups)
            for k in range(2):
                start = pl.multiple_of((2 * place + k) * rows, rows)
                weight_scr[pl.ds(start, rows), :] = ref[:, 3 * k * lanes : 3 * (k + 1) * lanes]

    normed = normed_ref[...]
    lin_ref[...] = lax.dot_general(
        normed, weight_scr[...], MM, preferred_element_type=F32
    ).astype(BF16)
    low = lax.dot_general(normed, low_ref[...], MM, preferred_element_type=F32)
    inner = low.shape[1] // 2
    decay = mul(jnp.tanh(low[:, :inner]), decay_up_ref[...]) + base_ref[0:1, :]
    log_ref[...] = jax.nn.sigmoid(decay) * -(2.718281828459045**-0.5)
    rate = mul(low[:, inner:], rate_up_ref[...]) + base_ref[1:2, :]
    rate_ref[...] = jax.nn.sigmoid(rate)


def lin_projections(at, normed, low, decay_up, rate_up, bases, sent):
    rows, width = normed.shape
    lanes = sent[0].shape[1] // 6
    tall = rows // 4
    whole = pl.BlockSpec(memory_space=pltpu.VMEM)
    return pl.pallas_call(
        lin_kernel,
        grid=(rows // tall,),
        out_shape=(
            jax.ShapeDtypeStruct((rows, 3 * lanes), BF16),
            jax.ShapeDtypeStruct((rows, lanes), F32),
            jax.ShapeDtypeStruct((rows, lanes), F32),
        ),
        in_specs=[
            pl.BlockSpec(memory_space=pltpu.SMEM),
            pl.BlockSpec((tall, width), lambda s: (s, 0)),
        ]
        + [whole] * (4 + len(sent)),
        out_specs=(
            pl.BlockSpec((tall, 3 * lanes), lambda s: (s, 0)),
            pl.BlockSpec((tall, lanes), lambda s: (s, 0)),
            pl.BlockSpec((tall, lanes), lambda s: (s, 0)),
        ),
        scratch_shapes=[pltpu.VMEM((width, 3 * lanes), BF16)],
        compiler_params=pltpu.CompilerParams(vmem_limit_bytes=VMEM_BYTES),
        cost_estimate=pl.CostEstimate(
            flops=10 * rows * width * lanes,
            bytes_accessed=2 * rows * width,
            transcendentals=3 * rows * lanes,
        ),
        name="lin_projections",
    )(at, normed, low, decay_up, rate_up, bases, *sent)


def heads_kernel(back_ref, q_ref, o_ref, gain_ref, out_ref):
    n = HEAD_CHANNELS
    lanes = 2 * n
    pairs, _, tok_count = back_ref.shape
    groups, rows, _ = out_ref.shape
    head_block = (places((lanes, lanes), 0) < n) == (places((lanes, lanes), 1) < n)
    average = jnp.where(head_block, 1.0 / n, 0.0).astype(BF16)
    first = places((n // 2, lanes), 1) < n
    gain = gain_ref[...].astype(F32)

    def mean(values):
        high = values.astype(BF16)
        low = (values - high.astype(F32)).astype(BF16)
        return mul(high, average) + mul(low, average)

    raws = []
    for s in range(pairs // 2):
        here = slice(s * tok_count, (s + 1) * tok_count)
        group, at = s * tok_count // rows, s * tok_count % rows
        fox = jnp.concatenate((back_ref[2 * s, :n, :], back_ref[2 * s + 1, :n, :]), 0)
        out_ref[group, at : at + tok_count, :lanes] = fox.astype(F32).T.astype(BF16)
        packed = [back_ref[2 * s + k, n:, :].astype(F32) for k in range(2)]
        turned = [pltpu.roll(x, n, 1) for x in packed]
        state = jnp.concatenate(
            (
                jnp.where(first, packed[0], 0.0),
                jnp.where(first, turned[0], 0.0),
                jnp.where(first, 0.0, turned[1]),
                jnp.where(first, 0.0, packed[1]),
            ),
            0,
        )
        raws.append(mul(q_ref[here, :], state, NT) + o_ref[here, :])
    centred = [raw - mean(raw) for raw in raws]
    spreads = [mean(x * x) for x in centred]
    for s, (x, spread) in enumerate(zip(centred, spreads)):
        group, at = s * tok_count // rows, s * tok_count % rows
        lin = x * lax.rsqrt(spread + 0.00064) * gain
        out_ref[group, at : at + tok_count, lanes:] = lin.astype(BF16)


def heads_out(back, query, ready, gain, groups):
    rows, lanes = query.shape
    whole = pl.BlockSpec(memory_space=pltpu.VMEM)
    return pl.pallas_call(
        heads_kernel,
        out_shape=jax.ShapeDtypeStruct((groups, rows // groups, 2 * lanes), BF16),
        in_specs=[whole] * 4,
        out_specs=whole,
        compiler_params=pltpu.CompilerParams(vmem_limit_bytes=VMEM_BYTES),
        cost_estimate=pl.CostEstimate(
            flops=10 * rows * lanes * lanes, bytes_accessed=12 * rows * lanes, transcendentals=0
        ),
        name="heads_out",
    )(back, query, ready, gain)


def closing_kernel(acts_ref, fox_w_ref, lin_w_ref, out_ref, act_scr):
    groups, rows, both = acts_ref.shape
    lanes = both // 2
    cols = groups * lanes

    @pl.when(pl.program_id(0) == 0)
    def _():
        for g in range(groups):
            act_scr[:, g * lanes : (g + 1) * lanes] = acts_ref[g, :, :lanes]
            act_scr[:, cols + g * lanes : cols + (g + 1) * lanes] = acts_ref[g, :, lanes:]

    out_ref[...] = (
        lax.dot_general(act_scr[:, :cols], fox_w_ref[...], NT, preferred_element_type=F32)
        + lax.dot_general(act_scr[:, cols:], lin_w_ref[...], NT, preferred_element_type=F32)
    ).astype(BF16)


def closing(acts, fox_w, lin_w):
    groups, rows, both = acts.shape
    width, cols = fox_w.shape
    tile = 512
    return pl.pallas_call(
        closing_kernel,
        grid=(width // tile,),
        out_shape=jax.ShapeDtypeStruct((rows, width), BF16),
        in_specs=[
            pl.BlockSpec(memory_space=pltpu.VMEM),
            pl.BlockSpec((tile, cols), lambda i: (i, 0)),
            pl.BlockSpec((tile, cols), lambda i: (i, 0)),
        ],
        out_specs=pl.BlockSpec((rows, tile), lambda i: (0, i)),
        scratch_shapes=[pltpu.VMEM((rows, 2 * cols), BF16)],
        compiler_params=pltpu.CompilerParams(vmem_limit_bytes=VMEM_BYTES),
        cost_estimate=pl.CostEstimate(
            flops=4 * rows * cols * width,
            bytes_accessed=4 * cols * width + 2 * rows * width,
            transcendentals=0,
        ),
        name="closing",
    )(acts, fox_w, lin_w)


def exchange(x, axis):
    return lax.all_to_all(x, axis, 0, 0, tiled=True)


def by_permutes(x, axis):
    size = lax.axis_size(axis)
    here = lax.axis_index(axis)
    return [
        lax.ppermute(block, axis, [(i, (i + d) % size) for i in range(size)]) if d else block
        for d in range(size)
        for block in [lax.dynamic_index_in_dim(x, lax.rem(here + d, size), 0, False)]
    ]


def per_device(
    inputs,
    input_norm_gain,
    softmax_query_matrix,
    softmax_key_matrix,
    softmax_value_matrix,
    running_forget_gate,
    receptance_weight,
    linear_key_weight,
    linear_value_weight,
    decay_lower_map,
    decay_upper_map,
    decay_offset_base,
    decay_extra_log,
    rate_lower_map,
    rate_upper_map,
    rate_offset_base,
    linear_head_gain,
    starting_state,
    softmax_output_weight,
    linear_output_weight,
):
    n = HEAD_CHANNELS
    seq_count, tok_count, half_width = inputs.shape
    rows = seq_count * tok_count
    cols = softmax_query_matrix.shape[1]
    groups, tp = lax.axis_size("fs"), lax.axis_size("tp")
    lanes = cols // groups
    heads = lanes // n
    seqs = groups * seq_count
    length = running_forget_gate.shape[1]
    place = lax.axis_index("sp")
    col_start = lax.axis_index("tp") * cols + lax.axis_index("fs") * lanes

    here, side = lax.axis_index("fs"), lax.axis_index("tp")
    at = jnp.stack((side, here)).astype(jnp.int32)
    mine = exchange(
        packed(
            (inputs.reshape(rows, half_width),),
            (softmax_query_matrix, softmax_key_matrix, softmax_value_matrix),
            groups,
        ),
        "fs",
    )
    lin_sent = packed((), (receptance_weight, linear_key_weight, linear_value_weight), groups)
    mine, lin_sent = lax.optimization_barrier((mine, lin_sent))
    lin_sent = by_permutes(lin_sent, "fs")

    pair_seq, pair_head = place // heads, lax.rem(place, heads)
    pair_group, pair_slot = pair_seq // seq_count, lax.rem(pair_seq, seq_count)

    def of_pair(table, head_dim):
        table = lax.dynamic_index_in_dim(table, pair_slot, 0, False)
        shape = table.shape
        table = table.reshape(*shape[:head_dim], groups, heads, *shape[head_dim + 1 :])
        return lax.dynamic_index_in_dim(table, pair_head, head_dim + 1, False)

    state = of_pair(starting_state, 0)
    state = jnp.concatenate((state[:, : n // 2], state[:, n // 2 :]), 2)
    gates = of_pair(running_forget_gate, 1).T.reshape(groups, length // tok_count, tok_count)
    extra = decay_extra_log.reshape(seq_count, tok_count, groups, heads).transpose(2, 0, 3, 1)
    extra = extra.reshape(groups, seq_count * heads, tok_count)
    small = jnp.stack(by_permutes(jnp.concatenate((state, gates, extra), 1), "fs"))
    half, after = n // 2, n // 2 + length // tok_count

    def small_from(group):
        return lax.dynamic_index_in_dim(small, lax.rem(here + groups - group, groups), 0, False)

    extra = jnp.concatenate([small_from(g)[after:] for g in range(groups)], 0)
    extra = extra.reshape(seqs, heads, tok_count)
    pair = small_from(pair_group)
    start, gate = pair[:half], pair[half:after]

    def own_columns(table, axis):
        return lax.dynamic_slice_in_dim(table, col_start, lanes, axis)

    def own_first(table, axis):
        return jnp.where(side == 0, table, jnp.roll(table, half_width, axis))

    swap = [(i, tp - 1 - i) for i in range(tp)]
    other = lax.ppermute(mine[:, :, :half_width], "tp", swap)
    fox, normed = fox_projections(
        at, mine, other, own_first(input_norm_gain.reshape(1, -1), 1), tok_count
    )
    fox = exchange(fox, "sp")
    lin, logged, rate = lin_projections(
        at,
        normed,
        own_first(jnp.concatenate((decay_lower_map, rate_lower_map), 1), 0),
        own_columns(decay_upper_map, 1),
        own_columns(rate_upper_map, 1),
        jnp.stack((own_columns(decay_offset_base, 0), own_columns(rate_offset_base, 0))),
        lin_sent,
    )
    query, ready, maps = position_maps(lin, logged, rate, extra)
    maps, fox = lax.optimization_barrier((maps, fox))
    maps = exchange(maps, "sp")
    fox_out = attention(fox, gate)
    states = states_ahead(maps, start)
    back = exchange(jnp.concatenate((fox_out, states), 1), "sp")
    gain = own_columns(linear_head_gain, 0).reshape(1, lanes)
    acts = exchange(heads_out(back, query, ready, gain, groups), "fs")
    partial = closing(acts, softmax_output_weight, linear_output_weight)
    pieces = exchange(partial.reshape(seq_count, tok_count, -1), "tp")
    mixed = jnp.sum(
        pieces.reshape(tp, seq_count // tp, tok_count, -1).astype(F32), axis=0
    )
    return mixed.astype(BF16)


def solution(mesh):
    placed = (
        P(("grp", "fs"), "sp", "tp"),
        P(),
        P("fs", "tp"),
        P("fs", "tp"),
        P("fs", "tp"),
        P(("grp", "fs"), None, "tp"),
        P("fs", "tp"),
        P("fs", "tp"),
        P("fs", "tp"),
        P(),
        P(),
        P(),
        P(("grp", "fs"), "sp", "tp"),
        P(),
        P(),
        P(),
        P(),
        P(("grp", "fs"), "tp", None, None),
        P(None, "tp"),
        P(None, "tp"),
    )
    return jax.shard_map(
        per_device,
        mesh=mesh,
        in_specs=placed,
        out_specs=P(("grp", "fs", "tp"), "sp", None),
        check_vma=False,
    )
```

```python
import jax
import jax.numpy as jnp
from jax import lax
from jax.experimental import pallas as pl
from jax.experimental.pallas import tpu as pltpu
from jax.sharding import PartitionSpec as P

HEAD_CHANNELS = 64
CHUNK = 64
F32 = jnp.float32
BF16 = jnp.bfloat16
VMEM_BYTES = 56 * 1024 * 1024

MM = (((1,), (0,)), ((), ()))
NT = (((1,), (1,)), ((), ()))
TN = (((0,), (0,)), ((), ()))


def mul(left, right, dims=MM):
    return lax.dot_general(
        left.astype(BF16), right.astype(BF16), dims, preferred_element_type=F32
    )


def places(shape, dim):
    return lax.broadcasted_iota(jnp.int32, shape, dim)


def attention_kernel(blocks_ref, gate_ref, out_ref, key_scr, value_scr):
    count, _, width = blocks_ref.shape
    channels = HEAD_CHANNELS
    for i in range(count):
        gate = gate_ref[i : i + 1, :]
        high = gate.astype(BF16).astype(F32)
        rest = gate - high
        middle = rest.astype(BF16).astype(F32)
        low = rest - middle
        row = places((channels, width), 0)
        extra = jnp.where(row == 0, high, jnp.where(row == 1, middle, jnp.where(row == 2, low, 0.0)))
        key_rows = blocks_ref[i, channels : 2 * channels, :].astype(F32)
        key_scr[i * width : (i + 1) * width, :] = jnp.concatenate((key_rows, extra), 0).T.astype(BF16)
        value_scr[:, i * width : (i + 1) * width] = blocks_ref[i, 2 * channels :, :]
    step = 2 * width
    row = places((channels, step), 0)
    tail = jnp.where(row < 3, -1.0, 0.0).astype(BF16)
    live = places((step, step), 0) <= places((step, step), 1)
    for i in range(count // 2):
        query = jnp.concatenate(
            (blocks_ref[2 * i, :channels, :], blocks_ref[2 * i + 1, :channels, :]), 1
        )
        query = (query.astype(F32) * channels ** (-0.5)).astype(BF16)
        query = jnp.concatenate((query, tail), 0)
        before = i * step
        own = lax.dot_general(
            key_scr[before : before + step, :], query, MM, preferred_element_type=F32
        )
        own = jnp.where(live, own, -1e30)
        top = jnp.max(own, axis=0, keepdims=True)
        if before:
            past = lax.dot_general(key_scr[:before, :], query, MM, preferred_element_type=F32)
            top = jnp.maximum(top, jnp.max(past, axis=0, keepdims=True))
        weight = jnp.exp(own - top)
        total = jnp.sum(weight, axis=0, keepdims=True)
        mixed = lax.dot_general(
            value_scr[:, before : before + step],
            weight.astype(BF16),
            MM,
            preferred_element_type=F32,
        )
        if before:
            weight = jnp.exp(past - top)
            total = total + jnp.sum(weight, axis=0, keepdims=True)
            mixed = mixed + lax.dot_general(
                value_scr[:, :before], weight.astype(BF16), MM, preferred_element_type=F32
            )
        mixed = (mixed / total).astype(BF16)
        out_ref[2 * i] = mixed[:, :width]
        out_ref[2 * i + 1] = mixed[:, width:]


def attention(blocks, gate):
    count, rows, width = blocks.shape
    whole = pl.BlockSpec(memory_space=pltpu.VMEM)
    return pl.pallas_call(
        attention_kernel,
        out_shape=jax.ShapeDtypeStruct((count, HEAD_CHANNELS, width), BF16),
        in_specs=[whole, whole],
        out_specs=whole,
        scratch_shapes=[
            pltpu.VMEM((count * width, 2 * HEAD_CHANNELS), BF16),
            pltpu.VMEM((HEAD_CHANNELS, count * width), BF16),
        ],
        compiler_params=pltpu.CompilerParams(vmem_limit_bytes=VMEM_BYTES),
        cost_estimate=pl.CostEstimate(
            flops=4 * HEAD_CHANNELS * (count * width) ** 2,
            bytes_accessed=4 * count * rows * width,
            transcendentals=(count * width) ** 2 // 2,
        ),
        name="attention",
    )(blocks, gate)


def chunk_masks(size):
    row, col = places((2 * size, 2 * size), 0), places((2 * size, 2 * size), 1)
    same = row // CHUNK == col // CHUNK
    return row, col, same


def maps_kernel(proj_ref, log_ref, rate_ref, extra_ref, q_ref, o_ref, maps_ref):
    seqs, _, size = extra_ref.shape
    lanes = 2 * HEAD_CHANNELS
    row, col, same = chunk_masks(size)
    strict = same & (row > col)
    upto = same & (row >= col)
    merges = []
    block = 2
    while block < CHUNK:
        merges.append((row // (2 * block) == col // (2 * block)) & (row // block > col // block))
        block *= 2
    pairs_of_two = (row // 2 == col // 2) & (row > col)
    identity = (row == col).astype(F32)
    lane = places((size, lanes), 1)
    first_head = lane < HEAD_CHANNELS
    head_block = (places((lanes, lanes), 0) < HEAD_CHANNELS) == (
        places((lanes, lanes), 1) < HEAD_CHANNELS
    )
    diagonal = places((lanes, lanes), 0) == places((lanes, lanes), 1)
    small_row, small_col = places((size, size), 0), places((size, size), 1)
    running = ((small_row // CHUNK == small_col // CHUNK) & (small_row >= small_col)).astype(F32)
    head_sum = head_block.astype(F32)
    tops, bottoms = slice(0, CHUNK), slice(CHUNK, 2 * CHUNK)

    def stacked(values):
        return jnp.concatenate(
            (jnp.where(first_head, values, 0.0), jnp.where(first_head, 0.0, values)), 0
        )

    def each_chunk(values, at):
        return jnp.concatenate(
            [jnp.broadcast_to(values[c + at : c + at + 1], (CHUNK, lanes)) for c in (0, CHUNK)], 0
        )

    held = []
    for p in range(seqs):
        at = slice(p * size, (p + 1) * size)
        rec = proj_ref[at, :lanes].astype(F32)
        key = proj_ref[at, lanes : 2 * lanes].astype(F32)
        value = proj_ref[at, 2 * lanes :].astype(F32)
        by_head = [
            jnp.broadcast_to(extra_ref[p, k : k + 1, :], (HEAD_CHANNELS, size)) for k in range(2)
        ]
        logged = log_ref[at, :] + jnp.concatenate(by_head, 0).T
        squares = lax.dot_general(
            key * key, head_sum, MM, precision=lax.Precision.HIGHEST, preferred_element_type=F32
        )
        unit = key * lax.rsqrt(squares + 1e-06)
        beta = unit * rate_ref[at, :]
        total = lax.dot_general(
            running, logged, MM, precision=lax.Precision.HIGHEST, preferred_element_type=F32
        )
        middle = each_chunk(total, CHUNK // 2 - 1)
        ending = each_chunk(total, CHUNK - 1)
        previous = total - logged
        fall = jnp.exp(middle - total)
        to_end = jnp.exp(ending - total)
        zeta = -unit
        left = jnp.concatenate(
            (stacked(zeta * jnp.exp(previous - middle)), stacked(rec * jnp.exp(total - middle))), 0
        )
        right = jnp.concatenate((beta * fall, key * fall), 0)
        held.append(
            dict(
                grams=mul(left, right, NT),
                zeta_true=zeta * jnp.exp(previous),
                rec_true=rec * jnp.exp(total),
                beta_end=beta * to_end,
                key_end=key * to_end,
                value=value,
                ending=jnp.exp(total),
            )
        )
    for h in held:
        grams = h.pop("grams")
        blank = jnp.zeros((size, size), F32)

        def spread(first, second, mask):
            both = jnp.concatenate(
                (
                    jnp.concatenate((first, blank), 1),
                    jnp.concatenate((blank, second), 1),
                ),
                0,
            )
            return jnp.where(mask, both, 0.0).astype(BF16)

        h["zb"] = spread(grams[:size, :size], grams[size : 2 * size, :size], strict)
        h["zk"] = spread(grams[:size, size:], grams[size : 2 * size, size:], strict)
        h["rb"] = spread(grams[2 * size : 3 * size, :size], grams[3 * size :, :size], upto)
        h["rk"] = spread(grams[2 * size : 3 * size, size:], grams[3 * size :, size:], upto)
        h["inverse"] = identity + jnp.where(pairs_of_two, h["zb"].astype(F32), 0.0)
        h["from_values"] = mul(
            jnp.concatenate((h["zk"], h["rk"]), 0), stacked(h["value"])
        )
    for merge in merges:
        for h in held:
            inner = mul(jnp.where(merge, h["zb"].astype(F32), 0.0), h["inverse"])
            h["inner"] = inner
        for h in held:
            h["inverse"] = h["inverse"] + mul(h["inverse"], h["inner"])
    for h in held:
        right = jnp.concatenate((stacked(h["zeta_true"]), h["from_values"][: 2 * size]), 1)
        h["pulled"] = mul(h["inverse"], right)
    for p, h in enumerate(held):
        start = jnp.concatenate((stacked(h["rec_true"]), h["from_values"][2 * size :]), 1)
        seen = start + mul(h["rb"], h["pulled"])
        seen = seen[:size] + seen[size:]
        pulled = h["pulled"][:size] + h["pulled"][size:]
        query, ready = seen[:, :lanes], seen[:, lanes:]
        maps = []
        for part, last in ((tops, CHUNK - 1), (bottoms, 2 * CHUNK - 1)):
            moved = mul(pulled[part], h["beta_end"][part], TN)
            added = mul(h["value"][part], h["key_end"][part], TN)
            kept = jnp.where(diagonal, h["ending"][last : last + 1], 0.0)
            maps.append(
                (
                    kept + jnp.where(head_block, moved[:lanes], 0.0),
                    jnp.where(head_block, moved[lanes:] + added, 0.0),
                )
            )
        both = mul(jnp.concatenate(maps[0], 0), maps[1][0])
        carry = both[:lanes]
        offset = both[lanes:] + maps[1][1]
        later = mul(query[bottoms], jnp.concatenate(maps[0], 0), NT)
        query = jnp.concatenate((query[tops], later[:, :lanes]), 0)
        ready = jnp.concatenate((ready[tops], ready[bottoms] + later[:, lanes:]), 0)
        at = slice(p * size, (p + 1) * size)
        q_ref[at, :] = query.astype(BF16)
        o_ref[at, :] = ready
        half = places((HEAD_CHANNELS, lanes), 1) < HEAD_CHANNELS
        turned_offset = pltpu.roll(offset, HEAD_CHANNELS, 1)
        turned_carry = pltpu.roll(carry, HEAD_CHANNELS, 1)
        maps_ref[2 * p] = jnp.where(
            half, carry[:HEAD_CHANNELS], turned_offset[:HEAD_CHANNELS]
        ).astype(BF16)
        maps_ref[2 * p + 1] = jnp.where(
            half, turned_carry[HEAD_CHANNELS:], offset[HEAD_CHANNELS:]
        ).astype(BF16)


def position_maps(proj, logged, rate, extra):
    seqs, heads, tok_count = extra.shape
    rows, lanes = logged.shape
    group = seqs // 2
    return pl.pallas_call(
        maps_kernel,
        grid=(seqs // group,),
        out_shape=(
            jax.ShapeDtypeStruct((rows, lanes), BF16),
            jax.ShapeDtypeStruct((rows, lanes), F32),
            jax.ShapeDtypeStruct((seqs * heads, HEAD_CHANNELS, lanes), BF16),
        ),
        in_specs=[
            pl.BlockSpec((group * tok_count, 3 * lanes), lambda s: (s, 0)),
            pl.BlockSpec((group * tok_count, lanes), lambda s: (s, 0)),
            pl.BlockSpec((group * tok_count, lanes), lambda s: (s, 0)),
            pl.BlockSpec((group, heads, tok_count), lambda s: (s, 0, 0)),
        ],
        out_specs=(
            pl.BlockSpec((group * tok_count, lanes), lambda s: (s, 0)),
            pl.BlockSpec((group * tok_count, lanes), lambda s: (s, 0)),
            pl.BlockSpec((group * heads, HEAD_CHANNELS, lanes), lambda s: (s, 0, 0)),
        ),
        compiler_params=pltpu.CompilerParams(vmem_limit_bytes=VMEM_BYTES),
        cost_estimate=pl.CostEstimate(
            flops=rows * lanes * 2 * 256 * 20,
            bytes_accessed=rows * lanes * 20,
            transcendentals=6 * rows * lanes,
        ),
        name="position_maps",
    )(proj, logged, rate, extra)


def states_kernel(maps_ref, start_ref, fox_ref, out_ref):
    count = maps_ref.shape[0]
    n = HEAD_CHANNELS
    out_ref[:, :n, :] = fox_ref[...]
    state = jnp.concatenate((start_ref[:, :n], start_ref[:, n:]), 0)
    for i in range(count):
        out_ref[i, n:, :] = jnp.concatenate((state[: n // 2], state[n // 2 :]), 1).astype(BF16)
        if i + 1 < count:
            pair = maps_ref[i]
            high = state.astype(BF16)
            low = (state - high.astype(F32)).astype(BF16)
            moved = mul(jnp.concatenate((high, low), 0), pair[:, :n])
            state = moved[:n] + moved[n:] + pair[:, n:].astype(F32)


def states_ahead(maps, start, fox):
    count = maps.shape[0]
    whole = pl.BlockSpec(memory_space=pltpu.VMEM)
    return pl.pallas_call(
        states_kernel,
        out_shape=jax.ShapeDtypeStruct((count, 3 * HEAD_CHANNELS // 2, 2 * HEAD_CHANNELS), BF16),
        in_specs=[whole, whole, whole],
        out_specs=whole,
        cost_estimate=pl.CostEstimate(
            flops=count * 4 * HEAD_CHANNELS**3, bytes_accessed=1 << 19, transcendentals=0
        ),
        name="states_ahead",
    )(maps, start, fox)


def halves(weights):
    rows = weights[0].shape[0] // 2
    return [w[k * rows : (k + 1) * rows, :] for k in range(2) for w in weights]


def pack_kernel(*refs):
    out_ref = refs[-1]
    at = 0
    for piece in [r[...] for r in refs[:-4]] + halves([r[...] for r in refs[-4:-1]]):
        out_ref[0, :, at : at + piece.shape[1]] = piece
        at += piece.shape[1]


def packed(leading, weights, groups):
    rows, cols = weights[0].shape
    lanes = cols // groups
    width = sum(x.shape[1] for x in leading) + 6 * lanes
    whole = pl.BlockSpec(memory_space=pltpu.VMEM)
    return pl.pallas_call(
        pack_kernel,
        grid=(groups,),
        out_shape=jax.ShapeDtypeStruct((groups, rows // 2, width), BF16),
        in_specs=[whole] * len(leading) + [pl.BlockSpec((rows, lanes), lambda g: (0, g))] * 3,
        out_specs=pl.BlockSpec((1, rows // 2, width), lambda g: (g, 0, 0)),
        compiler_params=pltpu.CompilerParams(vmem_limit_bytes=VMEM_BYTES),
        cost_estimate=pl.CostEstimate(
            flops=1 << 20, bytes_accessed=4 * groups * rows * width, transcendentals=0
        ),
        name="packed",
    )(*leading, *weights)


def fox_kernel(at_ref, mine_ref, other_ref, gain_ref, fox_ref, normed_ref, weight_scr):
    n = HEAD_CHANNELS
    groups, rows, width = other_ref.shape
    pairs, _, tok_count = fox_ref.shape
    heads = pairs * tok_count // rows
    lanes = heads * n
    step = pl.program_id(0)

    @pl.when(step == 0)
    def _():
        for i in range(groups):
            source = lax.rem(i + at_ref[0] * (groups // 2), groups)
            for k in range(2):
                at = width + 3 * k * lanes
                weight_scr[(2 * i + k) * rows : (2 * i + k + 1) * rows, :] = mine_ref[
                    source, :, at : at + 3 * lanes
                ]

    pieces = [mine_ref[step, :, :width].astype(F32), other_ref[step].astype(F32)]
    square = sum(jnp.sum(x * x, axis=1, keepdims=True) for x in pieces)
    scaling = lax.rsqrt(square / (2 * width) + 1e-06)
    normed = jnp.concatenate(
        [
            (x * scaling * gain_ref[:, i * width : (i + 1) * width].astype(F32)).astype(BF16)
            for i, x in enumerate(pieces)
        ],
        1,
    )
    normed_ref[...] = normed
    fox = lax.dot_general(normed, weight_scr[...], MM, preferred_element_type=F32)
    for s in range(rows // tok_count):
        here = slice(s * tok_count, (s + 1) * tok_count)
        for k in range(3):
            turned = fox[here, k * lanes : (k + 1) * lanes].T.astype(BF16)
            for h in range(heads):
                fox_ref[s * heads + h, k * n : (k + 1) * n, :] = turned[h * n : (h + 1) * n]


def fox_projections(at, mine, other, gain, tok_count):
    groups, rows, width = other.shape
    lanes = (mine.shape[2] - width) // 6
    heads = lanes // HEAD_CHANNELS
    pairs = rows // tok_count * heads
    whole = pl.BlockSpec(memory_space=pltpu.VMEM)
    return pl.pallas_call(
        fox_kernel,
        grid=(groups,),
        out_shape=(
            jax.ShapeDtypeStruct((groups * pairs, 3 * HEAD_CHANNELS, tok_count), BF16),
            jax.ShapeDtypeStruct((groups * rows, 2 * width), BF16),
        ),
        in_specs=[pl.BlockSpec(memory_space=pltpu.SMEM), whole, whole, whole],
        out_specs=(
            pl.BlockSpec((pairs, 3 * HEAD_CHANNELS, tok_count), lambda g: (g, 0, 0)),
            pl.BlockSpec((rows, 2 * width), lambda g: (g, 0)),
        ),
        scratch_shapes=[pltpu.VMEM((2 * width, 3 * lanes), BF16)],
        compiler_params=pltpu.CompilerParams(vmem_limit_bytes=VMEM_BYTES),
        cost_estimate=pl.CostEstimate(
            flops=12 * groups * rows * width * lanes,
            bytes_accessed=8 * groups * rows * width,
            transcendentals=0,
        ),
        name="fox_projections",
    )(at, mine, other, gain)


def lin_kernel(at_ref, normed_ref, low_ref, decay_up_ref, rate_up_ref, base_ref, *rest):
    sent_refs, (lin_ref, log_ref, rate_ref, weight_scr) = rest[:-4], rest[-4:]
    groups = len(sent_refs)
    rows, both = sent_refs[0].shape
    lanes = both // 6

    @pl.when(pl.program_id(0) == 0)
    def _():
        for d, ref in enumerate(sent_refs):
            source = lax.rem(at_ref[1] + (groups - d), groups)
            place = lax.rem(source + at_ref[0] * (groups // 2), groups)
            for k in range(2):
                start = pl.multiple_of((2 * place + k) * rows, rows)
                weight_scr[pl.ds(start, rows), :] = ref[:, 3 * k * lanes : 3 * (k + 1) * lanes]

    normed = normed_ref[...]
    lin_ref[...] = lax.dot_general(
        normed, weight_scr[...], MM, preferred_element_type=F32
    ).astype(BF16)
    low = lax.dot_general(normed, low_ref[...], MM, preferred_element_type=F32)
    inner = low.shape[1] // 2
    decay = mul(jnp.tanh(low[:, :inner]), decay_up_ref[...]) + base_ref[0:1, :]
    log_ref[...] = jax.nn.sigmoid(decay) * -(2.718281828459045**-0.5)
    rate = mul(low[:, inner:], rate_up_ref[...]) + base_ref[1:2, :]
    rate_ref[...] = jax.nn.sigmoid(rate)


def lin_projections(at, normed, low, decay_up, rate_up, bases, sent):
    rows, width = normed.shape
    lanes = sent[0].shape[1] // 6
    tall = rows // 4
    whole = pl.BlockSpec(memory_space=pltpu.VMEM)
    return pl.pallas_call(
        lin_kernel,
        grid=(rows // tall,),
        out_shape=(
            jax.ShapeDtypeStruct((rows, 3 * lanes), BF16),
            jax.ShapeDtypeStruct((rows, lanes), F32),
            jax.ShapeDtypeStruct((rows, lanes), F32),
        ),
        in_specs=[
            pl.BlockSpec(memory_space=pltpu.SMEM),
            pl.BlockSpec((tall, width), lambda s: (s, 0)),
        ]
        + [whole] * (4 + len(sent)),
        out_specs=(
            pl.BlockSpec((tall, 3 * lanes), lambda s: (s, 0)),
            pl.BlockSpec((tall, lanes), lambda s: (s, 0)),
            pl.BlockSpec((tall, lanes), lambda s: (s, 0)),
        ),
        scratch_shapes=[pltpu.VMEM((width, 3 * lanes), BF16)],
        compiler_params=pltpu.CompilerParams(vmem_limit_bytes=VMEM_BYTES),
        cost_estimate=pl.CostEstimate(
            flops=10 * rows * width * lanes,
            bytes_accessed=2 * rows * width,
            transcendentals=3 * rows * lanes,
        ),
        name="lin_projections",
    )(at, normed, low, decay_up, rate_up, bases, *sent)


def heads_kernel(back_ref, q_ref, o_ref, gain_ref, out_ref):
    n = HEAD_CHANNELS
    lanes = 2 * n
    pairs, _, tok_count = back_ref.shape
    _, rows, _ = out_ref.shape
    head_block = (places((lanes, lanes), 0) < n) == (places((lanes, lanes), 1) < n)
    average = jnp.where(head_block, 1.0 / n, 0.0).astype(BF16)
    first = places((n // 2, lanes), 1) < n
    gain = gain_ref[...].astype(F32)

    def mean(values):
        high = values.astype(BF16)
        low = (values - high.astype(F32)).astype(BF16)
        return mul(high, average) + mul(low, average)

    raws = []
    for s in range(pairs // 2):
        here = slice(s * tok_count, (s + 1) * tok_count)
        group, at = s * tok_count // rows, s * tok_count % rows
        fox = jnp.concatenate((back_ref[2 * s, :n, :], back_ref[2 * s + 1, :n, :]), 0)
        out_ref[group, at : at + tok_count, :lanes] = fox.astype(F32).T.astype(BF16)
        packed = [back_ref[2 * s + k, n:, :].astype(F32) for k in range(2)]
        turned = [pltpu.roll(x, n, 1) for x in packed]
        state = jnp.concatenate(
            (
                jnp.where(first, packed[0], 0.0),
                jnp.where(first, turned[0], 0.0),
                jnp.where(first, 0.0, turned[1]),
                jnp.where(first, 0.0, packed[1]),
            ),
            0,
        )
        raws.append(mul(q_ref[here, :], state, NT) + o_ref[here, :])
    centred = [raw - mean(raw) for raw in raws]
    spreads = [mean(x * x) for x in centred]
    for s, (x, spread) in enumerate(zip(centred, spreads)):
        group, at = s * tok_count // rows, s * tok_count % rows
        lin = x * lax.rsqrt(spread + 0.00064) * gain
        out_ref[group, at : at + tok_count, lanes:] = lin.astype(BF16)


def heads_out(back, query, ready, gain, groups):
    rows, lanes = query.shape
    whole = pl.BlockSpec(memory_space=pltpu.VMEM)
    return pl.pallas_call(
        heads_kernel,
        out_shape=jax.ShapeDtypeStruct((groups, rows // groups, 2 * lanes), BF16),
        in_specs=[whole] * 4,
        out_specs=whole,
        compiler_params=pltpu.CompilerParams(vmem_limit_bytes=VMEM_BYTES),
        cost_estimate=pl.CostEstimate(
            flops=10 * rows * lanes * lanes, bytes_accessed=12 * rows * lanes, transcendentals=0
        ),
        name="heads_out",
    )(back, query, ready, gain)


def closing_kernel(seq_ref, acts_ref, fox_w_ref, lin_w_ref, out_ref, act_scr):
    groups, _, both = acts_ref.shape
    rows = act_scr.shape[0]
    lanes = both // 2
    cols = groups * lanes

    @pl.when(pl.program_id(0) == 0)
    def _():
        here = pl.ds(pl.multiple_of(seq_ref[0] * rows, rows), rows)
        for g in range(groups):
            act_scr[:, g * lanes : (g + 1) * lanes] = acts_ref[g, here, :lanes]
            act_scr[:, cols + g * lanes : cols + (g + 1) * lanes] = acts_ref[g, here, lanes:]

    out_ref[...] = (
        lax.dot_general(act_scr[:, :cols], fox_w_ref[...], NT, preferred_element_type=F32)
        + lax.dot_general(act_scr[:, cols:], lin_w_ref[...], NT, preferred_element_type=F32)
    ).astype(BF16)


def closing(part, parts, acts, fox_w, lin_w):
    _, rows, _ = acts.shape
    rows = rows // parts
    width, cols = fox_w.shape
    tile = 512
    return pl.pallas_call(
        closing_kernel,
        grid=(width // tile,),
        out_shape=jax.ShapeDtypeStruct((rows, width), BF16),
        in_specs=[
            pl.BlockSpec(memory_space=pltpu.SMEM),
            pl.BlockSpec(memory_space=pltpu.VMEM),
            pl.BlockSpec((tile, cols), lambda i: (i, 0)),
            pl.BlockSpec((tile, cols), lambda i: (i, 0)),
        ],
        out_specs=pl.BlockSpec((rows, tile), lambda i: (0, i)),
        scratch_shapes=[pltpu.VMEM((rows, 2 * cols), BF16)],
        compiler_params=pltpu.CompilerParams(vmem_limit_bytes=VMEM_BYTES),
        cost_estimate=pl.CostEstimate(
            flops=4 * rows * cols * width,
            bytes_accessed=4 * cols * width + 2 * rows * width,
            transcendentals=0,
        ),
        name="closing",
    )(part, acts, fox_w, lin_w)


def exchange(x, axis):
    return lax.all_to_all(x, axis, 0, 0, tiled=True)


def in_turn(x, axis):
    size = lax.axis_size(axis)
    here = lax.axis_index(axis)
    return [lax.dynamic_index_in_dim(x, lax.rem(here + d, size), 0, False) for d in range(size)]


def by_permutes(blocks, axis):
    size = lax.axis_size(axis)
    return [
        lax.ppermute(block, axis, [(i, (i + d) % size) for i in range(size)]) if d else block
        for d, block in enumerate(blocks)
    ]


def per_device(
    inputs,
    input_norm_gain,
    softmax_query_matrix,
    softmax_key_matrix,
    softmax_value_matrix,
    running_forget_gate,
    receptance_weight,
    linear_key_weight,
    linear_value_weight,
    decay_lower_map,
    decay_upper_map,
    decay_offset_base,
    decay_extra_log,
    rate_lower_map,
    rate_upper_map,
    rate_offset_base,
    linear_head_gain,
    starting_state,
    softmax_output_weight,
    linear_output_weight,
):
    n = HEAD_CHANNELS
    seq_count, tok_count, half_width = inputs.shape
    rows = seq_count * tok_count
    cols = softmax_query_matrix.shape[1]
    groups, tp = lax.axis_size("fs"), lax.axis_size("tp")
    lanes = cols // groups
    heads = lanes // n
    seqs = groups * seq_count
    length = running_forget_gate.shape[1]
    place = lax.axis_index("sp")
    col_start = lax.axis_index("tp") * cols + lax.axis_index("fs") * lanes

    here, side = lax.axis_index("fs"), lax.axis_index("tp").astype(jnp.int32)
    at = jnp.stack((side, here)).astype(jnp.int32)
    mine = exchange(
        packed(
            (inputs.reshape(rows, half_width),),
            (softmax_query_matrix, softmax_key_matrix, softmax_value_matrix),
            groups,
        ),
        "fs",
    )
    lin_sent = packed((), (receptance_weight, linear_key_weight, linear_value_weight), groups)
    mine, lin_sent = lax.optimization_barrier((mine, in_turn(lin_sent, "fs")))
    lin_sent = by_permutes(lin_sent, "fs")

    pair_seq, pair_head = place // heads, lax.rem(place, heads)
    pair_group, pair_slot = pair_seq // seq_count, lax.rem(pair_seq, seq_count)

    def of_pair(table, head_dim):
        table = lax.dynamic_index_in_dim(table, pair_slot, 0, False)
        shape = table.shape
        table = table.reshape(*shape[:head_dim], groups, heads, *shape[head_dim + 1 :])
        return lax.dynamic_index_in_dim(table, pair_head, head_dim + 1, False)

    state = of_pair(starting_state, 0)
    state = jnp.concatenate((state[:, : n // 2], state[:, n // 2 :]), 2)
    gates = of_pair(running_forget_gate, 1).T.reshape(groups, length // tok_count, tok_count)
    extra = decay_extra_log.reshape(seq_count, tok_count, groups, heads).transpose(2, 0, 3, 1)
    extra = extra.reshape(groups, seq_count * heads, tok_count)
    small = in_turn(jnp.concatenate((state, gates, extra), 1), "fs")
    small = jnp.stack(by_permutes(small, "fs"))
    half, after = n // 2, n // 2 + length // tok_count

    def small_from(group):
        return lax.dynamic_index_in_dim(small, lax.rem(here + groups - group, groups), 0, False)

    extra = jnp.concatenate([small_from(g)[after:] for g in range(groups)], 0)
    extra = extra.reshape(seqs, heads, tok_count)
    pair = small_from(pair_group)
    start, gate = pair[:half], pair[half:after]

    def own_columns(table, axis):
        return lax.dynamic_slice_in_dim(table, col_start, lanes, axis)

    def own_first(table, axis):
        return jnp.where(side == 0, table, jnp.roll(table, half_width, axis))

    swap = [(i, tp - 1 - i) for i in range(tp)]
    other = lax.ppermute(mine[:, :, :half_width], "tp", swap)
    fox, normed = fox_projections(
        at, mine, other, own_first(input_norm_gain.reshape(1, -1), 1), tok_count
    )
    fox = exchange(fox, "sp")
    lin, logged, rate = lin_projections(
        at,
        normed,
        own_first(jnp.concatenate((decay_lower_map, rate_lower_map), 1), 0),
        own_columns(decay_upper_map, 1),
        own_columns(rate_upper_map, 1),
        jnp.stack((own_columns(decay_offset_base, 0), own_columns(rate_offset_base, 0))),
        lin_sent,
    )
    query, ready, maps = position_maps(lin, logged, rate, extra)
    maps, fox = lax.optimization_barrier((maps, fox))
    maps = exchange(maps, "sp")
    fox_out = attention(fox, gate)
    back = exchange(states_ahead(maps, start, fox_out), "sp")
    gain = own_columns(linear_head_gain, 0).reshape(1, lanes)
    acts = exchange(heads_out(back, query, ready, gain, groups), "fs")
    weights = (softmax_output_weight, linear_output_weight)
    theirs = closing((tp - 1 - side).reshape(1), tp, acts, *weights)
    theirs = lax.ppermute(theirs, "tp", swap)
    own = closing(side.reshape(1), tp, acts, *weights)
    mixed = (own.astype(F32) + theirs.astype(F32)).reshape(seq_count // tp, tok_count, -1)
    return mixed.astype(BF16)


def solution(mesh):
    placed = (
        P(("grp", "fs"), "sp", "tp"),
        P(),
        P("fs", "tp"),
        P("fs", "tp"),
        P("fs", "tp"),
        P(("grp", "fs"), None, "tp"),
        P("fs", "tp"),
        P("fs", "tp"),
        P("fs", "tp"),
        P(),
        P(),
        P(),
        P(("grp", "fs"), "sp", "tp"),
        P(),
        P(),
        P(),
        P(),
        P(("grp", "fs"), "tp", None, None),
        P(None, "tp"),
        P(None, "tp"),
    )

    return jax.shard_map(
        per_device,
        mesh=mesh,
        in_specs=placed,
        out_specs=P(("grp", "fs", "tp"), "sp", None),
        check_vma=False,
    )
```

```python
import functools

import jax
import jax.numpy as jnp
from jax import lax
from jax.experimental import pallas as pl
from jax.experimental.pallas import tpu as pltpu
from jax.sharding import PartitionSpec as P

HEAD_CHANNELS = 64
CHUNK = 64
F32 = jnp.float32
BF16 = jnp.bfloat16
MIB = 1024 * 1024
VMEM_BYTES = 56 * MIB

MM = (((1,), (0,)), ((), ()))
NT = (((1,), (1,)), ((), ()))
TN = (((0,), (0,)), ((), ()))


def mul(left, right, dims=MM):
    return lax.dot_general(
        left.astype(BF16), right.astype(BF16), dims, preferred_element_type=F32
    )


def places(shape, dim):
    return lax.broadcasted_iota(jnp.int32, shape, dim)


def attention_kernel(blocks_ref, gate_ref, out_ref, key_scr, value_scr):
    count, _, width = blocks_ref.shape
    channels = HEAD_CHANNELS
    for i in range(count):
        gate = gate_ref[i : i + 1, :]
        high = gate.astype(BF16).astype(F32)
        rest = gate - high
        middle = rest.astype(BF16).astype(F32)
        low = rest - middle
        row = places((channels, width), 0)
        extra = jnp.where(row == 0, high, jnp.where(row == 1, middle, jnp.where(row == 2, low, 0.0)))
        key_rows = blocks_ref[i, channels : 2 * channels, :].astype(F32)
        key_scr[i * width : (i + 1) * width, :] = jnp.concatenate((key_rows, extra), 0).T.astype(BF16)
        value_scr[:, i * width : (i + 1) * width] = blocks_ref[i, 2 * channels :, :]
    step = 2 * width
    row = places((channels, step), 0)
    tail = jnp.where(row < 3, -1.0, 0.0).astype(BF16)
    live = places((step, step), 0) <= places((step, step), 1)
    for i in range(count // 2):
        query = jnp.concatenate(
            (blocks_ref[2 * i, :channels, :], blocks_ref[2 * i + 1, :channels, :]), 1
        )
        query = (query.astype(F32) * channels ** (-0.5)).astype(BF16)
        query = jnp.concatenate((query, tail), 0)
        before = i * step
        own = lax.dot_general(
            key_scr[before : before + step, :], query, MM, preferred_element_type=F32
        )
        own = jnp.where(live, own, -1e30)
        top = jnp.max(own, axis=0, keepdims=True)
        if before:
            past = lax.dot_general(key_scr[:before, :], query, MM, preferred_element_type=F32)
            top = jnp.maximum(top, jnp.max(past, axis=0, keepdims=True))
        weight = jnp.exp(own - top)
        total = jnp.sum(weight, axis=0, keepdims=True)
        mixed = lax.dot_general(
            value_scr[:, before : before + step],
            weight.astype(BF16),
            MM,
            preferred_element_type=F32,
        )
        if before:
            weight = jnp.exp(past - top)
            total = total + jnp.sum(weight, axis=0, keepdims=True)
            mixed = mixed + lax.dot_general(
                value_scr[:, :before], weight.astype(BF16), MM, preferred_element_type=F32
            )
        mixed = (mixed / total).astype(BF16)
        out_ref[2 * i] = mixed[:, :width]
        out_ref[2 * i + 1] = mixed[:, width:]


def attention(blocks, gate):
    count, rows, width = blocks.shape
    whole = pl.BlockSpec(memory_space=pltpu.VMEM)
    return pl.pallas_call(
        attention_kernel,
        out_shape=jax.ShapeDtypeStruct((count, HEAD_CHANNELS, width), BF16),
        in_specs=[whole, whole],
        out_specs=whole,
        scratch_shapes=[
            pltpu.VMEM((count * width, 2 * HEAD_CHANNELS), BF16),
            pltpu.VMEM((HEAD_CHANNELS, count * width), BF16),
        ],
        compiler_params=pltpu.CompilerParams(vmem_limit_bytes=16 * MIB),
        cost_estimate=pl.CostEstimate(
            flops=4 * HEAD_CHANNELS * (count * width) ** 2,
            bytes_accessed=4 * count * rows * width,
            transcendentals=(count * width) ** 2 // 2,
        ),
        name="attention",
    )(blocks, gate)


def chunk_masks(size):
    row, col = places((2 * size, 2 * size), 0), places((2 * size, 2 * size), 1)
    same = row // CHUNK == col // CHUNK
    return row, col, same


def maps_kernel(proj_ref, log_ref, rate_ref, extra_ref, q_ref, o_ref, maps_ref):
    seqs, _, size = extra_ref.shape
    lanes = 2 * HEAD_CHANNELS
    row, col, same = chunk_masks(size)
    strict = same & (row > col)
    upto = same & (row >= col)
    merges = []
    block = 2
    while block < CHUNK:
        merges.append((row // (2 * block) == col // (2 * block)) & (row // block > col // block))
        block *= 2
    pairs_of_two = (row // 2 == col // 2) & (row > col)
    identity = (row == col).astype(F32)
    lane = places((size, lanes), 1)
    first_head = lane < HEAD_CHANNELS
    head_block = (places((lanes, lanes), 0) < HEAD_CHANNELS) == (
        places((lanes, lanes), 1) < HEAD_CHANNELS
    )
    diagonal = places((lanes, lanes), 0) == places((lanes, lanes), 1)
    small_row, small_col = places((size, size), 0), places((size, size), 1)
    running = ((small_row // CHUNK == small_col // CHUNK) & (small_row >= small_col)).astype(F32)
    head_sum = head_block.astype(F32)
    tops, bottoms = slice(0, CHUNK), slice(CHUNK, 2 * CHUNK)

    def stacked(values):
        return jnp.concatenate(
            (jnp.where(first_head, values, 0.0), jnp.where(first_head, 0.0, values)), 0
        )

    def each_chunk(values, at):
        return jnp.concatenate(
            [jnp.broadcast_to(values[c + at : c + at + 1], (CHUNK, lanes)) for c in (0, CHUNK)], 0
        )

    held = []
    for p in range(seqs):
        at = slice(p * size, (p + 1) * size)
        rec = proj_ref[at, :lanes].astype(F32)
        key = proj_ref[at, lanes : 2 * lanes].astype(F32)
        value = proj_ref[at, 2 * lanes :].astype(F32)
        by_head = [
            jnp.broadcast_to(extra_ref[p, k : k + 1, :], (HEAD_CHANNELS, size)) for k in range(2)
        ]
        logged = log_ref[at, :] + jnp.concatenate(by_head, 0).T
        squares = lax.dot_general(
            key * key, head_sum, MM, precision=lax.Precision.HIGHEST, preferred_element_type=F32
        )
        unit = key * lax.rsqrt(squares + 1e-06)
        beta = unit * rate_ref[at, :]
        total = lax.dot_general(
            running, logged, MM, precision=lax.Precision.HIGHEST, preferred_element_type=F32
        )
        middle = each_chunk(total, CHUNK // 2 - 1)
        ending = each_chunk(total, CHUNK - 1)
        previous = total - logged
        fall = jnp.exp(middle - total)
        to_end = jnp.exp(ending - total)
        zeta = -unit
        left = jnp.concatenate(
            (stacked(zeta * jnp.exp(previous - middle)), stacked(rec * jnp.exp(total - middle))), 0
        )
        right = jnp.concatenate((beta * fall, key * fall), 0)
        held.append(
            dict(
                grams=mul(left, right, NT),
                zeta_true=zeta * jnp.exp(previous),
                rec_true=rec * jnp.exp(total),
                beta_end=beta * to_end,
                key_end=key * to_end,
                value=value,
                ending=jnp.exp(total),
            )
        )
    for h in held:
        grams = h.pop("grams")
        blank = jnp.zeros((size, size), F32)

        def spread(first, second, mask):
            both = jnp.concatenate(
                (
                    jnp.concatenate((first, blank), 1),
                    jnp.concatenate((blank, second), 1),
                ),
                0,
            )
            return jnp.where(mask, both, 0.0).astype(BF16)

        h["zb"] = spread(grams[:size, :size], grams[size : 2 * size, :size], strict)
        h["zk"] = spread(grams[:size, size:], grams[size : 2 * size, size:], strict)
        h["rb"] = spread(grams[2 * size : 3 * size, :size], grams[3 * size :, :size], upto)
        h["rk"] = spread(grams[2 * size : 3 * size, size:], grams[3 * size :, size:], upto)
        h["inverse"] = identity + jnp.where(pairs_of_two, h["zb"].astype(F32), 0.0)
        h["from_values"] = mul(
            jnp.concatenate((h["zk"], h["rk"]), 0), stacked(h["value"])
        )
    for merge in merges:
        for h in held:
            inner = mul(jnp.where(merge, h["zb"].astype(F32), 0.0), h["inverse"])
            h["inner"] = inner
        for h in held:
            h["inverse"] = h["inverse"] + mul(h["inverse"], h["inner"])
    for h in held:
        right = jnp.concatenate((stacked(h["zeta_true"]), h["from_values"][: 2 * size]), 1)
        h["pulled"] = mul(h["inverse"], right)
    for p, h in enumerate(held):
        start = jnp.concatenate((stacked(h["rec_true"]), h["from_values"][2 * size :]), 1)
        seen = start + mul(h["rb"], h["pulled"])
        seen = seen[:size] + seen[size:]
        pulled = h["pulled"][:size] + h["pulled"][size:]
        query, ready = seen[:, :lanes], seen[:, lanes:]
        maps = []
        for part, last in ((tops, CHUNK - 1), (bottoms, 2 * CHUNK - 1)):
            moved = mul(pulled[part], h["beta_end"][part], TN)
            added = mul(h["value"][part], h["key_end"][part], TN)
            kept = jnp.where(diagonal, h["ending"][last : last + 1], 0.0)
            maps.append(
                (
                    kept + jnp.where(head_block, moved[:lanes], 0.0),
                    jnp.where(head_block, moved[lanes:] + added, 0.0),
                )
            )
        both = mul(jnp.concatenate(maps[0], 0), maps[1][0])
        carry = both[:lanes]
        offset = both[lanes:] + maps[1][1]
        later = mul(query[bottoms], jnp.concatenate(maps[0], 0), NT)
        query = jnp.concatenate((query[tops], later[:, :lanes]), 0)
        ready = jnp.concatenate((ready[tops], ready[bottoms] + later[:, lanes:]), 0)
        at = slice(p * size, (p + 1) * size)
        q_ref[at, :] = query.astype(BF16)
        o_ref[at, :] = ready
        half = places((HEAD_CHANNELS, lanes), 1) < HEAD_CHANNELS
        turned_offset = pltpu.roll(offset, HEAD_CHANNELS, 1)
        turned_carry = pltpu.roll(carry, HEAD_CHANNELS, 1)
        maps_ref[2 * p] = jnp.where(
            half, carry[:HEAD_CHANNELS], turned_offset[:HEAD_CHANNELS]
        ).astype(BF16)
        maps_ref[2 * p + 1] = jnp.where(
            half, turned_carry[HEAD_CHANNELS:], offset[HEAD_CHANNELS:]
        ).astype(BF16)


def position_maps(proj, logged, rate, extra):
    seqs, heads, tok_count = extra.shape
    rows, lanes = logged.shape
    group = seqs // 2
    return pl.pallas_call(
        maps_kernel,
        grid=(seqs // group,),
        out_shape=(
            jax.ShapeDtypeStruct((rows, lanes), BF16),
            jax.ShapeDtypeStruct((rows, lanes), F32),
            jax.ShapeDtypeStruct((seqs * heads, HEAD_CHANNELS, lanes), BF16),
        ),
        in_specs=[
            pl.BlockSpec((group * tok_count, 3 * lanes), lambda s: (s, 0)),
            pl.BlockSpec((group * tok_count, lanes), lambda s: (s, 0)),
            pl.BlockSpec((group * tok_count, lanes), lambda s: (s, 0)),
            pl.BlockSpec((group, heads, tok_count), lambda s: (s, 0, 0)),
        ],
        out_specs=(
            pl.BlockSpec((group * tok_count, lanes), lambda s: (s, 0)),
            pl.BlockSpec((group * tok_count, lanes), lambda s: (s, 0)),
            pl.BlockSpec((group * heads, HEAD_CHANNELS, lanes), lambda s: (s, 0, 0)),
        ),
        compiler_params=pltpu.CompilerParams(vmem_limit_bytes=24 * MIB),
        cost_estimate=pl.CostEstimate(
            flops=rows * lanes * 2 * 256 * 20,
            bytes_accessed=rows * lanes * 20,
            transcendentals=6 * rows * lanes,
        ),
        name="position_maps",
    )(proj, logged, rate, extra)


def states_kernel(maps_ref, start_ref, fox_ref, out_ref):
    count = maps_ref.shape[0]
    n = HEAD_CHANNELS
    out_ref[:, :n, :] = fox_ref[...]
    state = jnp.concatenate((start_ref[:, :n], start_ref[:, n:]), 0)
    for i in range(count):
        out_ref[i, n:, :] = jnp.concatenate((state[: n // 2], state[n // 2 :]), 1).astype(BF16)
        if i + 1 < count:
            pair = maps_ref[i]
            high = state.astype(BF16)
            low = (state - high.astype(F32)).astype(BF16)
            moved = mul(jnp.concatenate((high, low), 0), pair[:, :n])
            state = moved[:n] + moved[n:] + pair[:, n:].astype(F32)


def states_ahead(maps, start, fox):
    count = maps.shape[0]
    whole = pl.BlockSpec(memory_space=pltpu.VMEM)
    return pl.pallas_call(
        states_kernel,
        out_shape=jax.ShapeDtypeStruct((count, 3 * HEAD_CHANNELS // 2, 2 * HEAD_CHANNELS), BF16),
        in_specs=[whole, whole, whole],
        out_specs=whole,
        compiler_params=pltpu.CompilerParams(vmem_limit_bytes=16 * MIB),
        cost_estimate=pl.CostEstimate(
            flops=count * 4 * HEAD_CHANNELS**3, bytes_accessed=1 << 19, transcendentals=0
        ),
        name="states_ahead",
    )(maps, start, fox)


def pack_kernel(groups, *refs):
    *piece_refs, out_ref, sems = refs
    leading, weights = piece_refs[:-3], piece_refs[-3:]
    rows = out_ref.shape[1]
    lanes = weights[0].shape[1] // groups
    copies = []

    def send(source, group, at, width):
        copies.append(
            pltpu.make_async_copy(
                source, out_ref.at[group, :, at : at + width], sems.at[len(copies)]
            )
        )

    for g in range(groups):
        at = 0
        for ref in leading:
            send(ref, g, at, ref.shape[1])
            at += ref.shape[1]
        for k in range(2):
            for ref in weights:
                block = ref.at[k * rows : (k + 1) * rows, g * lanes : (g + 1) * lanes]
                send(block, g, at, lanes)
                at += lanes
    for copy in copies:
        copy.start()
    for copy in copies:
        copy.wait()


def packed(leading, weights, groups):
    rows, cols = weights[0].shape
    width = sum(x.shape[1] for x in leading) + 6 * cols // groups
    whole = pl.BlockSpec(memory_space=pltpu.VMEM)
    return pl.pallas_call(
        functools.partial(pack_kernel, groups),
        out_shape=jax.ShapeDtypeStruct((groups, rows // 2, width), BF16),
        in_specs=[whole] * (len(leading) + 3),
        out_specs=pl.BlockSpec(memory_space=pl.ANY),
        scratch_shapes=[pltpu.SemaphoreType.DMA((groups * (len(leading) + 6),))],
        compiler_params=pltpu.CompilerParams(vmem_limit_bytes=VMEM_BYTES),
        cost_estimate=pl.CostEstimate(
            flops=1 << 20, bytes_accessed=4 * groups * rows * width, transcendentals=0
        ),
        name="packed",
    )(*leading, *weights)


def fox_kernel(
    at_ref,
    mine_ref,
    other_ref,
    first_ref,
    second_ref,
    third_ref,
    gain_ref,
    fox_ref,
    normed_ref,
    weight_scr,
):
    n = HEAD_CHANNELS
    groups = first_ref.shape[0]
    _, rows, width = other_ref.shape
    pairs, _, tok_count = fox_ref.shape
    heads = pairs * tok_count // rows
    lanes = heads * n

    @pl.when(pl.program_id(0) == 0)
    def _():
        for i in range(groups):
            source = lax.rem(i + at_ref[0] * (groups // 2), groups)
            upper = slice(2 * i * rows, (2 * i + 1) * rows)
            lower = slice((2 * i + 1) * rows, (2 * i + 2) * rows)
            weight_scr[upper, : 2 * lanes] = first_ref[source]
            weight_scr[upper, 2 * lanes :] = second_ref[source, :, :lanes]
            weight_scr[lower, :lanes] = second_ref[source, :, lanes:]
            weight_scr[lower, lanes:] = third_ref[source]

    pieces = [mine_ref[0].astype(F32), other_ref[0].astype(F32)]
    square = sum(jnp.sum(x * x, axis=1, keepdims=True) for x in pieces)
    scaling = lax.rsqrt(square / (2 * width) + 1e-06)
    normed = jnp.concatenate(
        [
            (x * scaling * gain_ref[:, i * width : (i + 1) * width].astype(F32)).astype(BF16)
            for i, x in enumerate(pieces)
        ],
        1,
    )
    normed_ref[...] = normed
    fox = lax.dot_general(normed, weight_scr[...], MM, preferred_element_type=F32)
    for s in range(rows // tok_count):
        here = slice(s * tok_count, (s + 1) * tok_count)
        for k in range(3):
            turned = fox[here, k * lanes : (k + 1) * lanes].T.astype(BF16)
            for h in range(heads):
                fox_ref[s * heads + h, k * n : (k + 1) * n, :] = turned[h * n : (h + 1) * n]


def fox_projections(at, mine, other, gain, tok_count):
    groups, rows, width = other.shape
    lanes = (mine.shape[2] - width) // 6
    heads = lanes // HEAD_CHANNELS
    pairs = rows // tok_count * heads
    whole = pl.BlockSpec(memory_space=pltpu.VMEM)
    return pl.pallas_call(
        fox_kernel,
        grid=(groups,),
        out_shape=(
            jax.ShapeDtypeStruct((groups * pairs, 3 * HEAD_CHANNELS, tok_count), BF16),
            jax.ShapeDtypeStruct((groups * rows, 2 * width), BF16),
        ),
        in_specs=[
            pl.BlockSpec(memory_space=pltpu.SMEM),
            pl.BlockSpec((1, rows, width), lambda g: (g, 0, 0)),
            pl.BlockSpec((1, rows, width), lambda g: (g, 0, 0)),
            *(
                pl.BlockSpec((groups, rows, 2 * lanes), lambda g, at=at: (0, 0, at))
                for at in range(width // (2 * lanes), width // (2 * lanes) + 3)
            ),
            whole,
        ],
        out_specs=(
            pl.BlockSpec((pairs, 3 * HEAD_CHANNELS, tok_count), lambda g: (g, 0, 0)),
            pl.BlockSpec((rows, 2 * width), lambda g: (g, 0)),
        ),
        scratch_shapes=[pltpu.VMEM((2 * width, 3 * lanes), BF16)],
        compiler_params=pltpu.CompilerParams(vmem_limit_bytes=24 * MIB),
        cost_estimate=pl.CostEstimate(
            flops=12 * groups * rows * width * lanes,
            bytes_accessed=8 * groups * rows * width,
            transcendentals=0,
        ),
        name="fox_projections",
    )(at, mine, other, mine, mine, mine, gain)


def lin_kernel(at_ref, normed_ref, low_ref, decay_up_ref, rate_up_ref, base_ref, *rest):
    sent_refs, (lin_ref, log_ref, rate_ref, weight_scr) = rest[:-4], rest[-4:]
    groups = len(sent_refs)
    rows, both = sent_refs[0].shape
    lanes = both // 6

    @pl.when(pl.program_id(0) == 0)
    def _():
        for d, ref in enumerate(sent_refs):
            source = lax.rem(at_ref[1] + (groups - d), groups)
            place = lax.rem(source + at_ref[0] * (groups // 2), groups)
            for k in range(2):
                start = pl.multiple_of((2 * place + k) * rows, rows)
                weight_scr[pl.ds(start, rows), :] = ref[:, 3 * k * lanes : 3 * (k + 1) * lanes]

    normed = normed_ref[...]
    lin_ref[...] = lax.dot_general(
        normed, weight_scr[...], MM, preferred_element_type=F32
    ).astype(BF16)
    low = lax.dot_general(normed, low_ref[...], MM, preferred_element_type=F32)
    inner = low.shape[1] // 2
    decay = mul(jnp.tanh(low[:, :inner]), decay_up_ref[...]) + base_ref[0:1, :]
    log_ref[...] = jax.nn.sigmoid(decay) * -(2.718281828459045**-0.5)
    rate = mul(low[:, inner:], rate_up_ref[...]) + base_ref[1:2, :]
    rate_ref[...] = jax.nn.sigmoid(rate)


def lin_projections(at, normed, low, decay_up, rate_up, bases, sent):
    rows, width = normed.shape
    lanes = sent[0].shape[1] // 6
    tall = rows // 4
    whole = pl.BlockSpec(memory_space=pltpu.VMEM)
    return pl.pallas_call(
        lin_kernel,
        grid=(rows // tall,),
        out_shape=(
            jax.ShapeDtypeStruct((rows, 3 * lanes), BF16),
            jax.ShapeDtypeStruct((rows, lanes), F32),
            jax.ShapeDtypeStruct((rows, lanes), F32),
        ),
        in_specs=[
            pl.BlockSpec(memory_space=pltpu.SMEM),
            pl.BlockSpec((tall, width), lambda s: (s, 0)),
        ]
        + [whole] * (4 + len(sent)),
        out_specs=(
            pl.BlockSpec((tall, 3 * lanes), lambda s: (s, 0)),
            pl.BlockSpec((tall, lanes), lambda s: (s, 0)),
            pl.BlockSpec((tall, lanes), lambda s: (s, 0)),
        ),
        scratch_shapes=[pltpu.VMEM((width, 3 * lanes), BF16)],
        compiler_params=pltpu.CompilerParams(vmem_limit_bytes=24 * MIB),
        cost_estimate=pl.CostEstimate(
            flops=10 * rows * width * lanes,
            bytes_accessed=2 * rows * width,
            transcendentals=3 * rows * lanes,
        ),
        name="lin_projections",
    )(at, normed, low, decay_up, rate_up, bases, *sent)


def heads_kernel(back_ref, q_ref, o_ref, gain_ref, out_ref):
    n = HEAD_CHANNELS
    lanes = 2 * n
    pairs, _, tok_count = back_ref.shape
    _, rows, _ = out_ref.shape
    head_block = (places((lanes, lanes), 0) < n) == (places((lanes, lanes), 1) < n)
    average = jnp.where(head_block, 1.0 / n, 0.0).astype(BF16)
    first = places((n // 2, lanes), 1) < n
    gain = gain_ref[...].astype(F32)

    def mean(values):
        high = values.astype(BF16)
        low = (values - high.astype(F32)).astype(BF16)
        return mul(high, average) + mul(low, average)

    raws = []
    for s in range(pairs // 2):
        here = slice(s * tok_count, (s + 1) * tok_count)
        group, at = s * tok_count // rows, s * tok_count % rows
        fox = jnp.concatenate((back_ref[2 * s, :n, :], back_ref[2 * s + 1, :n, :]), 0)
        out_ref[group, at : at + tok_count, :lanes] = fox.astype(F32).T.astype(BF16)
        packed = [back_ref[2 * s + k, n:, :].astype(F32) for k in range(2)]
        turned = [pltpu.roll(x, n, 1) for x in packed]
        state = jnp.concatenate(
            (
                jnp.where(first, packed[0], 0.0),
                jnp.where(first, turned[0], 0.0),
                jnp.where(first, 0.0, turned[1]),
                jnp.where(first, 0.0, packed[1]),
            ),
            0,
        )
        raws.append(mul(q_ref[here, :], state, NT) + o_ref[here, :])
    centred = [raw - mean(raw) for raw in raws]
    spreads = [mean(x * x) for x in centred]
    for s, (x, spread) in enumerate(zip(centred, spreads)):
        group, at = s * tok_count // rows, s * tok_count % rows
        lin = x * lax.rsqrt(spread + 0.00064) * gain
        out_ref[group, at : at + tok_count, lanes:] = lin.astype(BF16)


def heads_out(back, query, ready, gain, groups):
    rows, lanes = query.shape
    whole = pl.BlockSpec(memory_space=pltpu.VMEM)
    return pl.pallas_call(
        heads_kernel,
        out_shape=jax.ShapeDtypeStruct((groups, rows // groups, 2 * lanes), BF16),
        in_specs=[whole] * 4,
        out_specs=whole,
        compiler_params=pltpu.CompilerParams(vmem_limit_bytes=16 * MIB),
        cost_estimate=pl.CostEstimate(
            flops=10 * rows * lanes * lanes, bytes_accessed=12 * rows * lanes, transcendentals=0
        ),
        name="heads_out",
    )(back, query, ready, gain)


def closing_kernel(seq_ref, acts_ref, fox_w_ref, lin_w_ref, out_ref, act_scr):
    groups, _, both = acts_ref.shape
    rows = act_scr.shape[0]
    lanes = both // 2
    cols = groups * lanes

    @pl.when(pl.program_id(0) == 0)
    def _():
        here = pl.ds(pl.multiple_of(seq_ref[0] * rows, rows), rows)
        for g in range(groups):
            act_scr[:, g * lanes : (g + 1) * lanes] = acts_ref[g, here, :lanes]
            act_scr[:, cols + g * lanes : cols + (g + 1) * lanes] = acts_ref[g, here, lanes:]

    turned = lax.dot_general(
        fox_w_ref[...], act_scr[:, :cols], NT, preferred_element_type=F32
    ) + lax.dot_general(lin_w_ref[...], act_scr[:, cols:], NT, preferred_element_type=F32)
    out_ref[...] = turned.T.astype(BF16)


def closing(part, parts, acts, fox_w, lin_w):
    _, rows, _ = acts.shape
    rows = rows // parts
    width, cols = fox_w.shape
    tile = 512
    return pl.pallas_call(
        closing_kernel,
        grid=(width // tile,),
        out_shape=jax.ShapeDtypeStruct((rows, width), BF16),
        in_specs=[
            pl.BlockSpec(memory_space=pltpu.SMEM),
            pl.BlockSpec(memory_space=pltpu.VMEM),
            pl.BlockSpec((tile, cols), lambda i: (i, 0)),
            pl.BlockSpec((tile, cols), lambda i: (i, 0)),
        ],
        out_specs=pl.BlockSpec((rows, tile), lambda i: (0, i)),
        scratch_shapes=[pltpu.VMEM((rows, 2 * cols), BF16)],
        compiler_params=pltpu.CompilerParams(vmem_limit_bytes=16 * MIB),
        cost_estimate=pl.CostEstimate(
            flops=4 * rows * cols * width,
            bytes_accessed=4 * cols * width + 2 * rows * width,
            transcendentals=0,
        ),
        name="closing",
    )(part, acts, fox_w, lin_w)


def exchange(x, axis):
    return lax.all_to_all(x, axis, 0, 0, tiled=True)


def in_turn(x, axis):
    size = lax.axis_size(axis)
    here = lax.axis_index(axis)
    return [lax.dynamic_index_in_dim(x, lax.rem(here + d, size), 0, False) for d in range(size)]


def by_permutes(blocks, axis):
    size = lax.axis_size(axis)
    return [
        lax.ppermute(block, axis, [(i, (i + d) % size) for i in range(size)]) if d else block
        for d, block in enumerate(blocks)
    ]


def per_device(
    inputs,
    input_norm_gain,
    softmax_query_matrix,
    softmax_key_matrix,
    softmax_value_matrix,
    running_forget_gate,
    receptance_weight,
    linear_key_weight,
    linear_value_weight,
    decay_lower_map,
    decay_upper_map,
    decay_offset_base,
    decay_extra_log,
    rate_lower_map,
    rate_upper_map,
    rate_offset_base,
    linear_head_gain,
    starting_state,
    softmax_output_weight,
    linear_output_weight,
):
    n = HEAD_CHANNELS
    seq_count, tok_count, half_width = inputs.shape
    rows = seq_count * tok_count
    cols = softmax_query_matrix.shape[1]
    groups, tp = lax.axis_size("fs"), lax.axis_size("tp")
    lanes = cols // groups
    heads = lanes // n
    seqs = groups * seq_count
    length = running_forget_gate.shape[1]
    place = lax.axis_index("sp")
    col_start = lax.axis_index("tp") * cols + lax.axis_index("fs") * lanes

    here, side = lax.axis_index("fs"), lax.axis_index("tp").astype(jnp.int32)
    at = jnp.stack((side, here)).astype(jnp.int32)
    mine = exchange(
        packed(
            (inputs.reshape(rows, half_width),),
            (softmax_query_matrix, softmax_key_matrix, softmax_value_matrix),
            groups,
        ),
        "fs",
    )
    lin_sent = packed((), (receptance_weight, linear_key_weight, linear_value_weight), groups)
    mine, lin_sent = lax.optimization_barrier((mine, in_turn(lin_sent, "fs")))
    lin_sent = by_permutes(lin_sent, "fs")

    pair_seq, pair_head = place // heads, lax.rem(place, heads)
    pair_group, pair_slot = pair_seq // seq_count, lax.rem(pair_seq, seq_count)

    def of_pair(table, head_dim):
        table = lax.dynamic_index_in_dim(table, pair_slot, 0, False)
        shape = table.shape
        table = table.reshape(*shape[:head_dim], groups, heads, *shape[head_dim + 1 :])
        return lax.dynamic_index_in_dim(table, pair_head, head_dim + 1, False)

    state = of_pair(starting_state, 0)
    state = jnp.concatenate((state[:, : n // 2], state[:, n // 2 :]), 2)
    gates = of_pair(running_forget_gate, 1).T.reshape(groups, length // tok_count, tok_count)
    extra = decay_extra_log.reshape(seq_count, tok_count, groups, heads).transpose(2, 0, 3, 1)
    extra = extra.reshape(groups, seq_count * heads, tok_count)
    small = in_turn(jnp.concatenate((state, gates, extra), 1), "fs")
    small = jnp.stack(by_permutes(small, "fs"))
    half, after = n // 2, n // 2 + length // tok_count

    def small_from(group):
        return lax.dynamic_index_in_dim(small, lax.rem(here + groups - group, groups), 0, False)

    extra = jnp.concatenate([small_from(g)[after:] for g in range(groups)], 0)
    extra = extra.reshape(seqs, heads, tok_count)
    pair = small_from(pair_group)
    start, gate = pair[:half], pair[half:after]

    def own_columns(table, axis):
        return lax.dynamic_slice_in_dim(table, col_start, lanes, axis)

    def own_first(table, axis):
        return jnp.where(side == 0, table, jnp.roll(table, half_width, axis))

    swap = [(i, tp - 1 - i) for i in range(tp)]
    other = lax.ppermute(mine[:, :, :half_width], "tp", swap)
    fox, normed = fox_projections(
        at, mine, other, own_first(input_norm_gain.reshape(1, -1), 1), tok_count
    )
    fox = exchange(fox, "sp")
    lin, logged, rate = lin_projections(
        at,
        normed,
        own_first(jnp.concatenate((decay_lower_map, rate_lower_map), 1), 0),
        own_columns(decay_upper_map, 1),
        own_columns(rate_upper_map, 1),
        jnp.stack((own_columns(decay_offset_base, 0), own_columns(rate_offset_base, 0))),
        lin_sent,
    )
    query, ready, maps = position_maps(lin, logged, rate, extra)
    maps, fox = lax.optimization_barrier((maps, fox))
    maps = exchange(maps, "sp")
    fox_out = attention(fox, gate)
    back = exchange(states_ahead(maps, start, fox_out), "sp")
    gain = own_columns(linear_head_gain, 0).reshape(1, lanes)
    acts = exchange(heads_out(back, query, ready, gain, groups), "fs")
    weights = (softmax_output_weight, linear_output_weight)
    theirs = closing((tp - 1 - side).reshape(1), tp, acts, *weights)
    theirs = lax.ppermute(theirs, "tp", swap)
    own = closing(side.reshape(1), tp, acts, *weights)
    mixed = (own.astype(F32) + theirs.astype(F32)).reshape(seq_count // tp, tok_count, -1)
    return mixed.astype(BF16)


def solution(mesh):
    placed = (
        P(("grp", "fs"), "sp", "tp"),
        P(),
        P("fs", "tp"),
        P("fs", "tp"),
        P("fs", "tp"),
        P(("grp", "fs"), None, "tp"),
        P("fs", "tp"),
        P("fs", "tp"),
        P("fs", "tp"),
        P(),
        P(),
        P(),
        P(("grp", "fs"), "sp", "tp"),
        P(),
        P(),
        P(),
        P(),
        P(("grp", "fs"), "tp", None, None),
        P(None, "tp"),
        P(None, "tp"),
    )

    return jax.shard_map(
        per_device,
        mesh=mesh,
        in_specs=placed,
        out_specs=P(("grp", "fs", "tp"), "sp", None),
        check_vma=False,
    )
```

```python
import functools

import jax
import jax.numpy as jnp
from jax import lax
from jax.experimental import pallas as pl
from jax.experimental.pallas import tpu as pltpu
from jax.sharding import PartitionSpec as P

HEAD_CHANNELS = 64
CHUNK = 64
F32 = jnp.float32
BF16 = jnp.bfloat16
MIB = 1024 * 1024
VMEM_BYTES = 56 * MIB

MM = (((1,), (0,)), ((), ()))
NT = (((1,), (1,)), ((), ()))
TN = (((0,), (0,)), ((), ()))


def mul(left, right, dims=MM):
    return lax.dot_general(
        left.astype(BF16), right.astype(BF16), dims, preferred_element_type=F32
    )


def places(shape, dim):
    return lax.broadcasted_iota(jnp.int32, shape, dim)


def attention_kernel(blocks_ref, gate_ref, out_ref, key_scr, value_scr):
    count, _, width = blocks_ref.shape
    channels = HEAD_CHANNELS
    for i in range(count):
        gate = gate_ref[i : i + 1, :]
        high = gate.astype(BF16).astype(F32)
        rest = gate - high
        middle = rest.astype(BF16).astype(F32)
        low = rest - middle
        row = places((channels, width), 0)
        extra = jnp.where(row == 0, high, jnp.where(row == 1, middle, jnp.where(row == 2, low, 0.0)))
        key_rows = blocks_ref[i, channels : 2 * channels, :].astype(F32)
        key_scr[i * width : (i + 1) * width, :] = jnp.concatenate((key_rows, extra), 0).T.astype(BF16)
        value_scr[:, i * width : (i + 1) * width] = blocks_ref[i, 2 * channels :, :]
    step = 2 * width
    row = places((channels, step), 0)
    tail = jnp.where(row < 3, -1.0, 0.0).astype(BF16)
    live = places((step, step), 0) <= places((step, step), 1)
    for i in range(count // 2):
        query = jnp.concatenate(
            (blocks_ref[2 * i, :channels, :], blocks_ref[2 * i + 1, :channels, :]), 1
        )
        query = (query.astype(F32) * channels ** (-0.5)).astype(BF16)
        query = jnp.concatenate((query, tail), 0)
        before = i * step
        own = lax.dot_general(
            key_scr[before : before + step, :], query, MM, preferred_element_type=F32
        )
        own = jnp.where(live, own, -1e30)
        top = jnp.max(own, axis=0, keepdims=True)
        if before:
            past = lax.dot_general(key_scr[:before, :], query, MM, preferred_element_type=F32)
            top = jnp.maximum(top, jnp.max(past, axis=0, keepdims=True))
        weight = jnp.exp(own - top)
        total = jnp.sum(weight, axis=0, keepdims=True)
        mixed = lax.dot_general(
            value_scr[:, before : before + step],
            weight.astype(BF16),
            MM,
            preferred_element_type=F32,
        )
        if before:
            weight = jnp.exp(past - top)
            total = total + jnp.sum(weight, axis=0, keepdims=True)
            mixed = mixed + lax.dot_general(
                value_scr[:, :before], weight.astype(BF16), MM, preferred_element_type=F32
            )
        mixed = (mixed / total).astype(BF16)
        out_ref[2 * i] = mixed[:, :width]
        out_ref[2 * i + 1] = mixed[:, width:]


def attention(blocks, gate):
    count, rows, width = blocks.shape
    whole = pl.BlockSpec(memory_space=pltpu.VMEM)
    return pl.pallas_call(
        attention_kernel,
        out_shape=pltpu.HBM((count, HEAD_CHANNELS, width), BF16),
        in_specs=[whole, whole],
        out_specs=whole,
        scratch_shapes=[
            pltpu.VMEM((count * width, 2 * HEAD_CHANNELS), BF16),
            pltpu.VMEM((HEAD_CHANNELS, count * width), BF16),
        ],
        compiler_params=pltpu.CompilerParams(vmem_limit_bytes=16 * MIB),
        cost_estimate=pl.CostEstimate(
            flops=4 * HEAD_CHANNELS * (count * width) ** 2,
            bytes_accessed=4 * count * rows * width,
            transcendentals=(count * width) ** 2 // 2,
        ),
        name="attention",
    )(blocks, gate)


def chunk_masks(size):
    row, col = places((2 * size, 2 * size), 0), places((2 * size, 2 * size), 1)
    same = row // CHUNK == col // CHUNK
    return row, col, same


def maps_kernel(proj_ref, log_ref, rate_ref, extra_ref, q_ref, o_ref, maps_ref):
    seqs, _, size = extra_ref.shape
    lanes = 2 * HEAD_CHANNELS
    row, col, same = chunk_masks(size)
    strict = same & (row > col)
    upto = same & (row >= col)
    merges = []
    block = 2
    while block < CHUNK:
        merges.append((row // (2 * block) == col // (2 * block)) & (row // block > col // block))
        block *= 2
    pairs_of_two = (row // 2 == col // 2) & (row > col)
    identity = (row == col).astype(F32)
    lane = places((size, lanes), 1)
    first_head = lane < HEAD_CHANNELS
    head_block = (places((lanes, lanes), 0) < HEAD_CHANNELS) == (
        places((lanes, lanes), 1) < HEAD_CHANNELS
    )
    diagonal = places((lanes, lanes), 0) == places((lanes, lanes), 1)
    small_row, small_col = places((size, size), 0), places((size, size), 1)
    running = ((small_row // CHUNK == small_col // CHUNK) & (small_row >= small_col)).astype(F32)
    head_sum = head_block.astype(F32)
    tops, bottoms = slice(0, CHUNK), slice(CHUNK, 2 * CHUNK)

    def stacked(values):
        return jnp.concatenate(
            (jnp.where(first_head, values, 0.0), jnp.where(first_head, 0.0, values)), 0
        )

    def each_chunk(values, at):
        return jnp.concatenate(
            [jnp.broadcast_to(values[c + at : c + at + 1], (CHUNK, lanes)) for c in (0, CHUNK)], 0
        )

    held = []
    for p in range(seqs):
        at = slice(p * size, (p + 1) * size)
        rec = proj_ref[at, :lanes].astype(F32)
        key = proj_ref[at, lanes : 2 * lanes].astype(F32)
        value = proj_ref[at, 2 * lanes :].astype(F32)
        by_head = [
            jnp.broadcast_to(extra_ref[p, k : k + 1, :], (HEAD_CHANNELS, size)) for k in range(2)
        ]
        logged = log_ref[at, :] + jnp.concatenate(by_head, 0).T
        squares = lax.dot_general(
            key * key, head_sum, MM, precision=lax.Precision.HIGHEST, preferred_element_type=F32
        )
        unit = key * lax.rsqrt(squares + 1e-06)
        beta = unit * rate_ref[at, :]
        total = lax.dot_general(
            running, logged, MM, precision=lax.Precision.HIGHEST, preferred_element_type=F32
        )
        middle = each_chunk(total, CHUNK // 2 - 1)
        ending = each_chunk(total, CHUNK - 1)
        previous = total - logged
        fall = jnp.exp(middle - total)
        to_end = jnp.exp(ending - total)
        zeta = -unit
        left = jnp.concatenate(
            (stacked(zeta * jnp.exp(previous - middle)), stacked(rec * jnp.exp(total - middle))), 0
        )
        right = jnp.concatenate((beta * fall, key * fall), 0)
        held.append(
            dict(
                grams=mul(left, right, NT),
                zeta_true=zeta * jnp.exp(previous),
                rec_true=rec * jnp.exp(total),
                beta_end=beta * to_end,
                key_end=key * to_end,
                value=value,
                ending=jnp.exp(total),
            )
        )
    for h in held:
        grams = h.pop("grams")
        blank = jnp.zeros((size, size), F32)

        def spread(first, second, mask):
            both = jnp.concatenate(
                (
                    jnp.concatenate((first, blank), 1),
                    jnp.concatenate((blank, second), 1),
                ),
                0,
            )
            return jnp.where(mask, both, 0.0).astype(BF16)

        h["zb"] = spread(grams[:size, :size], grams[size : 2 * size, :size], strict)
        h["zk"] = spread(grams[:size, size:], grams[size : 2 * size, size:], strict)
        h["rb"] = spread(grams[2 * size : 3 * size, :size], grams[3 * size :, :size], upto)
        h["rk"] = spread(grams[2 * size : 3 * size, size:], grams[3 * size :, size:], upto)
        h["inverse"] = identity + jnp.where(pairs_of_two, h["zb"].astype(F32), 0.0)
        h["from_values"] = mul(
            jnp.concatenate((h["zk"], h["rk"]), 0), stacked(h["value"])
        )
    for merge in merges:
        for h in held:
            inner = mul(jnp.where(merge, h["zb"].astype(F32), 0.0), h["inverse"])
            h["inner"] = inner
        for h in held:
            h["inverse"] = h["inverse"] + mul(h["inverse"], h["inner"])
    for h in held:
        right = jnp.concatenate((stacked(h["zeta_true"]), h["from_values"][: 2 * size]), 1)
        h["pulled"] = mul(h["inverse"], right)
    for p, h in enumerate(held):
        start = jnp.concatenate((stacked(h["rec_true"]), h["from_values"][2 * size :]), 1)
        seen = start + mul(h["rb"], h["pulled"])
        seen = seen[:size] + seen[size:]
        pulled = h["pulled"][:size] + h["pulled"][size:]
        query, ready = seen[:, :lanes], seen[:, lanes:]
        maps = []
        for part, last in ((tops, CHUNK - 1), (bottoms, 2 * CHUNK - 1)):
            moved = mul(pulled[part], h["beta_end"][part], TN)
            added = mul(h["value"][part], h["key_end"][part], TN)
            kept = jnp.where(diagonal, h["ending"][last : last + 1], 0.0)
            maps.append(
                (
                    kept + jnp.where(head_block, moved[:lanes], 0.0),
                    jnp.where(head_block, moved[lanes:] + added, 0.0),
                )
            )
        both = mul(jnp.concatenate(maps[0], 0), maps[1][0])
        carry = both[:lanes]
        offset = both[lanes:] + maps[1][1]
        later = mul(query[bottoms], jnp.concatenate(maps[0], 0), NT)
        query = jnp.concatenate((query[tops], later[:, :lanes]), 0)
        ready = jnp.concatenate((ready[tops], ready[bottoms] + later[:, lanes:]), 0)
        at = slice(p * size, (p + 1) * size)
        q_ref[at, :] = query.astype(BF16)
        o_ref[at, :] = ready
        half = places((HEAD_CHANNELS, lanes), 1) < HEAD_CHANNELS
        turned_offset = pltpu.roll(offset, HEAD_CHANNELS, 1)
        turned_carry = pltpu.roll(carry, HEAD_CHANNELS, 1)
        maps_ref[2 * p] = jnp.where(
            half, carry[:HEAD_CHANNELS], turned_offset[:HEAD_CHANNELS]
        ).astype(BF16)
        maps_ref[2 * p + 1] = jnp.where(
            half, turned_carry[HEAD_CHANNELS:], offset[HEAD_CHANNELS:]
        ).astype(BF16)


def position_maps(proj, logged, rate, extra):
    seqs, heads, tok_count = extra.shape
    rows, lanes = logged.shape
    group = seqs // 2
    return pl.pallas_call(
        maps_kernel,
        grid=(seqs // group,),
        out_shape=(
            pltpu.HBM((rows, lanes), BF16),
            jax.ShapeDtypeStruct((rows, lanes), F32),
            jax.ShapeDtypeStruct((seqs * heads, HEAD_CHANNELS, lanes), BF16),
        ),
        in_specs=[
            pl.BlockSpec((group * tok_count, 3 * lanes), lambda s: (s, 0)),
            pl.BlockSpec((group * tok_count, lanes), lambda s: (s, 0)),
            pl.BlockSpec((group * tok_count, lanes), lambda s: (s, 0)),
            pl.BlockSpec((group, heads, tok_count), lambda s: (s, 0, 0)),
        ],
        out_specs=(
            pl.BlockSpec((group * tok_count, lanes), lambda s: (s, 0)),
            pl.BlockSpec((group * tok_count, lanes), lambda s: (s, 0)),
            pl.BlockSpec((group * heads, HEAD_CHANNELS, lanes), lambda s: (s, 0, 0)),
        ),
        compiler_params=pltpu.CompilerParams(vmem_limit_bytes=24 * MIB),
        cost_estimate=pl.CostEstimate(
            flops=rows * lanes * 2 * 256 * 20,
            bytes_accessed=rows * lanes * 20,
            transcendentals=6 * rows * lanes,
        ),
        name="position_maps",
    )(proj, logged, rate, extra)


def states_kernel(maps_ref, start_ref, fox_ref, out_ref):
    count = maps_ref.shape[0]
    n = HEAD_CHANNELS
    out_ref[:, :n, :] = fox_ref[...]
    state = jnp.concatenate((start_ref[:, :n], start_ref[:, n:]), 0)
    for i in range(count):
        out_ref[i, n:, :] = jnp.concatenate((state[: n // 2], state[n // 2 :]), 1).astype(BF16)
        if i + 1 < count:
            pair = maps_ref[i]
            high = state.astype(BF16)
            low = (state - high.astype(F32)).astype(BF16)
            moved = mul(jnp.concatenate((high, low), 0), pair[:, :n])
            state = moved[:n] + moved[n:] + pair[:, n:].astype(F32)


def states_ahead(maps, start, fox):
    count = maps.shape[0]
    whole = pl.BlockSpec(memory_space=pltpu.VMEM)
    return pl.pallas_call(
        states_kernel,
        out_shape=jax.ShapeDtypeStruct((count, 3 * HEAD_CHANNELS // 2, 2 * HEAD_CHANNELS), BF16),
        in_specs=[whole, whole, whole],
        out_specs=whole,
        compiler_params=pltpu.CompilerParams(vmem_limit_bytes=16 * MIB),
        cost_estimate=pl.CostEstimate(
            flops=count * 4 * HEAD_CHANNELS**3, bytes_accessed=1 << 19, transcendentals=0
        ),
        name="states_ahead",
    )(maps, start, fox)


def pack_kernel(groups, *refs):
    *piece_refs, out_ref, sems = refs
    leading, weights = piece_refs[:-3], piece_refs[-3:]
    _, _, rows, wide = out_ref.shape
    lanes = weights[0].shape[1] // groups
    copies = []

    def send(source, group, at):
        block, start = at // wide, at % wide
        target = out_ref.at[group, block, :, start : start + source.shape[1]]
        copies.append(pltpu.make_async_copy(source, target, sems.at[len(copies)]))

    for g in range(groups):
        at = 0
        for ref in leading:
            for start in range(0, ref.shape[1], wide):
                send(ref.at[:, start : start + wide], g, at)
                at += wide
        for k in range(2):
            for ref in weights:
                send(ref.at[k * rows : (k + 1) * rows, g * lanes : (g + 1) * lanes], g, at)
                at += lanes
    for copy in copies:
        copy.start()
    for copy in copies:
        copy.wait()


def packed(leading, weights, groups):
    rows, cols = weights[0].shape
    wide = 2 * cols // groups
    blocks = sum(x.shape[1] for x in leading) // wide + 3
    whole = pl.BlockSpec(memory_space=pltpu.VMEM)
    return pl.pallas_call(
        functools.partial(pack_kernel, groups),
        out_shape=jax.ShapeDtypeStruct((groups, blocks, rows // 2, wide), BF16),
        in_specs=[whole] * (len(leading) + 3),
        out_specs=pl.BlockSpec(memory_space=pl.ANY),
        scratch_shapes=[pltpu.SemaphoreType.DMA((groups * (blocks + 3),))],
        compiler_params=pltpu.CompilerParams(vmem_limit_bytes=VMEM_BYTES),
        cost_estimate=pl.CostEstimate(
            flops=1 << 20, bytes_accessed=2 * groups * blocks * rows * wide, transcendentals=0
        ),
        name="packed",
    )(*leading, *weights)


def fox_kernel(
    at_ref,
    mine_ref,
    other_ref,
    first_ref,
    second_ref,
    third_ref,
    gain_ref,
    fox_ref,
    normed_ref,
    weight_scr,
):
    n = HEAD_CHANNELS
    groups = first_ref.shape[0]
    _, blocks, rows, wide = other_ref.shape
    pairs, _, tok_count = fox_ref.shape
    heads = pairs * tok_count // rows
    lanes = heads * n

    @pl.when(pl.program_id(0) == 0)
    def _():
        for i in range(groups):
            source = lax.rem(i + at_ref[0] * (groups // 2), groups)
            upper = slice(2 * i * rows, (2 * i + 1) * rows)
            lower = slice((2 * i + 1) * rows, (2 * i + 2) * rows)
            weight_scr[upper, : 2 * lanes] = first_ref[source, 0]
            weight_scr[upper, 2 * lanes :] = second_ref[source, 0, :, :lanes]
            weight_scr[lower, :lanes] = second_ref[source, 0, :, lanes:]
            weight_scr[lower, lanes:] = third_ref[source, 0]

    pieces = [ref[0, i].astype(F32) for ref in (mine_ref, other_ref) for i in range(blocks)]
    square = sum(jnp.sum(x * x, axis=1, keepdims=True) for x in pieces)
    scaling = lax.rsqrt(square / (2 * blocks * wide) + 1e-06)
    normed = jnp.concatenate(
        [
            (x * scaling * gain_ref[:, i * wide : (i + 1) * wide].astype(F32)).astype(BF16)
            for i, x in enumerate(pieces)
        ],
        1,
    )
    normed_ref[...] = normed
    fox = lax.dot_general(normed, weight_scr[...], MM, preferred_element_type=F32)
    for s in range(rows // tok_count):
        here = slice(s * tok_count, (s + 1) * tok_count)
        for k in range(3):
            turned = fox[here, k * lanes : (k + 1) * lanes].T.astype(BF16)
            for h in range(heads):
                fox_ref[s * heads + h, k * n : (k + 1) * n, :] = turned[h * n : (h + 1) * n]


def fox_projections(at, mine, other, gain, tok_count):
    groups, blocks, rows, wide = other.shape
    width, lanes = blocks * wide, wide // 2
    heads = lanes // HEAD_CHANNELS
    pairs = rows // tok_count * heads
    whole = pl.BlockSpec(memory_space=pltpu.VMEM)
    return pl.pallas_call(
        fox_kernel,
        grid=(groups,),
        out_shape=(
            jax.ShapeDtypeStruct((groups * pairs, 3 * HEAD_CHANNELS, tok_count), BF16),
            pltpu.HBM((groups * rows, 2 * width), BF16),
        ),
        in_specs=[
            pl.BlockSpec(memory_space=pltpu.SMEM),
            pl.BlockSpec((1, blocks, rows, wide), lambda g: (g, 0, 0, 0)),
            pl.BlockSpec((1, blocks, rows, wide), lambda g: (g, 0, 0, 0)),
            *(
                pl.BlockSpec((groups, 1, rows, wide), lambda g, at=at: (0, at, 0, 0))
                for at in range(blocks, blocks + 3)
            ),
            whole,
        ],
        out_specs=(
            pl.BlockSpec((pairs, 3 * HEAD_CHANNELS, tok_count), lambda g: (g, 0, 0)),
            pl.BlockSpec((rows, 2 * width), lambda g: (g, 0)),
        ),
        scratch_shapes=[pltpu.VMEM((2 * width, 3 * lanes), BF16)],
        compiler_params=pltpu.CompilerParams(vmem_limit_bytes=24 * MIB),
        cost_estimate=pl.CostEstimate(
            flops=12 * groups * rows * width * lanes,
            bytes_accessed=8 * groups * rows * width,
            transcendentals=0,
        ),
        name="fox_projections",
    )(at, mine, other, mine, mine, mine, gain)


def lin_kernel(at_ref, normed_ref, low_ref, decay_up_ref, rate_up_ref, base_ref, *rest):
    sent_refs, (lin_ref, log_ref, rate_ref, weight_scr) = rest[:-4], rest[-4:]
    groups = len(sent_refs)
    _, rows, wide = sent_refs[0].shape
    lanes = wide // 2

    @pl.when(pl.program_id(0) == 0)
    def _():
        for d, ref in enumerate(sent_refs):
            source = lax.rem(at_ref[1] + (groups - d), groups)
            place = lax.rem(source + at_ref[0] * (groups // 2), groups)
            upper = pl.ds(pl.multiple_of(2 * place * rows, rows), rows)
            lower = pl.ds(pl.multiple_of((2 * place + 1) * rows, rows), rows)
            weight_scr[upper, : 2 * lanes] = ref[0]
            weight_scr[upper, 2 * lanes :] = ref[1, :, :lanes]
            weight_scr[lower, :lanes] = ref[1, :, lanes:]
            weight_scr[lower, lanes:] = ref[2]

    normed = normed_ref[...]
    lin_ref[...] = lax.dot_general(
        normed, weight_scr[...], MM, preferred_element_type=F32
    ).astype(BF16)
    low = lax.dot_general(normed, low_ref[...], MM, preferred_element_type=F32)
    inner = low.shape[1] // 2
    decay = mul(jnp.tanh(low[:, :inner]), decay_up_ref[...]) + base_ref[0:1, :]
    log_ref[...] = jax.nn.sigmoid(decay) * -(2.718281828459045**-0.5)
    rate = mul(low[:, inner:], rate_up_ref[...]) + base_ref[1:2, :]
    rate_ref[...] = jax.nn.sigmoid(rate)


def lin_projections(at, normed, low, decay_up, rate_up, bases, sent):
    rows, width = normed.shape
    lanes = sent[0].shape[2] // 2
    tall = rows // 4
    whole = pl.BlockSpec(memory_space=pltpu.VMEM)
    return pl.pallas_call(
        lin_kernel,
        grid=(rows // tall,),
        out_shape=(
            jax.ShapeDtypeStruct((rows, 3 * lanes), BF16),
            jax.ShapeDtypeStruct((rows, lanes), F32),
            jax.ShapeDtypeStruct((rows, lanes), F32),
        ),
        in_specs=[
            pl.BlockSpec(memory_space=pltpu.SMEM),
            pl.BlockSpec((tall, width), lambda s: (s, 0)),
        ]
        + [whole] * (4 + len(sent)),
        out_specs=(
            pl.BlockSpec((tall, 3 * lanes), lambda s: (s, 0)),
            pl.BlockSpec((tall, lanes), lambda s: (s, 0)),
            pl.BlockSpec((tall, lanes), lambda s: (s, 0)),
        ),
        scratch_shapes=[pltpu.VMEM((width, 3 * lanes), BF16)],
        compiler_params=pltpu.CompilerParams(vmem_limit_bytes=24 * MIB),
        cost_estimate=pl.CostEstimate(
            flops=10 * rows * width * lanes,
            bytes_accessed=2 * rows * width,
            transcendentals=3 * rows * lanes,
        ),
        name="lin_projections",
    )(at, normed, low, decay_up, rate_up, bases, *sent)


def heads_kernel(back_ref, q_ref, o_ref, gain_ref, out_ref):
    n = HEAD_CHANNELS
    lanes = 2 * n
    pairs, _, tok_count = back_ref.shape
    _, rows, _ = out_ref.shape
    head_block = (places((lanes, lanes), 0) < n) == (places((lanes, lanes), 1) < n)
    average = jnp.where(head_block, 1.0 / n, 0.0).astype(BF16)
    first = places((n // 2, lanes), 1) < n
    gain = gain_ref[...].astype(F32)

    def mean(values):
        high = values.astype(BF16)
        low = (values - high.astype(F32)).astype(BF16)
        return mul(high, average) + mul(low, average)

    raws = []
    for s in range(pairs // 2):
        here = slice(s * tok_count, (s + 1) * tok_count)
        group, at = s * tok_count // rows, s * tok_count % rows
        fox = jnp.concatenate((back_ref[2 * s, :n, :], back_ref[2 * s + 1, :n, :]), 0)
        out_ref[group, at : at + tok_count, :lanes] = fox.astype(F32).T.astype(BF16)
        packed = [back_ref[2 * s + k, n:, :].astype(F32) for k in range(2)]
        turned = [pltpu.roll(x, n, 1) for x in packed]
        state = jnp.concatenate(
            (
                jnp.where(first, packed[0], 0.0),
                jnp.where(first, turned[0], 0.0),
                jnp.where(first, 0.0, turned[1]),
                jnp.where(first, 0.0, packed[1]),
            ),
            0,
        )
        raws.append(mul(q_ref[here, :], state, NT) + o_ref[here, :])
    centred = [raw - mean(raw) for raw in raws]
    spreads = [mean(x * x) for x in centred]
    for s, (x, spread) in enumerate(zip(centred, spreads)):
        group, at = s * tok_count // rows, s * tok_count % rows
        lin = x * lax.rsqrt(spread + 0.00064) * gain
        out_ref[group, at : at + tok_count, lanes:] = lin.astype(BF16)


def heads_out(back, query, ready, gain, groups):
    rows, lanes = query.shape
    whole = pl.BlockSpec(memory_space=pltpu.VMEM)
    return pl.pallas_call(
        heads_kernel,
        out_shape=pltpu.HBM((groups, rows // groups, 2 * lanes), BF16),
        in_specs=[whole] * 4,
        out_specs=whole,
        compiler_params=pltpu.CompilerParams(vmem_limit_bytes=16 * MIB),
        cost_estimate=pl.CostEstimate(
            flops=10 * rows * lanes * lanes, bytes_accessed=12 * rows * lanes, transcendentals=0
        ),
        name="heads_out",
    )(back, query, ready, gain)


def closing_kernel(seq_ref, acts_ref, fox_w_ref, lin_w_ref, out_ref, act_scr):
    groups, _, both = acts_ref.shape
    rows = act_scr.shape[0]
    lanes = both // 2
    cols = groups * lanes

    @pl.when(pl.program_id(0) == 0)
    def _():
        here = pl.ds(pl.multiple_of(seq_ref[0] * rows, rows), rows)
        for g in range(groups):
            act_scr[:, g * lanes : (g + 1) * lanes] = acts_ref[g, here, :lanes]
            act_scr[:, cols + g * lanes : cols + (g + 1) * lanes] = acts_ref[g, here, lanes:]

    turned = lax.dot_general(
        fox_w_ref[...], act_scr[:, :cols], NT, preferred_element_type=F32
    ) + lax.dot_general(lin_w_ref[...], act_scr[:, cols:], NT, preferred_element_type=F32)
    out_ref[...] = turned.T.astype(BF16)


def closing(part, parts, acts, fox_w, lin_w):
    _, rows, _ = acts.shape
    rows = rows // parts
    width, cols = fox_w.shape
    tile = 512
    return pl.pallas_call(
        closing_kernel,
        grid=(width // tile,),
        out_shape=jax.ShapeDtypeStruct((rows, width), BF16),
        in_specs=[
            pl.BlockSpec(memory_space=pltpu.SMEM),
            pl.BlockSpec(memory_space=pltpu.VMEM),
            pl.BlockSpec((tile, cols), lambda i: (i, 0)),
            pl.BlockSpec((tile, cols), lambda i: (i, 0)),
        ],
        out_specs=pl.BlockSpec((rows, tile), lambda i: (0, i)),
        scratch_shapes=[pltpu.VMEM((rows, 2 * cols), BF16)],
        compiler_params=pltpu.CompilerParams(vmem_limit_bytes=16 * MIB),
        cost_estimate=pl.CostEstimate(
            flops=4 * rows * cols * width,
            bytes_accessed=4 * cols * width + 2 * rows * width,
            transcendentals=0,
        ),
        name="closing",
    )(part, acts, fox_w, lin_w)


def exchange(x, axis):
    return lax.all_to_all(x, axis, 0, 0, tiled=True)


def in_turn(x, axis):
    size = lax.axis_size(axis)
    here = lax.axis_index(axis)
    return [lax.dynamic_index_in_dim(x, lax.rem(here + d, size), 0, False) for d in range(size)]


def by_permutes(blocks, axis):
    size = lax.axis_size(axis)
    return [
        lax.ppermute(block, axis, [(i, (i + d) % size) for i in range(size)]) if d else block
        for d, block in enumerate(blocks)
    ]


def per_device(
    inputs,
    input_norm_gain,
    softmax_query_matrix,
    softmax_key_matrix,
    softmax_value_matrix,
    running_forget_gate,
    receptance_weight,
    linear_key_weight,
    linear_value_weight,
    decay_lower_map,
    decay_upper_map,
    decay_offset_base,
    decay_extra_log,
    rate_lower_map,
    rate_upper_map,
    rate_offset_base,
    linear_head_gain,
    starting_state,
    softmax_output_weight,
    linear_output_weight,
):
    n = HEAD_CHANNELS
    seq_count, tok_count, half_width = inputs.shape
    rows = seq_count * tok_count
    cols = softmax_query_matrix.shape[1]
    groups, tp = lax.axis_size("fs"), lax.axis_size("tp")
    lanes = cols // groups
    heads = lanes // n
    seqs = groups * seq_count
    length = running_forget_gate.shape[1]
    place = lax.axis_index("sp")
    col_start = lax.axis_index("tp") * cols + lax.axis_index("fs") * lanes

    here, side = lax.axis_index("fs"), lax.axis_index("tp").astype(jnp.int32)
    at = jnp.stack((side, here)).astype(jnp.int32)
    mine = exchange(
        packed(
            (inputs.reshape(rows, half_width),),
            (softmax_query_matrix, softmax_key_matrix, softmax_value_matrix),
            groups,
        ),
        "fs",
    )
    lin_sent = packed((), (receptance_weight, linear_key_weight, linear_value_weight), groups)
    mine, lin_sent = lax.optimization_barrier((mine, in_turn(lin_sent, "fs")))
    lin_sent = by_permutes(lin_sent, "fs")

    pair_seq, pair_head = place // heads, lax.rem(place, heads)
    pair_group, pair_slot = pair_seq // seq_count, lax.rem(pair_seq, seq_count)

    def of_pair(table, head_dim):
        table = lax.dynamic_index_in_dim(table, pair_slot, 0, False)
        shape = table.shape
        table = table.reshape(*shape[:head_dim], groups, heads, *shape[head_dim + 1 :])
        return lax.dynamic_index_in_dim(table, pair_head, head_dim + 1, False)

    state = of_pair(starting_state, 0)
    state = jnp.concatenate((state[:, : n // 2], state[:, n // 2 :]), 2)
    gates = of_pair(running_forget_gate, 1).T.reshape(groups, length // tok_count, tok_count)
    extra = decay_extra_log.reshape(seq_count, tok_count, groups, heads).transpose(2, 0, 3, 1)
    extra = extra.reshape(groups, seq_count * heads, tok_count)
    small = in_turn(jnp.concatenate((state, gates, extra), 1), "fs")
    small = jnp.stack(by_permutes(small, "fs"))
    half, after = n // 2, n // 2 + length // tok_count

    def small_from(group):
        return lax.dynamic_index_in_dim(small, lax.rem(here + groups - group, groups), 0, False)

    extra = jnp.concatenate([small_from(g)[after:] for g in range(groups)], 0)
    extra = extra.reshape(seqs, heads, tok_count)
    pair = small_from(pair_group)
    start, gate = pair[:half], pair[half:after]

    def own_columns(table, axis):
        return lax.dynamic_slice_in_dim(table, col_start, lanes, axis)

    def own_first(table, axis):
        return jnp.where(side == 0, table, jnp.roll(table, half_width, axis))

    swap = [(i, tp - 1 - i) for i in range(tp)]
    other = lax.ppermute(mine[:, : half_width // (2 * lanes)], "tp", swap)
    fox, normed = fox_projections(
        at, mine, other, own_first(input_norm_gain.reshape(1, -1), 1), tok_count
    )
    fox = exchange(fox, "sp")
    lin, logged, rate = lin_projections(
        at,
        normed,
        own_first(jnp.concatenate((decay_lower_map, rate_lower_map), 1), 0),
        own_columns(decay_upper_map, 1),
        own_columns(rate_upper_map, 1),
        jnp.stack((own_columns(decay_offset_base, 0), own_columns(rate_offset_base, 0))),
        lin_sent,
    )
    query, ready, maps = position_maps(lin, logged, rate, extra)
    maps, fox = lax.optimization_barrier((maps, fox))
    maps = exchange(maps, "sp")
    fox_out = attention(fox, gate)
    back = exchange(states_ahead(maps, start, fox_out), "sp")
    gain = own_columns(linear_head_gain, 0).reshape(1, lanes)
    acts = exchange(heads_out(back, query, ready, gain, groups), "fs")
    weights = (softmax_output_weight, linear_output_weight)
    theirs = closing((tp - 1 - side).reshape(1), tp, acts, *weights)
    theirs = lax.ppermute(theirs, "tp", swap)
    own = closing(side.reshape(1), tp, acts, *weights)
    mixed = (own.astype(F32) + theirs.astype(F32)).reshape(seq_count // tp, tok_count, -1)
    return mixed.astype(BF16)


def solution(mesh):
    placed = (
        P(("grp", "fs"), "sp", "tp"),
        P(),
        P("fs", "tp"),
        P("fs", "tp"),
        P("fs", "tp"),
        P(("grp", "fs"), None, "tp"),
        P("fs", "tp"),
        P("fs", "tp"),
        P("fs", "tp"),
        P(),
        P(),
        P(),
        P(("grp", "fs"), "sp", "tp"),
        P(),
        P(),
        P(),
        P(),
        P(("grp", "fs"), "tp", None, None),
        P(None, "tp"),
        P(None, "tp"),
    )

    return jax.shard_map(
        per_device,
        mesh=mesh,
        in_specs=placed,
        out_specs=P(("grp", "fs", "tp"), "sp", None),
        check_vma=False,
    )
```

```python
import functools

import jax
import jax.numpy as jnp
from jax import lax
from jax.experimental import pallas as pl
from jax.experimental.pallas import tpu as pltpu
from jax.sharding import PartitionSpec as P

HEAD_CHANNELS = 64
CHUNK = 64
F32 = jnp.float32
BF16 = jnp.bfloat16
MIB = 1024 * 1024
VMEM_BYTES = 56 * MIB

MM = (((1,), (0,)), ((), ()))
NT = (((1,), (1,)), ((), ()))
TN = (((0,), (0,)), ((), ()))


def mul(left, right, dims=MM):
    return lax.dot_general(
        left.astype(BF16), right.astype(BF16), dims, preferred_element_type=F32
    )


def places(shape, dim):
    return lax.broadcasted_iota(jnp.int32, shape, dim)


def attention_kernel(blocks_ref, gate_ref, out_ref, key_scr, value_scr):
    count, _, width = blocks_ref.shape
    channels = HEAD_CHANNELS
    for i in range(count):
        gate = gate_ref[i : i + 1, :]
        high = gate.astype(BF16).astype(F32)
        rest = gate - high
        middle = rest.astype(BF16).astype(F32)
        low = rest - middle
        row = places((channels, width), 0)
        extra = jnp.where(row == 0, high, jnp.where(row == 1, middle, jnp.where(row == 2, low, 0.0)))
        key_rows = blocks_ref[i, channels : 2 * channels, :].astype(F32)
        key_scr[i * width : (i + 1) * width, :] = jnp.concatenate((key_rows, extra), 0).T.astype(BF16)
        value_scr[:, i * width : (i + 1) * width] = blocks_ref[i, 2 * channels :, :]
    step = 2 * width
    row = places((channels, step), 0)
    tail = jnp.where(row < 3, -1.0, 0.0).astype(BF16)
    live = places((step, step), 0) <= places((step, step), 1)
    for i in range(count // 2):
        query = jnp.concatenate(
            (blocks_ref[2 * i, :channels, :], blocks_ref[2 * i + 1, :channels, :]), 1
        )
        query = (query.astype(F32) * channels ** (-0.5)).astype(BF16)
        query = jnp.concatenate((query, tail), 0)
        before = i * step
        own = lax.dot_general(
            key_scr[before : before + step, :], query, MM, preferred_element_type=F32
        )
        own = jnp.where(live, own, -1e30)
        top = jnp.max(own, axis=0, keepdims=True)
        if before:
            past = lax.dot_general(key_scr[:before, :], query, MM, preferred_element_type=F32)
            top = jnp.maximum(top, jnp.max(past, axis=0, keepdims=True))
        weight = jnp.exp(own - top)
        total = jnp.sum(weight, axis=0, keepdims=True)
        mixed = lax.dot_general(
            value_scr[:, before : before + step],
            weight.astype(BF16),
            MM,
            preferred_element_type=F32,
        )
        if before:
            weight = jnp.exp(past - top)
            total = total + jnp.sum(weight, axis=0, keepdims=True)
            mixed = mixed + lax.dot_general(
                value_scr[:, :before], weight.astype(BF16), MM, preferred_element_type=F32
            )
        mixed = (mixed / total).astype(BF16)
        out_ref[2 * i] = mixed[:, :width]
        out_ref[2 * i + 1] = mixed[:, width:]


def attention(blocks, gate):
    count, rows, width = blocks.shape
    whole = pl.BlockSpec(memory_space=pltpu.VMEM)
    return pl.pallas_call(
        attention_kernel,
        out_shape=pltpu.HBM((count, HEAD_CHANNELS, width), BF16),
        in_specs=[whole, whole],
        out_specs=whole,
        scratch_shapes=[
            pltpu.VMEM((count * width, 2 * HEAD_CHANNELS), BF16),
            pltpu.VMEM((HEAD_CHANNELS, count * width), BF16),
        ],
        compiler_params=pltpu.CompilerParams(vmem_limit_bytes=16 * MIB),
        cost_estimate=pl.CostEstimate(
            flops=4 * HEAD_CHANNELS * (count * width) ** 2,
            bytes_accessed=4 * count * rows * width,
            transcendentals=(count * width) ** 2 // 2,
        ),
        name="attention",
    )(blocks, gate)


def chunk_masks(size):
    row, col = places((2 * size, 2 * size), 0), places((2 * size, 2 * size), 1)
    same = row // CHUNK == col // CHUNK
    return row, col, same


def maps_kernel(proj_ref, log_ref, rate_ref, extra_ref, q_ref, o_ref, maps_ref):
    seqs, _, size = extra_ref.shape
    lanes = 2 * HEAD_CHANNELS
    row, col, same = chunk_masks(size)
    strict = same & (row > col)
    upto = same & (row >= col)
    merges = []
    block = 2
    while block < CHUNK:
        merges.append((row // (2 * block) == col // (2 * block)) & (row // block > col // block))
        block *= 2
    pairs_of_two = (row // 2 == col // 2) & (row > col)
    identity = (row == col).astype(F32)
    lane = places((size, lanes), 1)
    first_head = lane < HEAD_CHANNELS
    head_block = (places((lanes, lanes), 0) < HEAD_CHANNELS) == (
        places((lanes, lanes), 1) < HEAD_CHANNELS
    )
    diagonal = places((lanes, lanes), 0) == places((lanes, lanes), 1)
    small_row, small_col = places((size, size), 0), places((size, size), 1)
    running = ((small_row // CHUNK == small_col // CHUNK) & (small_row >= small_col)).astype(F32)
    head_sum = head_block.astype(F32)
    tops, bottoms = slice(0, CHUNK), slice(CHUNK, 2 * CHUNK)

    def stacked(values):
        return jnp.concatenate(
            (jnp.where(first_head, values, 0.0), jnp.where(first_head, 0.0, values)), 0
        )

    def each_chunk(values, at):
        return jnp.concatenate(
            [jnp.broadcast_to(values[c + at : c + at + 1], (CHUNK, lanes)) for c in (0, CHUNK)], 0
        )

    held = []
    for p in range(seqs):
        at = slice(p * size, (p + 1) * size)
        rec = proj_ref[at, :lanes].astype(F32)
        key = proj_ref[at, lanes : 2 * lanes].astype(F32)
        value = proj_ref[at, 2 * lanes :].astype(F32)
        by_head = [
            jnp.broadcast_to(extra_ref[p, k : k + 1, :], (HEAD_CHANNELS, size)) for k in range(2)
        ]
        logged = log_ref[at, :] + jnp.concatenate(by_head, 0).T
        squares = lax.dot_general(
            key * key, head_sum, MM, precision=lax.Precision.HIGHEST, preferred_element_type=F32
        )
        unit = key * lax.rsqrt(squares + 1e-06)
        beta = unit * rate_ref[at, :]
        total = lax.dot_general(
            running, logged, MM, precision=lax.Precision.HIGHEST, preferred_element_type=F32
        )
        middle = each_chunk(total, CHUNK // 2 - 1)
        ending = each_chunk(total, CHUNK - 1)
        previous = total - logged
        fall = jnp.exp(middle - total)
        to_end = jnp.exp(ending - total)
        zeta = -unit
        left = jnp.concatenate(
            (stacked(zeta * jnp.exp(previous - middle)), stacked(rec * jnp.exp(total - middle))), 0
        )
        right = jnp.concatenate((beta * fall, key * fall), 0)
        held.append(
            dict(
                grams=mul(left, right, NT),
                zeta_true=zeta * jnp.exp(previous),
                rec_true=rec * jnp.exp(total),
                beta_end=beta * to_end,
                key_end=key * to_end,
                value=value,
                ending=jnp.exp(total),
            )
        )
    for h in held:
        grams = h.pop("grams")
        blank = jnp.zeros((size, size), F32)

        def spread(first, second, mask):
            both = jnp.concatenate(
                (
                    jnp.concatenate((first, blank), 1),
                    jnp.concatenate((blank, second), 1),
                ),
                0,
            )
            return jnp.where(mask, both, 0.0).astype(BF16)

        h["zb"] = spread(grams[:size, :size], grams[size : 2 * size, :size], strict)
        h["zk"] = spread(grams[:size, size:], grams[size : 2 * size, size:], strict)
        h["rb"] = spread(grams[2 * size : 3 * size, :size], grams[3 * size :, :size], upto)
        h["rk"] = spread(grams[2 * size : 3 * size, size:], grams[3 * size :, size:], upto)
        h["inverse"] = identity + jnp.where(pairs_of_two, h["zb"].astype(F32), 0.0)
        h["from_values"] = mul(
            jnp.concatenate((h["zk"], h["rk"]), 0), stacked(h["value"])
        )
    for merge in merges:
        for h in held:
            inner = mul(jnp.where(merge, h["zb"].astype(F32), 0.0), h["inverse"])
            h["inner"] = inner
        for h in held:
            h["inverse"] = h["inverse"] + mul(h["inverse"], h["inner"])
    for h in held:
        right = jnp.concatenate((stacked(h["zeta_true"]), h["from_values"][: 2 * size]), 1)
        h["pulled"] = mul(h["inverse"], right)
    for p, h in enumerate(held):
        start = jnp.concatenate((stacked(h["rec_true"]), h["from_values"][2 * size :]), 1)
        seen = start + mul(h["rb"], h["pulled"])
        seen = seen[:size] + seen[size:]
        pulled = h["pulled"][:size] + h["pulled"][size:]
        query, ready = seen[:, :lanes], seen[:, lanes:]
        maps = []
        for part, last in ((tops, CHUNK - 1), (bottoms, 2 * CHUNK - 1)):
            moved = mul(pulled[part], h["beta_end"][part], TN)
            added = mul(h["value"][part], h["key_end"][part], TN)
            kept = jnp.where(diagonal, h["ending"][last : last + 1], 0.0)
            maps.append(
                (
                    kept + jnp.where(head_block, moved[:lanes], 0.0),
                    jnp.where(head_block, moved[lanes:] + added, 0.0),
                )
            )
        both = mul(jnp.concatenate(maps[0], 0), maps[1][0])
        carry = both[:lanes]
        offset = both[lanes:] + maps[1][1]
        later = mul(query[bottoms], jnp.concatenate(maps[0], 0), NT)
        query = jnp.concatenate((query[tops], later[:, :lanes]), 0)
        ready = jnp.concatenate((ready[tops], ready[bottoms] + later[:, lanes:]), 0)
        at = slice(p * size, (p + 1) * size)
        q_ref[at, :] = query.astype(BF16)
        o_ref[at, :] = ready
        half = places((HEAD_CHANNELS, lanes), 1) < HEAD_CHANNELS
        turned_offset = pltpu.roll(offset, HEAD_CHANNELS, 1)
        turned_carry = pltpu.roll(carry, HEAD_CHANNELS, 1)
        maps_ref[2 * p] = jnp.where(
            half, carry[:HEAD_CHANNELS], turned_offset[:HEAD_CHANNELS]
        ).astype(BF16)
        maps_ref[2 * p + 1] = jnp.where(
            half, turned_carry[HEAD_CHANNELS:], offset[HEAD_CHANNELS:]
        ).astype(BF16)


def position_maps(proj, logged, rate, extra):
    seqs, heads, tok_count = extra.shape
    rows, lanes = logged.shape
    group = seqs // 2
    return pl.pallas_call(
        maps_kernel,
        grid=(seqs // group,),
        out_shape=(
            pltpu.HBM((rows, lanes), BF16),
            jax.ShapeDtypeStruct((rows, lanes), F32),
            jax.ShapeDtypeStruct((seqs * heads, HEAD_CHANNELS, lanes), BF16),
        ),
        in_specs=[
            pl.BlockSpec((group * tok_count, 3 * lanes), lambda s: (s, 0)),
            pl.BlockSpec((group * tok_count, lanes), lambda s: (s, 0)),
            pl.BlockSpec((group * tok_count, lanes), lambda s: (s, 0)),
            pl.BlockSpec((group, heads, tok_count), lambda s: (s, 0, 0)),
        ],
        out_specs=(
            pl.BlockSpec((group * tok_count, lanes), lambda s: (s, 0)),
            pl.BlockSpec((group * tok_count, lanes), lambda s: (s, 0)),
            pl.BlockSpec((group * heads, HEAD_CHANNELS, lanes), lambda s: (s, 0, 0)),
        ),
        compiler_params=pltpu.CompilerParams(vmem_limit_bytes=24 * MIB),
        cost_estimate=pl.CostEstimate(
            flops=rows * lanes * 2 * 256 * 20,
            bytes_accessed=rows * lanes * 20,
            transcendentals=6 * rows * lanes,
        ),
        name="position_maps",
    )(proj, logged, rate, extra)


def states_kernel(maps_ref, start_ref, fox_ref, out_ref, sem):
    count = maps_ref.shape[0]
    n = HEAD_CHANNELS
    copy = pltpu.make_async_copy(fox_ref, out_ref.at[:, :n, :], sem)
    copy.start()
    state = jnp.concatenate((start_ref[:, :n], start_ref[:, n:]), 0)
    for i in range(count):
        out_ref[i, n:, :] = jnp.concatenate((state[: n // 2], state[n // 2 :]), 1).astype(BF16)
        if i + 1 < count:
            pair = maps_ref[i]
            high = state.astype(BF16)
            low = (state - high.astype(F32)).astype(BF16)
            moved = mul(jnp.concatenate((high, low), 0), pair[:, :n])
            state = moved[:n] + moved[n:] + pair[:, n:].astype(F32)
    copy.wait()


def states_ahead(maps, start, fox):
    count = maps.shape[0]
    whole = pl.BlockSpec(memory_space=pltpu.VMEM)
    return pl.pallas_call(
        states_kernel,
        out_shape=jax.ShapeDtypeStruct((count, 3 * HEAD_CHANNELS // 2, 2 * HEAD_CHANNELS), BF16),
        in_specs=[whole, whole, pl.BlockSpec(memory_space=pltpu.HBM)],
        out_specs=whole,
        scratch_shapes=[pltpu.SemaphoreType.DMA],
        compiler_params=pltpu.CompilerParams(vmem_limit_bytes=16 * MIB),
        cost_estimate=pl.CostEstimate(
            flops=count * 4 * HEAD_CHANNELS**3, bytes_accessed=1 << 19, transcendentals=0
        ),
        name="states_ahead",
    )(maps, start, pltpu.with_memory_space_constraint(fox, pltpu.HBM))


def pack_kernel(groups, *refs):
    *piece_refs, out_ref, sems = refs
    leading, weights = piece_refs[:-3], piece_refs[-3:]
    _, _, rows, wide = out_ref.shape
    lanes = weights[0].shape[1] // groups
    copies = []

    def send(source, group, at):
        block, start = at // wide, at % wide
        target = out_ref.at[group, block, :, start : start + source.shape[1]]
        copies.append(pltpu.make_async_copy(source, target, sems.at[len(copies)]))

    for g in range(groups):
        at = 0
        for ref in leading:
            for start in range(0, ref.shape[1], wide):
                send(ref.at[:, start : start + wide], g, at)
                at += wide
        for k in range(2):
            for ref in weights:
                send(ref.at[k * rows : (k + 1) * rows, g * lanes : (g + 1) * lanes], g, at)
                at += lanes
    for copy in copies:
        copy.start()
    for copy in copies:
        copy.wait()


def packed(leading, weights, groups):
    rows, cols = weights[0].shape
    wide = 2 * cols // groups
    blocks = sum(x.shape[1] for x in leading) // wide + 3
    whole = pl.BlockSpec(memory_space=pltpu.VMEM)
    return pl.pallas_call(
        functools.partial(pack_kernel, groups),
        out_shape=jax.ShapeDtypeStruct((groups, blocks, rows // 2, wide), BF16),
        in_specs=[whole] * (len(leading) + 3),
        out_specs=pl.BlockSpec(memory_space=pl.ANY),
        scratch_shapes=[pltpu.SemaphoreType.DMA((groups * (blocks + 3),))],
        compiler_params=pltpu.CompilerParams(vmem_limit_bytes=VMEM_BYTES),
        cost_estimate=pl.CostEstimate(
            flops=1 << 20, bytes_accessed=2 * groups * blocks * rows * wide, transcendentals=0
        ),
        name="packed",
    )(*leading, *weights)


def fox_kernel(
    at_ref,
    mine_ref,
    other_ref,
    first_ref,
    second_ref,
    third_ref,
    gain_ref,
    fox_ref,
    normed_ref,
    weight_scr,
):
    n = HEAD_CHANNELS
    groups = first_ref.shape[0]
    _, blocks, rows, wide = other_ref.shape
    pairs, _, tok_count = fox_ref.shape
    heads = pairs * tok_count // rows
    lanes = heads * n

    @pl.when(pl.program_id(0) == 0)
    def _():
        for i in range(groups):
            source = lax.rem(i + at_ref[0] * (groups // 2), groups)
            upper = slice(2 * i * rows, (2 * i + 1) * rows)
            lower = slice((2 * i + 1) * rows, (2 * i + 2) * rows)
            weight_scr[upper, : 2 * lanes] = first_ref[source, 0]
            weight_scr[upper, 2 * lanes :] = second_ref[source, 0, :, :lanes]
            weight_scr[lower, :lanes] = second_ref[source, 0, :, lanes:]
            weight_scr[lower, lanes:] = third_ref[source, 0]

    pieces = [ref[0, i].astype(F32) for ref in (mine_ref, other_ref) for i in range(blocks)]
    square = sum(jnp.sum(x * x, axis=1, keepdims=True) for x in pieces)
    scaling = lax.rsqrt(square / (2 * blocks * wide) + 1e-06)
    normed = jnp.concatenate(
        [
            (x * scaling * gain_ref[:, i * wide : (i + 1) * wide].astype(F32)).astype(BF16)
            for i, x in enumerate(pieces)
        ],
        1,
    )
    normed_ref[...] = normed
    fox = lax.dot_general(normed, weight_scr[...], MM, preferred_element_type=F32)
    for s in range(rows // tok_count):
        here = slice(s * tok_count, (s + 1) * tok_count)
        for k in range(3):
            turned = fox[here, k * lanes : (k + 1) * lanes].T.astype(BF16)
            for h in range(heads):
                fox_ref[s * heads + h, k * n : (k + 1) * n, :] = turned[h * n : (h + 1) * n]


def fox_projections(at, mine, other, gain, tok_count):
    groups, blocks, rows, wide = other.shape
    width, lanes = blocks * wide, wide // 2
    heads = lanes // HEAD_CHANNELS
    pairs = rows // tok_count * heads
    whole = pl.BlockSpec(memory_space=pltpu.VMEM)
    return pl.pallas_call(
        fox_kernel,
        grid=(groups,),
        out_shape=(
            jax.ShapeDtypeStruct((groups * pairs, 3 * HEAD_CHANNELS, tok_count), BF16),
            pltpu.HBM((groups * rows, 2 * width), BF16),
        ),
        in_specs=[
            pl.BlockSpec(memory_space=pltpu.SMEM),
            pl.BlockSpec((1, blocks, rows, wide), lambda g: (g, 0, 0, 0)),
            pl.BlockSpec((1, blocks, rows, wide), lambda g: (g, 0, 0, 0)),
            *(
                pl.BlockSpec((groups, 1, rows, wide), lambda g, at=at: (0, at, 0, 0))
                for at in range(blocks, blocks + 3)
            ),
            whole,
        ],
        out_specs=(
            pl.BlockSpec((pairs, 3 * HEAD_CHANNELS, tok_count), lambda g: (g, 0, 0)),
            pl.BlockSpec((rows, 2 * width), lambda g: (g, 0)),
        ),
        scratch_shapes=[pltpu.VMEM((2 * width, 3 * lanes), BF16)],
        compiler_params=pltpu.CompilerParams(vmem_limit_bytes=24 * MIB),
        cost_estimate=pl.CostEstimate(
            flops=12 * groups * rows * width * lanes,
            bytes_accessed=8 * groups * rows * width,
            transcendentals=0,
        ),
        name="fox_projections",
    )(at, mine, other, mine, mine, mine, gain)


def lin_kernel(at_ref, normed_ref, low_ref, decay_up_ref, rate_up_ref, base_ref, *rest):
    sent_refs, (lin_ref, log_ref, rate_ref, weight_scr) = rest[:-4], rest[-4:]
    groups = len(sent_refs)
    _, rows, wide = sent_refs[0].shape
    lanes = wide // 2

    @pl.when(pl.program_id(0) == 0)
    def _():
        for d, ref in enumerate(sent_refs):
            source = lax.rem(at_ref[1] + (groups - d), groups)
            place = lax.rem(source + at_ref[0] * (groups // 2), groups)
            upper = pl.ds(pl.multiple_of(2 * place * rows, rows), rows)
            lower = pl.ds(pl.multiple_of((2 * place + 1) * rows, rows), rows)
            weight_scr[upper, : 2 * lanes] = ref[0]
            weight_scr[upper, 2 * lanes :] = ref[1, :, :lanes]
            weight_scr[lower, :lanes] = ref[1, :, lanes:]
            weight_scr[lower, lanes:] = ref[2]

    normed = normed_ref[...]
    lin_ref[...] = lax.dot_general(
        normed, weight_scr[...], MM, preferred_element_type=F32
    ).astype(BF16)
    low = lax.dot_general(normed, low_ref[...], MM, preferred_element_type=F32)
    inner = low.shape[1] // 2
    decay = mul(jnp.tanh(low[:, :inner]), decay_up_ref[...]) + base_ref[0:1, :]
    log_ref[...] = jax.nn.sigmoid(decay) * -(2.718281828459045**-0.5)
    rate = mul(low[:, inner:], rate_up_ref[...]) + base_ref[1:2, :]
    rate_ref[...] = jax.nn.sigmoid(rate)


def lin_projections(at, normed, low, decay_up, rate_up, bases, sent):
    rows, width = normed.shape
    lanes = sent[0].shape[2] // 2
    tall = rows // 4
    whole = pl.BlockSpec(memory_space=pltpu.VMEM)
    return pl.pallas_call(
        lin_kernel,
        grid=(rows // tall,),
        out_shape=(
            jax.ShapeDtypeStruct((rows, 3 * lanes), BF16),
            jax.ShapeDtypeStruct((rows, lanes), F32),
            jax.ShapeDtypeStruct((rows, lanes), F32),
        ),
        in_specs=[
            pl.BlockSpec(memory_space=pltpu.SMEM),
            pl.BlockSpec((tall, width), lambda s: (s, 0)),
        ]
        + [whole] * (4 + len(sent)),
        out_specs=(
            pl.BlockSpec((tall, 3 * lanes), lambda s: (s, 0)),
            pl.BlockSpec((tall, lanes), lambda s: (s, 0)),
            pl.BlockSpec((tall, lanes), lambda s: (s, 0)),
        ),
        scratch_shapes=[pltpu.VMEM((width, 3 * lanes), BF16)],
        compiler_params=pltpu.CompilerParams(vmem_limit_bytes=24 * MIB),
        cost_estimate=pl.CostEstimate(
            flops=10 * rows * width * lanes,
            bytes_accessed=2 * rows * width,
            transcendentals=3 * rows * lanes,
        ),
        name="lin_projections",
    )(at, normed, low, decay_up, rate_up, bases, *sent)


def heads_kernel(back_ref, q_hbm_ref, o_ref, gain_ref, out_ref, q_ref, sem):
    copy = pltpu.make_async_copy(q_hbm_ref, q_ref, sem)
    copy.start()
    n = HEAD_CHANNELS
    lanes = 2 * n
    pairs, _, tok_count = back_ref.shape
    _, rows, _ = out_ref.shape
    head_block = (places((lanes, lanes), 0) < n) == (places((lanes, lanes), 1) < n)
    average = jnp.where(head_block, 1.0 / n, 0.0).astype(BF16)
    first = places((n // 2, lanes), 1) < n
    gain = gain_ref[...].astype(F32)

    def mean(values):
        high = values.astype(BF16)
        low = (values - high.astype(F32)).astype(BF16)
        return mul(high, average) + mul(low, average)

    for s in range(pairs // 2):
        group, at = s * tok_count // rows, s * tok_count % rows
        fox = jnp.concatenate((back_ref[2 * s, :n, :], back_ref[2 * s + 1, :n, :]), 0)
        out_ref[group, at : at + tok_count, :lanes] = fox.astype(F32).T.astype(BF16)
    copy.wait()
    raws = []
    for s in range(pairs // 2):
        here = slice(s * tok_count, (s + 1) * tok_count)
        packed = [back_ref[2 * s + k, n:, :].astype(F32) for k in range(2)]
        turned = [pltpu.roll(x, n, 1) for x in packed]
        state = jnp.concatenate(
            (
                jnp.where(first, packed[0], 0.0),
                jnp.where(first, turned[0], 0.0),
                jnp.where(first, 0.0, turned[1]),
                jnp.where(first, 0.0, packed[1]),
            ),
            0,
        )
        raws.append(mul(q_ref[here, :], state, NT) + o_ref[here, :])
    centred = [raw - mean(raw) for raw in raws]
    spreads = [mean(x * x) for x in centred]
    for s, (x, spread) in enumerate(zip(centred, spreads)):
        group, at = s * tok_count // rows, s * tok_count % rows
        lin = x * lax.rsqrt(spread + 0.00064) * gain
        out_ref[group, at : at + tok_count, lanes:] = lin.astype(BF16)


def heads_out(back, query, ready, gain, groups):
    rows, lanes = query.shape
    whole = pl.BlockSpec(memory_space=pltpu.VMEM)
    return pl.pallas_call(
        heads_kernel,
        out_shape=pltpu.HBM((groups, rows // groups, 2 * lanes), BF16),
        in_specs=[whole, pl.BlockSpec(memory_space=pltpu.HBM), whole, whole],
        out_specs=whole,
        scratch_shapes=[pltpu.VMEM((rows, lanes), BF16), pltpu.SemaphoreType.DMA],
        compiler_params=pltpu.CompilerParams(vmem_limit_bytes=16 * MIB),
        cost_estimate=pl.CostEstimate(
            flops=10 * rows * lanes * lanes, bytes_accessed=12 * rows * lanes, transcendentals=0
        ),
        name="heads_out",
    )(back, pltpu.with_memory_space_constraint(query, pltpu.HBM), ready, gain)


def closing_kernel(seq_ref, acts_ref, fox_w_ref, lin_w_ref, out_ref, act_scr):
    groups, _, both = acts_ref.shape
    rows = act_scr.shape[0]
    lanes = both // 2
    cols = groups * lanes

    @pl.when(pl.program_id(0) == 0)
    def _():
        here = pl.ds(pl.multiple_of(seq_ref[0] * rows, rows), rows)
        for g in range(groups):
            act_scr[:, g * lanes : (g + 1) * lanes] = acts_ref[g, here, :lanes]
            act_scr[:, cols + g * lanes : cols + (g + 1) * lanes] = acts_ref[g, here, lanes:]

    turned = lax.dot_general(
        fox_w_ref[...], act_scr[:, :cols], NT, preferred_element_type=F32
    ) + lax.dot_general(lin_w_ref[...], act_scr[:, cols:], NT, preferred_element_type=F32)
    out_ref[...] = turned.T.astype(BF16)


def closing(part, parts, acts, fox_w, lin_w):
    _, rows, _ = acts.shape
    rows = rows // parts
    width, cols = fox_w.shape
    tile = 512
    return pl.pallas_call(
        closing_kernel,
        grid=(width // tile,),
        out_shape=jax.ShapeDtypeStruct((rows, width), BF16),
        in_specs=[
            pl.BlockSpec(memory_space=pltpu.SMEM),
            pl.BlockSpec(memory_space=pltpu.VMEM),
            pl.BlockSpec((tile, cols), lambda i: (i, 0)),
            pl.BlockSpec((tile, cols), lambda i: (i, 0)),
        ],
        out_specs=pl.BlockSpec((rows, tile), lambda i: (0, i)),
        scratch_shapes=[pltpu.VMEM((rows, 2 * cols), BF16)],
        compiler_params=pltpu.CompilerParams(vmem_limit_bytes=VMEM_BYTES),
        cost_estimate=pl.CostEstimate(
            flops=4 * rows * cols * width,
            bytes_accessed=4 * cols * width + 2 * rows * width,
            transcendentals=0,
        ),
        name="closing",
    )(part, acts, fox_w, lin_w)


def exchange(x, axis):
    return lax.all_to_all(x, axis, 0, 0, tiled=True)


def in_turn(x, axis):
    size = lax.axis_size(axis)
    here = lax.axis_index(axis)
    return [lax.dynamic_index_in_dim(x, lax.rem(here + d, size), 0, False) for d in range(size)]


def by_permutes(blocks, axis):
    size = lax.axis_size(axis)
    return [
        lax.ppermute(block, axis, [(i, (i + d) % size) for i in range(size)]) if d else block
        for d, block in enumerate(blocks)
    ]


def per_device(
    inputs,
    input_norm_gain,
    softmax_query_matrix,
    softmax_key_matrix,
    softmax_value_matrix,
    running_forget_gate,
    receptance_weight,
    linear_key_weight,
    linear_value_weight,
    decay_lower_map,
    decay_upper_map,
    decay_offset_base,
    decay_extra_log,
    rate_lower_map,
    rate_upper_map,
    rate_offset_base,
    linear_head_gain,
    starting_state,
    softmax_output_weight,
    linear_output_weight,
):
    n = HEAD_CHANNELS
    seq_count, tok_count, half_width = inputs.shape
    rows = seq_count * tok_count
    cols = softmax_query_matrix.shape[1]
    groups, tp = lax.axis_size("fs"), lax.axis_size("tp")
    lanes = cols // groups
    heads = lanes // n
    seqs = groups * seq_count
    length = running_forget_gate.shape[1]
    place = lax.axis_index("sp")
    col_start = lax.axis_index("tp") * cols + lax.axis_index("fs") * lanes

    here, side = lax.axis_index("fs"), lax.axis_index("tp").astype(jnp.int32)
    at = jnp.stack((side, here)).astype(jnp.int32)
    mine = exchange(
        packed(
            (inputs.reshape(rows, half_width),),
            (softmax_query_matrix, softmax_key_matrix, softmax_value_matrix),
            groups,
        ),
        "fs",
    )
    lin_sent = packed((), (receptance_weight, linear_key_weight, linear_value_weight), groups)
    mine, lin_sent = lax.optimization_barrier((mine, in_turn(lin_sent, "fs")))
    lin_sent = by_permutes(lin_sent, "fs")

    pair_seq, pair_head = place // heads, lax.rem(place, heads)
    pair_group, pair_slot = pair_seq // seq_count, lax.rem(pair_seq, seq_count)

    def of_pair(table, head_dim):
        table = lax.dynamic_index_in_dim(table, pair_slot, 0, False)
        shape = table.shape
        table = table.reshape(*shape[:head_dim], groups, heads, *shape[head_dim + 1 :])
        return lax.dynamic_index_in_dim(table, pair_head, head_dim + 1, False)

    state = of_pair(starting_state, 0)
    state = jnp.concatenate((state[:, : n // 2], state[:, n // 2 :]), 2)
    gates = of_pair(running_forget_gate, 1).T.reshape(groups, length // tok_count, tok_count)
    extra = decay_extra_log.reshape(seq_count, tok_count, groups, heads).transpose(2, 0, 3, 1)
    extra = extra.reshape(groups, seq_count * heads, tok_count)
    small = in_turn(jnp.concatenate((state, gates, extra), 1), "fs")
    small = jnp.stack(by_permutes(small, "fs"))
    half, after = n // 2, n // 2 + length // tok_count

    def small_from(group):
        return lax.dynamic_index_in_dim(small, lax.rem(here + groups - group, groups), 0, False)

    extra = jnp.concatenate([small_from(g)[after:] for g in range(groups)], 0)
    extra = extra.reshape(seqs, heads, tok_count)
    pair = small_from(pair_group)
    start, gate = pair[:half], pair[half:after]

    def own_columns(table, axis):
        return lax.dynamic_slice_in_dim(table, col_start, lanes, axis)

    def own_first(table, axis):
        return jnp.where(side == 0, table, jnp.roll(table, half_width, axis))

    swap = [(i, tp - 1 - i) for i in range(tp)]
    other = lax.ppermute(mine[:, : half_width // (2 * lanes)], "tp", swap)
    fox, normed = fox_projections(
        at, mine, other, own_first(input_norm_gain.reshape(1, -1), 1), tok_count
    )
    fox = exchange(fox, "sp")
    lin, logged, rate = lin_projections(
        at,
        normed,
        own_first(jnp.concatenate((decay_lower_map, rate_lower_map), 1), 0),
        own_columns(decay_upper_map, 1),
        own_columns(rate_upper_map, 1),
        jnp.stack((own_columns(decay_offset_base, 0), own_columns(rate_offset_base, 0))),
        lin_sent,
    )
    query, ready, maps = position_maps(lin, logged, rate, extra)
    maps, fox = lax.optimization_barrier((maps, fox))
    maps = exchange(maps, "sp")
    fox_out = attention(fox, gate)
    back = exchange(states_ahead(maps, start, fox_out), "sp")
    gain = own_columns(linear_head_gain, 0).reshape(1, lanes)
    acts = exchange(heads_out(back, query, ready, gain, groups), "fs")
    weights = (softmax_output_weight, linear_output_weight)
    theirs = closing((tp - 1 - side).reshape(1), tp, acts, *weights)
    theirs = lax.ppermute(theirs, "tp", swap)
    own = closing(side.reshape(1), tp, acts, *weights)
    mixed = (own.astype(F32) + theirs.astype(F32)).reshape(seq_count // tp, tok_count, -1)
    return mixed.astype(BF16)


def solution(mesh):
    placed = (
        P(("grp", "fs"), "sp", "tp"),
        P(),
        P("fs", "tp"),
        P("fs", "tp"),
        P("fs", "tp"),
        P(("grp", "fs"), None, "tp"),
        P("fs", "tp"),
        P("fs", "tp"),
        P("fs", "tp"),
        P(),
        P(),
        P(),
        P(("grp", "fs"), "sp", "tp"),
        P(),
        P(),
        P(),
        P(),
        P(("grp", "fs"), "tp", None, None),
        P(None, "tp"),
        P(None, "tp"),
    )

    return jax.shard_map(
        per_device,
        mesh=mesh,
        in_specs=placed,
        out_specs=P(("grp", "fs", "tp"), "sp", None),
        check_vma=False,
    )
```
